32 devices in a mesh: ep: 8 (over z, y), tp: 4 (over x, core).
Axes of the slice: x: 2, y: 2, z: 4, core: 2. Of those that a mesh axis runs over, the one named last changes fastest.
Arguments:
- tokens: bfloat16 [1024, 2048], P('ep'), may hold values from -6 to 6
- norm_gain: float32 [2048], replicated, may hold values from 0.1 to 1.9
- expert_ids: int32 [1024, 6], P('ep'), may hold values from 0 to 15, all different within a row; in each aligned block of 128 rows (0 to 127, 128 to 255, ...) at most 96 rows name the same one
- route_weights: float32 [1024, 6], P('ep'), may hold values from 0.1 to 1
- expert_gate: bfloat16 [32, 2048, 256], P(('ep', 'tp')), may hold values from -0.125 to 0.125
- expert_up: bfloat16 [32, 2048, 256], P(('ep', 'tp')), may hold values from -0.125 to 0.125
- expert_down: bfloat16 [32, 256, 2048], P(('ep', 'tp')), may hold values from -0.25 to 0.25
- shared_gate: bfloat16 [2048, 512], P(None, 'tp'), may hold values from -0.125 to 0.125
- shared_up: bfloat16 [2048, 512], P(None, 'tp'), may hold values from -0.125 to 0.125
- shared_down: bfloat16 [512, 2048], P(None, 'tp'), may hold values from -0.25 to 0.25
Outputs:
- mixed: bfloat16 [1024, 2048], P('ep', 'tp')
The draws below stay inside these ranges and needn't reach their ends.
Inputs may be any that keep to these rules, and one draw needn't show every extreme that they name: `expert_ids`: each row names 6 different experts. In each aligned block of 128 rows (the rows of one index of ep) no expert is named by more than 96 rows, a bound that some block reaches.
All inputs are finite; a program needn't handle non-finite values.
Results may differ from the reference program's by a relative error of at most 0.0073.
Values may be sent and summed in bfloat16 or wider, within the bound.
A program may use at most 64 MiB of HBM per device.

```python
import math
import jax
import jax.numpy as jnp
import numpy as np
from jax import lax

D = 2048
EXPERT_FF = 512
SHARED_FF = 512
TOP_K = 6
TOK_DEV = 128
EXP_HALF = 256
EXPERTS = 16
CAP = 96
TOKENS = 1024
N_EP = 8


def level_of(stream_key, extent, split, low, high):
    def one(dim, shards_of):
        heights = jax.random.uniform(jax.random.fold_in(jax.random.fold_in(stream_key, 6), dim), (shards_of,), jnp.float32, low / len(split), high / len(split))
        return jnp.repeat(jnp.exp(heights), extent[dim] // shards_of).reshape((-1,) + (1,) * (len(extent) - dim - 1))

    loudness = one(*split[0])
    for cut in split[1:]:
        loudness = loudness * one(*cut)
    return loudness


def deal_out(rng, own, number, rows, amount, top, bound, slope):
    ranking = jax.random.permutation(rng, amount)
    crowded, usual = portions_of(amount, rows * top, bound, slope, True), portions_of(amount, rows * top, bound, slope, False)
    places = jnp.arange(amount)

    def named(tallies, turn):
        used = int((tallies > 0).sum())
        fixed = max(1, used // 4)
        passed = fixed + (places - fixed + turn * (used - fixed)) % max(1, amount - fixed)
        return jnp.zeros((amount,), jnp.int32).at[ranking[jnp.where(places < fixed, places, passed)]].set(jnp.asarray(tallies, jnp.int32))

    tallies = jnp.where(number % 4 == 0, named(crowded, number // 4), named(usual, number - number // 4 - 1))
    mixed = jax.random.permutation(jax.random.fold_in(own, 3), amount)
    donor, taker = mixed[0:amount // 2 * 2:2], mixed[1:amount // 2 * 2:2]
    room = jnp.minimum(tallies[donor] - 1, bound - tallies[taker]) // 2
    room = jnp.where((donor == ranking[0]) | (taker == ranking[0]) | (tallies[taker] == 0), 0, jnp.maximum(room, 0))
    passed = jax.random.randint(jax.random.fold_in(own, 4), (amount // 2,), 0, 1 << 20) % (room + 1)
    tallies = tallies.at[donor].add(-passed).at[taker].add(passed)
    labels = jnp.searchsorted(jnp.cumsum(tallies), jnp.arange(rows * top), side="right").astype(jnp.int32)
    listing = labels.reshape(top, rows).T
    listing = listing[jax.random.permutation(jax.random.fold_in(own, 1), rows)]
    turn = jax.random.randint(jax.random.fold_in(own, 2), (rows, 1), 0, top)
    return jnp.take_along_axis(listing, (jnp.arange(top)[None, :] + turn) % top, axis=1)


def portions_of(count, total, reach, slope, full):
    loads = [(1 << 20) // math.isqrt(grade ** slope) + 1 for grade in range(1, count + 1)]
    largest = reach if full else min(reach, max(-(-total // count), total * loads[0] // sum(loads)))
    least = 1 if total - largest >= count - 1 else 0
    given, spare = [largest] + [least] * (count - 1), total - largest - least * (count - 1)
    while spare > 0:
        movable = [i for i in range(1, count) if given[i] < largest] or [i for i in range(1, count) if given[i] < reach]
        mass, budget = sum([loads[i] for i in movable]), spare
        for i in movable:
            addition = min(reach - given[i], max(1, budget * loads[i] // mass), spare)
            given[i] = given[i] + addition
            spare = spare - addition
    return np.array(given)


def bell_draw(stream_key, extent, spread, most, cuts=(), held_as=jnp.bfloat16):
    array = spread * jax.random.normal(stream_key, extent, jnp.float32)
    if cuts:
        array = array * level_of(stream_key, extent, cuts, -0.22, 0.18)
    return jnp.clip(array, -most, most).astype(held_as)


def setup_inputs(seed: int = 0) -> dict:
    keys = jax.random.split(jax.random.key(seed), 11)
    tokens = bell_draw(keys[0], (TOKENS, D), 1.0, 6.0, ((0, 8),))
    norm_gain = jnp.clip(1.0 + 0.18 * jax.random.normal(keys[1], (D,), jnp.float32), 0.1, 1.9)
    expert_ids_keys = jax.random.split(jax.random.fold_in(keys[2], 1), TOKENS // TOK_DEV)
    expert_ids_turns = jax.random.permutation(jax.random.fold_in(keys[2], 3), TOKENS // TOK_DEV)
    expert_ids = jax.vmap(lambda own, number: deal_out(jax.random.fold_in(keys[2], 2), own, number, TOK_DEV, EXPERTS, TOP_K, CAP, 2))(expert_ids_keys, expert_ids_turns).reshape((TOKENS, TOP_K))
    route_weights = jnp.clip(jnp.exp(math.log(1.0) - 2.3025851 * jax.random.uniform(keys[3], (TOKENS, TOP_K), jnp.float32) ** level_of(keys[3], (TOKENS, TOP_K), ((0, 8),), -0.2, 0.2)), 0.1, 1.0)
    expert_gate = bell_draw(keys[4], (2 * EXPERTS, D, EXP_HALF), D ** -0.5, 0.125, ((0, 32),))
    expert_up = bell_draw(keys[5], (2 * EXPERTS, D, EXP_HALF), D ** -0.5, 0.125, ((0, 32),))
    expert_down = bell_draw(keys[6], (2 * EXPERTS, EXP_HALF, D), EXPERT_FF ** -0.5, 0.25, ((0, 32),))
    shared_gate = bell_draw(keys[7], (D, SHARED_FF), D ** -0.5, 0.125, ((1, 4),))
    shared_up = bell_draw(keys[8], (D, SHARED_FF), D ** -0.5, 0.125, ((1, 4),))
    shared_down = bell_draw(keys[9], (SHARED_FF, D), SHARED_FF ** -0.5, 0.25, ((1, 4),))
    return {"tokens": tokens, "norm_gain": norm_gain, "expert_ids": expert_ids, "route_weights": route_weights, "expert_gate": expert_gate, "expert_up": expert_up, "expert_down": expert_down, "shared_gate": shared_gate, "shared_up": shared_up, "shared_down": shared_down}


NORM_EPSILON = 1e-06

def rms_normed(tokens, norm_gain):
    as_float = tokens.astype(jnp.float32)
    inverse_rms = lax.rsqrt(lax.optimization_barrier(jnp.mean(as_float * as_float, axis=-1, keepdims=True)) + NORM_EPSILON)
    return (as_float * inverse_rms * norm_gain).astype(jnp.bfloat16)

def slot_numbers(expert_ids, block_rows, expert_count):
    expert_iota = jnp.arange(expert_count, dtype=jnp.int32)
    counts = lax.optimization_barrier(jnp.sum((expert_ids[:, :, None] == expert_iota[None, None, :]).astype(jnp.int32), axis=1))
    blocked = counts.reshape(-1, block_rows, expert_count)
    prefix = (jnp.cumsum(blocked, axis=1) - blocked).reshape(counts.shape)
    return jnp.take_along_axis(prefix, expert_ids, axis=1).astype(jnp.int32)

def half_output(gathered, gate_half, up_half, down_half):
    hidden = (jax.nn.silu(jnp.dot(gathered, gate_half, preferred_element_type=jnp.float32)) * jnp.dot(gathered, up_half, preferred_element_type=jnp.float32)).astype(jnp.bfloat16)
    rounded = jnp.dot(hidden, down_half, preferred_element_type=jnp.float32).astype(jnp.bfloat16)
    return lax.optimization_barrier(rounded).astype(jnp.float32)

def reference(tokens, norm_gain, expert_ids, route_weights, expert_gate, expert_up, expert_down, shared_gate, shared_up, shared_down):
    normed = rms_normed(tokens, norm_gain)
    token_count, model_width = tokens.shape
    block_rows = token_count // N_EP
    slot_index = slot_numbers(expert_ids, block_rows, EXPERTS)
    token_iota = jnp.arange(token_count, dtype=jnp.int32)
    source_block = jnp.broadcast_to((token_iota // block_rows)[:, None], expert_ids.shape).astype(jnp.int32)
    token_rows = jnp.broadcast_to(token_iota[:, None], expert_ids.shape).astype(jnp.int32)
    token_table = jnp.full((EXPERTS, N_EP, CAP), token_count, jnp.int32)
    token_table = token_table.at[expert_ids, source_block, slot_index].set(token_rows)
    weight_table = jnp.zeros((EXPERTS, N_EP, CAP), jnp.float32)
    weight_table = weight_table.at[expert_ids, source_block, slot_index].set(route_weights)
    padded = jnp.concatenate([normed, jnp.zeros((1, model_width), jnp.bfloat16)], axis=0)
    gate_pairs = expert_gate.reshape(EXPERTS, 2, model_width, EXP_HALF)
    up_pairs = expert_up.reshape(EXPERTS, 2, model_width, EXP_HALF)
    down_pairs = expert_down.reshape(EXPERTS, 2, EXP_HALF, model_width)

    def expert_step(running, inputs):
        gate_two, up_two, down_two, table_rows, table_weights = inputs
        flat_tokens = table_rows.reshape(-1)
        gathered = padded[flat_tokens]
        first = half_output(gathered, gate_two[0], up_two[0], down_two[0])
        second = half_output(gathered, gate_two[1], up_two[1], down_two[1])
        output = (first + second).astype(jnp.bfloat16)
        running = running.at[flat_tokens].add(output.astype(jnp.float32) * table_weights.reshape(-1)[:, None])
        return (running, None)
    start = jnp.zeros((token_count + 1, model_width), jnp.float32)
    routed, _ = lax.scan(expert_step, start, (gate_pairs, up_pairs, down_pairs, token_table, weight_table))
    shared_act = (jax.nn.silu(jnp.dot(normed, shared_gate, preferred_element_type=jnp.float32)) * jnp.dot(normed, shared_up, preferred_element_type=jnp.float32)).astype(jnp.bfloat16)
    shared_out = jnp.dot(shared_act, shared_down, preferred_element_type=jnp.float32)
    return (routed[:token_count] + shared_out).astype(jnp.bfloat16)
```

```python
import functools

import jax
import jax.numpy as jnp
from jax import lax
from jax.experimental import pallas as pl
from jax.experimental.pallas import tpu as pltpu
from jax.sharding import PartitionSpec as P

NORM_EPSILON = 1e-06


def swapped(block, axis, distance):
    count = lax.axis_size(axis)
    route = []
    for low in range(count):
        high = low | 1 << distance
        if high != low and high < count:
            route += [(low, high), (high, low)]
    return lax.ppermute(block, axis, route)


def routed_exchange(
    tokens,
    norm_gain,
    expert_ids,
    route_weights,
    expert_gate,
    expert_up,
    expert_down,
    shared_gate,
    shared_up,
    shared_down,
):
    ep_count = lax.axis_size("ep")
    tp_count = lax.axis_size("tp")
    pair_count = tp_count // 2
    tp_index = lax.axis_index("tp")
    column = tp_index // 2
    half_index = tp_index % 2
    token_count, model_width = tokens.shape
    top_count = expert_ids.shape[1]
    expert_count = ep_count * pair_count
    capacity = 2 * max(1, token_count * top_count // expert_count)
    half_cap = capacity // 2
    as_float = tokens.astype(jnp.float32)
    inverse_rms = lax.rsqrt(jnp.mean(as_float * as_float, axis=-1, keepdims=True) + NORM_EPSILON)
    normed = (as_float * inverse_rms * norm_gain).astype(jnp.bfloat16)
    expert_iota = jnp.arange(expert_count, dtype=jnp.int32)
    token_iota = jnp.arange(token_count, dtype=jnp.int32)
    counts = jnp.sum(
        (expert_ids[:, :, None] == expert_iota[None, None, :]).astype(jnp.bfloat16), axis=1
    )
    strict_lower = (token_iota[:, None] > token_iota[None, :]).astype(jnp.bfloat16)
    prefix = jnp.dot(strict_lower, counts, preferred_element_type=jnp.float32)
    slot_index = jnp.take_along_axis(prefix, expert_ids, axis=1).astype(jnp.int32)
    target = expert_ids // pair_count
    owner_column = expert_ids % pair_count
    is_mine = owner_column == column
    position = target * capacity + slot_index
    slot_iota = jnp.arange(ep_count * capacity, dtype=jnp.int32)
    matches = is_mine[None, :, :] & (position[None, :, :] == slot_iota[:, None, None])
    slot_taken = jnp.any(matches, axis=2)
    token_of_slot = jnp.sum(jnp.where(slot_taken, token_iota[None, :], 0), axis=1)
    filled = jnp.any(slot_taken, axis=1)
    buffer = jnp.where(
        filled[:, None], jnp.take(normed, token_of_slot, axis=0), jnp.zeros((), jnp.bfloat16)
    )
    buffer = buffer.reshape(ep_count, capacity, model_width)
    gate_local = expert_gate[0]
    up_local = expert_up[0]
    down_local = expert_down[0]
    received = lax.all_to_all(buffer, "ep", split_axis=0, concat_axis=0, tiled=True)
    flat_rows = received.reshape(-1, model_width)
    hidden = (
        jax.nn.silu(jnp.dot(flat_rows, gate_local, preferred_element_type=jnp.float32))
        * jnp.dot(flat_rows, up_local, preferred_element_type=jnp.float32)
    ).astype(jnp.bfloat16)
    partial_out = jnp.dot(hidden, down_local, preferred_element_type=jnp.float32).astype(
        jnp.bfloat16
    )
    partial_out = partial_out.reshape(received.shape[0], received.shape[1], model_width)
    kept_part = lax.dynamic_slice_in_dim(partial_out, half_index * half_cap, half_cap, 1)
    other_part = lax.dynamic_slice_in_dim(partial_out, (1 - half_index) * half_cap, half_cap, 1)
    partner_part = swapped(other_part, "tp", 0)
    expert_out = (kept_part.astype(jnp.float32) + partner_part.astype(jnp.float32)).astype(
        jnp.bfloat16
    )
    returned = lax.all_to_all(expert_out, "ep", split_axis=0, concat_axis=0, tiled=True)
    row_total = ep_count * half_cap
    flat_rows = returned.reshape(row_total, model_width).astype(jnp.float32)
    is_valid = is_mine & (slot_index // half_cap == half_index)
    row_index = jnp.where(is_valid, target * half_cap + slot_index % half_cap, -1)
    row_iota = jnp.arange(row_total, dtype=jnp.int32)
    hits = row_index[:, :, None] == row_iota[None, None, :]
    combine_table = jnp.sum(jnp.where(hits, route_weights[:, :, None], 0.0), axis=1)
    partial_routed = jnp.dot(
        combine_table,
        flat_rows,
        precision=lax.Precision.HIGHEST,
        preferred_element_type=jnp.float32,
    )
    routed = lax.psum_scatter(partial_routed, "tp", scatter_dimension=1, tiled=True)
    shared_act = (
        jax.nn.silu(jnp.dot(normed, shared_gate, preferred_element_type=jnp.float32))
        * jnp.dot(normed, shared_up, preferred_element_type=jnp.float32)
    ).astype(jnp.bfloat16)
    shared_out = jnp.dot(
        lax.all_gather(shared_act, "tp", axis=1, tiled=True),
        shared_down,
        preferred_element_type=jnp.float32,
    )
    return (routed + shared_out).astype(jnp.bfloat16)


MESH = pl.DeviceIdType.MESH
LANES = 128
KEEP = 6
NEAR = 6
TURN = 2
LAG = 2


def silu(v):
    return v / (1.0 + jnp.exp(-v))


def dense_kernel(
    ep_count, tp_count, minor, near, keep, lag, turn,
    ids_ref, rw_ref, gain_ref, tok_hbm, gate_hbm, up_hbm, down_hbm, sg_hbm, su_hbm, sd_hbm,
    out_ref,
    tok, xb, xo, wtab, wr, wg, wu, wd, sg, su, sd, sh_all, sh_out,
    pa, pb, xs, xr, ys, yr, zas, zar, zbs, zbr, fs, fr, fin, fin_in, acc_a, acc_b,
    load_sem, wt_s, wt_r, we_s, we_r, sh_s, sh_r, yb_s,
    au_s, ad_s, a_r, bu_s, bd_s, b_r, ya_s, ya_r, xa_s, xa_r,
    rx_s, rx_r, ry_s, ry_r, rza_s, rza_r, rzb_s, rzb_r, f_s, f_r, o_s, o_r,
):
    n = ep_count
    major = n // minor
    half, width = xo.shape
    side = width // 2
    quarter = width // tp_count
    tail = side - keep
    e = lax.axis_index("ep")
    t = lax.axis_index("tp")
    z = e // minor
    y = e % minor
    xi = t // 2
    c = t % 2
    t2 = 2 * (1 - xi) + c
    other_y = z * minor + 1 - y
    mate_x = {"tp": t2}
    mate_c = {"tp": 2 * xi + 1 - c}
    mate_y = {"ep": other_y}
    across = {"ep": other_y, "tp": t2}
    z_up = {"ep": lax.rem(e + minor, n)}
    z_down = {"ep": lax.rem(e + n - minor, n)}
    is_end = (z == 0) | (z == major - 1)

    barrier = pltpu.get_barrier_semaphore()
    for k in range(1, n):
        pl.semaphore_signal(barrier, inc=1, device_id={"ep": lax.rem(e + k, n)}, device_id_type=MESH)
    for k in range(1, tp_count):
        pl.semaphore_signal(barrier, inc=1, device_id={"tp": lax.rem(t + k, tp_count)}, device_id_type=MESH)
    pl.semaphore_signal(barrier, inc=1, device_id=across, device_id_type=MESH)

    def remote(src, dst, s, r, who):
        return pltpu.make_async_remote_copy(
            src_ref=src, dst_ref=dst, send_sem=s, recv_sem=r, device_id=who, device_id_type=MESH
        )

    def rows_of(which):
        return pl.ds(pl.multiple_of(which * half, half), half)

    def side_of(which):
        return pl.ds(pl.multiple_of(which * side, side), side)

    loads = [
        pltpu.make_async_copy(a, b, load_sem.at[i])
        for i, (a, b) in enumerate(
            (
                (tok_hbm.at[rows_of(c)], tok.at[0]),
                (tok_hbm.at[rows_of(1 - c)], tok.at[1]),
                (gate_hbm, wg.at[c]),
                (up_hbm, wu.at[c]),
                (down_hbm.at[:, side_of(xi)], wd.at[c, :, pl.ds(0, side)]),
                (down_hbm.at[:, side_of(1 - xi)], wd.at[c, :, pl.ds(side, side)]),
                (sg_hbm, sg),
                (su_hbm, su),
                (sd_hbm, sd),
            )
        )
    ]
    for load in loads:
        load.start()

    step = 16

    def norm_into(which, store):
        def body(i, carry):
            part = pl.ds(pl.multiple_of(i * step, step), step)
            v = tok[which, part, :].astype(jnp.float32)
            r = lax.rsqrt(jnp.mean(v * v, axis=-1, keepdims=True) + NORM_EPSILON)
            store(part, (v * r * gain_ref[...]).astype(jnp.bfloat16))
            return carry

        lax.fori_loop(0, half // step, body, 0)

    def store_own(part, value):
        xb[e, part, :] = value

    def store_rest(part, value):
        xo[part, :] = value

    def weights_for(expert):
        row = jnp.zeros((1, ids_ref.shape[1]), jnp.float32)
        for k in range(ids_ref.shape[0]):
            row += jnp.where(ids_ref[k : k + 1, :] == expert, rw_ref[k : k + 1, :], 0.0)
        return row

    loads[0].wait()
    norm_into(0, store_own)
    for d in range(n):
        wtab[d] = weights_for(d * (tp_count // 2) + xi)
    wr[e] = weights_for(e * (tp_count // 2) + xi)
    pl.semaphore_wait(barrier, n + tp_count - 1)

    mine = pl.ds(pl.multiple_of(xi * near, LANES), near)
    theirs = pl.ds(pl.multiple_of((1 - xi) * near, LANES), near)
    rest = pl.ds(2 * near, width - 2 * near)

    def line_a(g, s, who):
        ref = xb.at[g, :, mine]
        return remote(ref, ref, s.at[g], a_r.at[g], who)

    def line_b(g, s, who):
        ref = xb.at[g, :, rest]
        return remote(ref, ref, s.at[g], b_r.at[g], who)

    def y_first():
        ref = xb.at[e, :, rest]
        return remote(ref, ref, yb_s, b_r.at[e], mate_y)

    def y_copy(g):
        ref = xb.at[g, :, mine]
        return remote(ref, ref, ya_s.at[g], ya_r.at[g], mate_y)

    def x_copy(g):
        ref = xb.at[g, :, mine]
        return remote(ref, ref, xa_s.at[g], xa_r.at[g], mate_x)

    def x_arrival(g):
        ref = xb.at[g, :, theirs]
        return remote(ref, ref, xa_s.at[g], xa_r.at[g], mate_x)

    def wt_copy(k, target):
        return remote(wtab.at[target], wr.at[e], wt_s.at[k], wt_r.at[e], {"ep": target})

    def wt_arrival(g):
        return remote(wtab.at[g], wr.at[g], wt_s.at[0], wt_r.at[g], mate_y)

    def weight_copy(i, which):
        ref = (wg, wu, wd)[i].at[which]
        return remote(ref, ref, we_s.at[i], we_r.at[i], mate_c)

    def sh_copy(k, slot, who):
        return remote(sh_all.at[slot], sh_all.at[slot], sh_s.at[k], sh_r.at[k], {"tp": who})

    def order(j):
        k = jnp.minimum(z, major - 1 - z)
        d = (j + 1) // 2
        close = jnp.where(j % 2 == 1, z - d, z + d)
        far = jnp.where(z <= major - 1 - z, j, major - 1 - j)
        return jnp.where(j <= 2 * k, close, far)

    def slot_group(i):
        p = order(i // 2)
        yy = jnp.where(i % 2 == 0, y, 1 - y)
        return p, p * minor + yy

    def ups(p):
        return (p <= z) & (z < major - 1)

    def downs(p):
        return (p >= z) & (z > 0)

    def forward(p, g, line, s_up, s_down):
        @pl.when(ups(p))
        def _():
            line(g, s_up, z_up).start()

        @pl.when(downs(p))
        def _():
            line(g, s_down, z_down).start()

    forward(z, e, line_a, au_s, ad_s)
    y_first().start()
    y_copy(e).start()
    forward(z, e, line_b, bu_s, bd_s)
    for k in range(1, n):
        wt_copy(k, lax.rem(e + k, n)).start()
    loads[2].wait()
    weight_copy(0, c).start()
    loads[3].wait()
    weight_copy(1, c).start()
    loads[4].wait()
    loads[5].wait()
    weight_copy(2, c).start()
    loads[1].wait()
    norm_into(1, store_rest)
    loads[6].wait()
    loads[7].wait()

    def shared_in(x):
        g_sum = jnp.dot(x, sg[...], preferred_element_type=jnp.float32)
        u_sum = jnp.dot(x, su[...], preferred_element_type=jnp.float32)
        return (silu(g_sum) * u_sum).astype(jnp.bfloat16)

    sh_all[t, c] = shared_in(xb[e])
    sh_all[t, 1 - c] = shared_in(xo[...])
    for k in range(1, tp_count):
        sh_copy(k, t, lax.rem(t + k, tp_count)).start()

    def rx_copy(g):
        return remote(xs.at[g], xr.at[g], rx_s.at[g], rx_r.at[g], mate_x)

    def ry_copy(p):
        return remote(ys.at[p], yr.at[p], ry_s.at[p], ry_r.at[p], mate_y)

    def rza_copy(p, lane, who):
        return remote(zas.at[p], zar.at[lane, p], rza_s.at[p], rza_r.at[lane, p], who)

    def rzb_copy(g, lane, who):
        return remote(zbs.at[g], zbr.at[lane, g], rzb_s.at[g], rzb_r.at[lane, g], who)

    diagonal = lax.broadcasted_iota(jnp.int32, (half, 2 * half), 1) == (
        lax.broadcasted_iota(jnp.int32, (half, 2 * half), 0) + c * half
    )

    def compute(g):
        weight = jnp.sum(jnp.where(diagonal, wr[g], 0.0), axis=1, keepdims=True)
        x = xb[g]
        acts = []
        for h in range(2):
            g_sum = jnp.dot(x, wg[h], preferred_element_type=jnp.float32)
            u_sum = jnp.dot(x, wu[h], preferred_element_type=jnp.float32)
            acts.append((silu(g_sum) * u_sum).astype(jnp.bfloat16))

        def columns(low, high):
            total = jnp.dot(acts[0], wd[0, :, low:high], preferred_element_type=jnp.float32)
            total += jnp.dot(acts[1], wd[1, :, low:high], preferred_element_type=jnp.float32)
            return total * weight

        xs[g] = columns(side, side + keep).astype(jnp.bfloat16)
        rx_copy(g).start()
        pa[g] = columns(0, keep)
        pb[g, :, :tail] = columns(keep, side)
        pb[g, :, tail:] = columns(side + keep, width)

    def sum_b(p, g):
        acc_b[...] = pb[g]

        @pl.when(downs(p))
        def _():
            rzb_copy(g, 0, z_up).wait_recv()
            acc_b[...] += zbr[0, g].astype(jnp.float32)

        @pl.when(ups(p))
        def _():
            rzb_copy(g, 1, z_up).wait_recv()
            acc_b[...] += zbr[1, g].astype(jnp.float32)

    def sum_a(p, g):
        rx_copy(g).wait_recv()
        ry_copy(p).wait_recv()
        acc_a[...] = pa[g] + xr[g].astype(jnp.float32) + yr[p].astype(jnp.float32)

        @pl.when(downs(p))
        def _():
            rza_copy(p, 0, z_up).wait_recv()
            acc_a[...] += zar[0, p].astype(jnp.float32)

        @pl.when(ups(p))
        def _():
            rza_copy(p, 1, z_up).wait_recv()
            acc_a[...] += zar[1, p].astype(jnp.float32)

    def line_sums(p):
        def send(copy, key):
            @pl.when(p > z)
            def _():
                copy(key, 0, z_up).start()

            @pl.when(p < z)
            def _():
                copy(key, 1, z_down).start()

        for yy in (1 - y, y):
            g = p * minor + yy
            sum_b(p, g)
            zbs[g] = acc_b[...].astype(jnp.bfloat16)
            send(rzb_copy, g)
        sum_a(p, p * minor + y)
        zas[p] = acc_a[...].astype(jnp.bfloat16)
        send(rza_copy, p)

    def main_step(i, carry):
        @pl.when((i >= 1) & (i < n))
        def _():
            p, g = slot_group(i)

            @pl.when(i % 2 == 0)
            def _():
                line_a(g, au_s, z_up).wait_recv()
                forward(p, g, line_a, au_s, ad_s)
                y_copy(g).start()
                x_copy(g).start()

            line_b(g, bu_s, z_up).wait_recv()
            forward(p, g, line_b, bu_s, bd_s)

        @pl.when((i >= 2) & (i <= n) & (i % 2 == 0))
        def _():
            _, g = slot_group(i - 1)
            y_copy(g).wait_recv()
            x_copy(g).start()

        @pl.when(i == lag)
        def _():
            for j in range(3):
                weight_copy(j, 1 - c).wait_recv()

        @pl.when((i >= lag) & (i < n + lag))
        def _():
            _, g = slot_group(i - lag)

            @pl.when(i > lag)
            def _():
                x_arrival(g).wait_recv()
                wt_arrival(g).wait_recv()

            compute(g)

        @pl.when(i == n)
        def _():
            loads[8].wait()
            for k in range(1, tp_count):
                sh_copy(k, lax.rem(t + tp_count - k, tp_count), t).wait_recv()
            share = sg.shape[1]
            for r in range(2):
                shared = jnp.zeros((half, quarter), jnp.float32)
                for q in range(tp_count):
                    shared += jnp.dot(
                        sh_all[q, r], sd[q * share : (q + 1) * share, :],
                        preferred_element_type=jnp.float32,
                    )
                sh_out[r] = shared

        @pl.when((i >= lag + turn + 1) & (i < n + lag + turn) & ((i - lag - turn) % 2 == 1))
        def _():
            p, g = slot_group(i - lag - turn)
            rx_copy(g).wait_recv()
            ys[p] = (pa[g] + xr[g].astype(jnp.float32)).astype(jnp.bfloat16)
            ry_copy(p).start()

        @pl.when(is_end & (i >= lag + turn + 4) & ((i - lag - turn) % 2 == 0))
        def _():
            line_sums(order((i - lag - turn - 2) // 2))

        return carry

    lax.fori_loop(0, n + lag + turn + 1, main_step, 0)

    @pl.when(jnp.logical_not(is_end))
    def _():
        def sum_step(q, carry):
            above = major - 1 - z
            low = jnp.where(q < above, z + 1 + q, z - 1 - (q - above))
            high = jnp.where(q < z, z - 1 - q, z + 1 + (q - z))
            line_sums(jnp.where(2 * z < major, low, high))
            return carry

        lax.fori_loop(0, major - 1, sum_step, 0)

    def last_copy(i):
        return remote(fs.at[i], fr.at[i], f_s.at[i], f_r.at[i], (mate_y, across, mate_x)[i])

    sum_b(z, other_y)
    fs[0] = acc_b[:, :tail].astype(jnp.bfloat16)
    fs[1] = acc_b[:, tail:].astype(jnp.bfloat16)
    last_copy(0).start()
    last_copy(1).start()
    sum_b(z, e)
    fs[2] = acc_b[:, tail:].astype(jnp.bfloat16)
    last_copy(2).start()
    sum_a(z, e)

    def place(low, value):
        for q in range(2):
            start, stop = max(low, q * quarter), min(low + value.shape[1], (q + 1) * quarter)
            if start < stop:
                fin[q, :, start - q * quarter : stop - q * quarter] = value[:, start - low : stop - low]

    place(0, acc_a[...])
    for i in range(3):
        last_copy(i).wait_recv()
    place(
        keep,
        acc_b[:, :tail] + fr[0].astype(jnp.float32) + fr[1].astype(jnp.float32) + fr[2].astype(jnp.float32),
    )
    swap = remote(fin.at[1 - c], fin_in, o_s, o_r, mate_c)
    swap.start()
    out_ref[rows_of(c), :] = (fin[c] + sh_out[c]).astype(jnp.bfloat16)
    swap.wait_recv()
    out_ref[rows_of(1 - c), :] = (fin_in[...] + sh_out[1 - c]).astype(jnp.bfloat16)

    swap.wait_send()
    for i in range(3):
        last_copy(i).wait_send()
        weight_copy(i, c).wait_send()
    y_first().wait_send()
    for k in range(1, n):
        wt_copy(k, lax.rem(e + k, n)).wait_send()
    for k in range(1, tp_count):
        sh_copy(k, t, lax.rem(t + k, tp_count)).wait_send()

    def drain(i, carry):
        p, g = slot_group(i)

        def sent(line, s_up, s_down):
            @pl.when(ups(p))
            def _():
                line(g, s_up, z_up).wait_send()

            @pl.when(downs(p))
            def _():
                line(g, s_down, z_down).wait_send()

        sent(line_b, bu_s, bd_s)

        @pl.when(i % 2 == 0)
        def _():
            sent(line_a, au_s, ad_s)
            y_copy(g).wait_send()

            @pl.when(p != z)
            def _():
                rza_copy(p, 0, z_up).wait_send()

        @pl.when(i % 2 == 1)
        def _():
            ry_copy(p).wait_send()

        @pl.when(i > 0)
        def _():
            x_copy(g).wait_send()

        rx_copy(g).wait_send()

        @pl.when(p != z)
        def _():
            rzb_copy(g, 0, z_up).wait_send()

        return carry

    lax.fori_loop(0, n, drain, 0)


def dense_exchange(
    tokens, norm_gain, expert_ids, route_weights, expert_gate, expert_up, expert_down,
    shared_gate, shared_up, shared_down,
):
    n = lax.axis_size("ep")
    tp_count = lax.axis_size("tp")
    minor = 1 << (n.bit_length() - 1) // 2
    major = n // minor
    rows, width = tokens.shape
    half = rows // 2
    side = width // 2
    quarter = width // tp_count
    near = side * NEAR // 8 // LANES * LANES
    keep = side * KEEP // 8 // LANES * LANES
    tail = side - keep
    ff = expert_gate.shape[2]
    share = shared_gate.shape[1]
    bf16, f32 = jnp.bfloat16, jnp.float32
    dma = pltpu.SemaphoreType.DMA
    vmem = pl.BlockSpec(memory_space=pltpu.VMEM)
    anywhere = pl.BlockSpec(memory_space=pl.ANY)
    return pl.pallas_call(
        functools.partial(dense_kernel, n, tp_count, minor, near, keep, LAG, TURN),
        out_shape=jax.ShapeDtypeStruct((rows, quarter), bf16),
        in_specs=[vmem] * 3 + [anywhere] * 7,
        out_specs=vmem,
        scratch_shapes=[
            pltpu.VMEM((2, half, width), bf16),
            pltpu.VMEM((n, half, width), bf16),
            pltpu.VMEM((half, width), bf16),
            pltpu.VMEM((n, 1, rows), f32),
            pltpu.VMEM((n, 1, rows), f32),
            pltpu.VMEM((2, width, ff), bf16),
            pltpu.VMEM((2, width, ff), bf16),
            pltpu.VMEM((2, ff, width), bf16),
            pltpu.VMEM((width, share), bf16),
            pltpu.VMEM((width, share), bf16),
            pltpu.VMEM((share * tp_count, quarter), bf16),
            pltpu.VMEM((tp_count, 2, half, share), bf16),
            pltpu.VMEM((2, half, quarter), f32),
            pltpu.VMEM((n, half, keep), f32),
            pltpu.VMEM((n, half, 2 * tail), f32),
            pltpu.VMEM((n, half, keep), bf16),
            pltpu.VMEM((n, half, keep), bf16),
            pltpu.VMEM((major, half, keep), bf16),
            pltpu.VMEM((major, half, keep), bf16),
            pltpu.VMEM((major, half, keep), bf16),
            pltpu.VMEM((2, major, half, keep), bf16),
            pltpu.VMEM((n, half, 2 * tail), bf16),
            pltpu.VMEM((2, n, half, 2 * tail), bf16),
            pltpu.VMEM((3, half, tail), bf16),
            pltpu.VMEM((3, half, tail), bf16),
            pltpu.VMEM((2, half, quarter), f32),
            pltpu.VMEM((half, quarter), f32),
            pltpu.VMEM((half, keep), f32),
            pltpu.VMEM((half, 2 * tail), f32),
            dma((9,)), dma((n,)), dma((n,)), dma((3,)), dma((3,)), dma((tp_count,)), dma((tp_count,)), dma,
            dma((n,)), dma((n,)), dma((n,)), dma((n,)), dma((n,)), dma((n,)),
            dma((n,)), dma((n,)), dma((n,)), dma((n,)),
            dma((n,)), dma((n,)), dma((major,)), dma((major,)),
            dma((major,)), dma((2, major)), dma((n,)), dma((2, n)), dma((3,)), dma((3,)), dma, dma,
        ],
        compiler_params=pltpu.CompilerParams(
            collective_id=0, has_side_effects=True, vmem_limit_bytes=60 << 20
        ),
        name="dense_moe",
    )(
        expert_ids.T, route_weights.T, norm_gain.reshape(1, width), tokens,
        expert_gate[0], expert_up[0], expert_down[0],
        shared_gate, shared_up, shared_down,
    )


def local(tokens, *rest):
    ep_count = lax.axis_size("ep")
    pair_count = lax.axis_size("tp") // 2
    dense_bytes = 4 * ep_count * tokens.size * tokens.dtype.itemsize
    minor = 1 << (ep_count.bit_length() - 1) // 2
    if pair_count == 2 and minor == 2 and dense_bytes <= 24 << 20:
        return dense_exchange(tokens, *rest)
    return routed_exchange(tokens, *rest)


def solution(mesh):
    return jax.shard_map(
        local,
        mesh=mesh,
        in_specs=(
            P("ep", None),
            P(),
            P("ep", None),
            P("ep", None),
            P(("ep", "tp"), None, None),
            P(("ep", "tp"), None, None),
            P(("ep", "tp"), None, None),
            P(None, "tp"),
            P(None, "tp"),
            P(None, "tp"),
        ),
        out_specs=P("ep", "tp"),
        check_vma=False,
    )
```

```python
import functools

import jax
import jax.numpy as jnp
from jax import lax
from jax.experimental import pallas as pl
from jax.experimental.pallas import tpu as pltpu
from jax.sharding import PartitionSpec as P

NORM_EPSILON = 1e-06


def swapped(block, axis, distance):
    count = lax.axis_size(axis)
    route = []
    for low in range(count):
        high = low | 1 << distance
        if high != low and high < count:
            route += [(low, high), (high, low)]
    return lax.ppermute(block, axis, route)


def routed_exchange(
    tokens,
    norm_gain,
    expert_ids,
    route_weights,
    expert_gate,
    expert_up,
    expert_down,
    shared_gate,
    shared_up,
    shared_down,
):
    ep_count = lax.axis_size("ep")
    tp_count = lax.axis_size("tp")
    pair_count = tp_count // 2
    tp_index = lax.axis_index("tp")
    column = tp_index // 2
    half_index = tp_index % 2
    token_count, model_width = tokens.shape
    top_count = expert_ids.shape[1]
    expert_count = ep_count * pair_count
    capacity = 2 * max(1, token_count * top_count // expert_count)
    half_cap = capacity // 2
    as_float = tokens.astype(jnp.float32)
    inverse_rms = lax.rsqrt(jnp.mean(as_float * as_float, axis=-1, keepdims=True) + NORM_EPSILON)
    normed = (as_float * inverse_rms * norm_gain).astype(jnp.bfloat16)
    expert_iota = jnp.arange(expert_count, dtype=jnp.int32)
    token_iota = jnp.arange(token_count, dtype=jnp.int32)
    counts = jnp.sum(
        (expert_ids[:, :, None] == expert_iota[None, None, :]).astype(jnp.bfloat16), axis=1
    )
    strict_lower = (token_iota[:, None] > token_iota[None, :]).astype(jnp.bfloat16)
    prefix = jnp.dot(strict_lower, counts, preferred_element_type=jnp.float32)
    slot_index = jnp.take_along_axis(prefix, expert_ids, axis=1).astype(jnp.int32)
    target = expert_ids // pair_count
    owner_column = expert_ids % pair_count
    is_mine = owner_column == column
    position = target * capacity + slot_index
    slot_iota = jnp.arange(ep_count * capacity, dtype=jnp.int32)
    matches = is_mine[None, :, :] & (position[None, :, :] == slot_iota[:, None, None])
    slot_taken = jnp.any(matches, axis=2)
    token_of_slot = jnp.sum(jnp.where(slot_taken, token_iota[None, :], 0), axis=1)
    filled = jnp.any(slot_taken, axis=1)
    buffer = jnp.where(
        filled[:, None], jnp.take(normed, token_of_slot, axis=0), jnp.zeros((), jnp.bfloat16)
    )
    buffer = buffer.reshape(ep_count, capacity, model_width)
    gate_local = expert_gate[0]
    up_local = expert_up[0]
    down_local = expert_down[0]
    received = lax.all_to_all(buffer, "ep", split_axis=0, concat_axis=0, tiled=True)
    flat_rows = received.reshape(-1, model_width)
    hidden = (
        jax.nn.silu(jnp.dot(flat_rows, gate_local, preferred_element_type=jnp.float32))
        * jnp.dot(flat_rows, up_local, preferred_element_type=jnp.float32)
    ).astype(jnp.bfloat16)
    partial_out = jnp.dot(hidden, down_local, preferred_element_type=jnp.float32).astype(
        jnp.bfloat16
    )
    partial_out = partial_out.reshape(received.shape[0], received.shape[1], model_width)
    kept_part = lax.dynamic_slice_in_dim(partial_out, half_index * half_cap, half_cap, 1)
    other_part = lax.dynamic_slice_in_dim(partial_out, (1 - half_index) * half_cap, half_cap, 1)
    partner_part = swapped(other_part, "tp", 0)
    expert_out = (kept_part.astype(jnp.float32) + partner_part.astype(jnp.float32)).astype(
        jnp.bfloat16
    )
    returned = lax.all_to_all(expert_out, "ep", split_axis=0, concat_axis=0, tiled=True)
    row_total = ep_count * half_cap
    flat_rows = returned.reshape(row_total, model_width).astype(jnp.float32)
    is_valid = is_mine & (slot_index // half_cap == half_index)
    row_index = jnp.where(is_valid, target * half_cap + slot_index % half_cap, -1)
    row_iota = jnp.arange(row_total, dtype=jnp.int32)
    hits = row_index[:, :, None] == row_iota[None, None, :]
    combine_table = jnp.sum(jnp.where(hits, route_weights[:, :, None], 0.0), axis=1)
    partial_routed = jnp.dot(
        combine_table,
        flat_rows,
        precision=lax.Precision.HIGHEST,
        preferred_element_type=jnp.float32,
    )
    routed = lax.psum_scatter(partial_routed, "tp", scatter_dimension=1, tiled=True)
    shared_act = (
        jax.nn.silu(jnp.dot(normed, shared_gate, preferred_element_type=jnp.float32))
        * jnp.dot(normed, shared_up, preferred_element_type=jnp.float32)
    ).astype(jnp.bfloat16)
    shared_out = jnp.dot(
        lax.all_gather(shared_act, "tp", axis=1, tiled=True),
        shared_down,
        preferred_element_type=jnp.float32,
    )
    return (routed + shared_out).astype(jnp.bfloat16)


MESH = pl.DeviceIdType.MESH
LANES = 128
BOTH_KEEP = 2
KEEP = 4
WIDE = 2
NEAR = 4


def silu(v):
    return v / (1.0 + jnp.exp(-v))


KINDS = ("a", "c", "b", "x", "k", "t", "r", "s", "zb", "zc", "za")
OUTER = [
    ("b", 1), ("a", 2), ("x", 1), ("c", 2), ("b", 2), ("k", 0), ("b", 3), ("x", 3), ("a", 4), ("c", 4), ("k", 1, 2), ("b", 4), ("b", 5),
    ("x", 5), ("a", 6), ("c", 6), ("k", 3, 4), ("b", 6), ("zb", 0), ("b", 7), ("x", 7), ("k", 5, 6), ("zb", 1), ("r", 3), ("zc", 0),
    ("za", 0), ("s", 0), ("k", 7), ("zb", 2), ("t", 0), ("t", 1), ("zc", 1), ("zc", 2), ("r", 5), ("za", 1), ("r", 7), ("za", 2), ("r", 1),
]
INNER = [
    ("b", 1), ("a", 2), ("a", 4), ("x", 1), ("c", 2), ("c", 4), ("b", 2), ("b", 4), ("b", 3), ("b", 5), ("k", 0), ("x", 3), ("x", 5), ("a", 6),
    ("k", 2, 4), ("c", 6), ("b", 6), ("b", 7), ("k", 1, 3), ("x", 7), ("k", 5, 6), ("k", 7), ("t", 0), ("t", 1), ("s", 0),
    ("r", 3), ("r", 5), ("zb", 0), ("zc", 0), ("r", 7), ("za", 0), ("zb", 1), ("zc", 1), ("za", 1), ("r", 1), ("zb", 2), ("zc", 2), ("za", 2),
]


def plans_for(n):
    return OUTER, INNER


def dense_kernel(
    ep_count, tp_count, minor, near, wide, keep, both_keep, plans,
    ids_hbm, rw_hbm, gain_hbm, tok_hbm, gate_hbm, up_hbm, down_hbm, sg_hbm, su_hbm, sd_hbm,
    out_ref,
    ids_ref, rw_ref, gain_ref, tok, xb, xo, wtab, wr, wg, wu, wd, sg, su, sd, sh_all, sh_out,
    pa, pb, pc, xs, xr, ys, yr, ycs, ycr, zas, zar, zbs, zbr, zcs, zcr, fs, fr, gs, gr, fin, fin_in, acc_a, acc_b, acc_c,
    load_sem, wt_s, wt_r, we_s, we_r, sh_s, sh_r, yb_s,
    au_s, ad_s, a_r, bu_s, bd_s, b_r, cu_s, cd_s, c_r, ya_s, ya_r, yc_s, yc_r, xa_s, xa_r,
    rx_s, rx_r, ry_s, ry_r, ryc_s, ryc_r, rza_s, rza_r, rzb_s, rzb_r, rzc_s, rzc_r, f_s, f_r, g_s, g_r, o_s, o_r,
):
    n = ep_count
    major = n // minor
    half, width = xo.shape
    side = width // 2
    quarter = width // tp_count
    tail = side - keep - both_keep
    middle = keep + both_keep
    e = lax.axis_index("ep")
    t = lax.axis_index("tp")
    z = e // minor
    y = e % minor
    xi = t // 2
    c = t % 2
    t2 = 2 * (1 - xi) + c
    other_y = z * minor + 1 - y
    mate_x = {"tp": t2}
    mate_c = {"tp": 2 * xi + 1 - c}
    mate_y = {"ep": other_y}
    across = {"ep": other_y, "tp": t2}
    z_up = {"ep": lax.rem(e + minor, n)}
    z_down = {"ep": lax.rem(e + n - minor, n)}
    far = {"ep": (major - 1 - z) * minor + y}
    is_end = (z == 0) | (z == major - 1)

    barrier = pltpu.get_barrier_semaphore()
    for k in range(1, n):
        pl.semaphore_signal(barrier, inc=1, device_id={"ep": lax.rem(e + k, n)}, device_id_type=MESH)
    for k in range(1, tp_count):
        pl.semaphore_signal(barrier, inc=1, device_id={"tp": lax.rem(t + k, tp_count)}, device_id_type=MESH)
    pl.semaphore_signal(barrier, inc=1, device_id=across, device_id_type=MESH)

    def remote(src, dst, s, r, who):
        return pltpu.make_async_remote_copy(
            src_ref=src, dst_ref=dst, send_sem=s, recv_sem=r, device_id=who, device_id_type=MESH
        )

    def rows_of(which):
        return pl.ds(pl.multiple_of(which * half, half), half)

    def side_of(which):
        return pl.ds(pl.multiple_of(which * side, side), side)

    loads = [
        pltpu.make_async_copy(a, b, load_sem.at[i])
        for i, (a, b) in enumerate(
            (
                (tok_hbm.at[rows_of(c)], tok.at[0]),
                (tok_hbm.at[rows_of(1 - c)], tok.at[1]),
                (gate_hbm, wg.at[c]),
                (up_hbm, wu.at[c]),
                (down_hbm.at[:, side_of(xi)], wd.at[c, :, pl.ds(0, side)]),
                (down_hbm.at[:, side_of(1 - xi)], wd.at[c, :, pl.ds(side, side)]),
                (sg_hbm, sg),
                (su_hbm, su),
                (sd_hbm, sd),
                (gain_hbm, gain_ref),
                (ids_hbm, ids_ref),
                (rw_hbm, rw_ref),
            )
        )
    ]
    for i in (0, 9, 10, 11, 2, 3, 4, 5, 1, 6, 7, 8):
        loads[i].start()

    step = 16

    def norm_into(which, store):
        def body(i, carry):
            part = pl.ds(pl.multiple_of(i * step, step), step)
            v = tok[which, part, :].astype(jnp.float32)
            r = lax.rsqrt(jnp.mean(v * v, axis=-1, keepdims=True) + NORM_EPSILON)
            store(part, (v * r * gain_ref[...]).astype(jnp.bfloat16))
            return carry

        lax.fori_loop(0, half // step, body, 0)

    def store_own(part, value):
        xb[e, part, :] = value

    def store_rest(part, value):
        xo[part, :] = value

    def weights_for(expert):
        row = jnp.zeros((1, ids_ref.shape[1]), jnp.float32)
        for k in range(ids_ref.shape[0]):
            row += jnp.where(ids_ref[k : k + 1, :] == expert, rw_ref[k : k + 1, :], 0.0)
        return row

    loads[0].wait()
    loads[9].wait()
    norm_into(0, store_own)
    loads[10].wait()
    loads[11].wait()
    for d in range(n):
        wtab[d] = weights_for(d * (tp_count // 2) + xi)
    wr[e] = weights_for(e * (tp_count // 2) + xi)
    pl.semaphore_wait(barrier, n + tp_count - 1)

    mine = pl.ds(pl.multiple_of(xi * near, LANES), near)
    theirs = pl.ds(pl.multiple_of((1 - xi) * near, LANES), near)
    shared_cols = pl.ds(2 * near, wide)
    rest = pl.ds(2 * near + wide, width - 2 * near - wide)

    def line_a(g, s, who):
        ref = xb.at[g, :, mine]
        return remote(ref, ref, s.at[g], a_r.at[g], who)

    def line_b(g, s, who):
        ref = xb.at[g, :, rest]
        return remote(ref, ref, s.at[g], b_r.at[g], who)

    def line_c(g, s, who):
        ref = xb.at[g, :, shared_cols]
        return remote(ref, ref, s.at[g], c_r.at[g], who)

    def y_shared(g):
        ref = xb.at[g, :, shared_cols]
        return remote(ref, ref, yc_s.at[g], yc_r.at[g], mate_y)

    def y_first():
        ref = xb.at[e, :, rest]
        return remote(ref, ref, yb_s, b_r.at[e], mate_y)

    def y_copy(g):
        ref = xb.at[g, :, mine]
        return remote(ref, ref, ya_s.at[g], ya_r.at[g], mate_y)

    def x_copy(g):
        ref = xb.at[g, :, mine]
        return remote(ref, ref, xa_s.at[g], xa_r.at[g], mate_x)

    def x_arrival(g):
        ref = xb.at[g, :, theirs]
        return remote(ref, ref, xa_s.at[g], xa_r.at[g], mate_x)

    def wt_copy(k, target):
        return remote(wtab.at[target], wr.at[e], wt_s.at[k], wt_r.at[e], {"ep": target})

    def wt_arrival(g):
        return remote(wtab.at[g], wr.at[g], wt_s.at[0], wt_r.at[g], mate_y)

    def weight_copy(i, which):
        ref = (wg, wu, wd)[i].at[which]
        return remote(ref, ref, we_s.at[i], we_r.at[i], mate_c)

    def sh_copy(k, slot, who):
        return remote(sh_all.at[slot], sh_all.at[slot], sh_s.at[k], sh_r.at[k], {"tp": who})

    def order(j):
        k = jnp.minimum(z, major - 1 - z)
        d = (j + 1) // 2
        close = jnp.where((j % 2 == 1) == (2 * z < major), z - d, z + d)
        far = jnp.where(z <= major - 1 - z, j, major - 1 - j)
        return jnp.where(j <= 2 * k, close, far)

    def slot_group(i):
        p = order(i // 2)
        yy = jnp.where(i % 2 == 0, y, 1 - y)
        return p, p * minor + yy

    def ups(p):
        return (p <= z) & (z < major - 1)

    def downs(p):
        return (p >= z) & (z > 0)

    def forward(p, g, line, s_up, s_down):
        @pl.when(ups(p))
        def _():
            line(g, s_up, z_up).start()

        @pl.when(downs(p))
        def _():
            line(g, s_down, z_down).start()

    forward(z, e, line_a, au_s, ad_s)
    y_first().start()
    forward(z, e, line_c, cu_s, cd_s)
    y_copy(e).start()
    y_shared(e).start()
    forward(z, e, line_b, bu_s, bd_s)
    for k in range(1, n):
        wt_copy(k, lax.rem(e + k, n)).start()
    loads[2].wait()
    weight_copy(0, c).start()
    loads[3].wait()
    weight_copy(1, c).start()
    loads[4].wait()
    loads[5].wait()
    weight_copy(2, c).start()
    loads[1].wait()
    norm_into(1, store_rest)
    loads[6].wait()
    loads[7].wait()

    def shared_in(x):
        g_sum = jnp.dot(x, sg[...], preferred_element_type=jnp.float32)
        u_sum = jnp.dot(x, su[...], preferred_element_type=jnp.float32)
        return (silu(g_sum) * u_sum).astype(jnp.bfloat16)

    sh_all[t, c] = shared_in(xb[e])
    sh_all[t, 1 - c] = shared_in(xo[...])
    for k in range(1, tp_count):
        sh_copy(k, t, lax.rem(t + k, tp_count)).start()

    def rx_copy(g):
        return remote(xs.at[g], xr.at[g], rx_s.at[g], rx_r.at[g], mate_x)

    def ry_copy(p):
        return remote(ys.at[p], yr.at[p], ry_s.at[p], ry_r.at[p], mate_y)

    def ryc_copy(p):
        return remote(ycs.at[p], ycr.at[p], ryc_s.at[p], ryc_r.at[p], mate_y)

    def rzc_copy(p, lane, who):
        return remote(zcs.at[p], zcr.at[lane, p], rzc_s.at[p], rzc_r.at[lane, p], who)

    def rza_copy(p, lane, who):
        return remote(zas.at[p], zar.at[lane, p], rza_s.at[p], rza_r.at[lane, p], who)

    def rzb_copy(g, lane, who):
        return remote(zbs.at[g], zbr.at[lane, g], rzb_s.at[g], rzb_r.at[lane, g], who)

    diagonal = lax.broadcasted_iota(jnp.int32, (half, 2 * half), 1) == (
        lax.broadcasted_iota(jnp.int32, (half, 2 * half), 0) + c * half
    )

    def weight_of(g):
        return jnp.sum(jnp.where(diagonal, wr[g], 0.0), axis=1, keepdims=True)

    def compute(i, j, first, second, both):
        pair = ((i, first), (j, second))
        weight = jnp.concatenate([weight_of(first), weight_of(second)], axis=0)
        x = jnp.concatenate([xb[first], xb[second]], axis=0)
        acts = []
        for h in range(2):
            g_sum = jnp.dot(x, wg[h], preferred_element_type=jnp.float32)
            u_sum = jnp.dot(x, wu[h], preferred_element_type=jnp.float32)
            acts.append((silu(g_sum) * u_sum).astype(jnp.bfloat16))

        def columns(low, high):
            total = jnp.dot(acts[0], wd[0, :, low:high], preferred_element_type=jnp.float32)
            total += jnp.dot(acts[1], wd[1, :, low:high], preferred_element_type=jnp.float32)
            return total * weight

        sent = columns(side, side + keep).astype(jnp.bfloat16)
        kept = columns(0, keep)
        kept_c = columns(keep, middle)
        rest_c = columns(side + keep, side + middle)
        main = columns(middle, side)
        rest = columns(side + middle, width)

        def put(k):
            index, g = pair[k]
            part = slice(k * half, (k + 1) * half)
            xs[g] = sent[part]

            @pl.when(index > 1)
            def _():
                rx_copy(g).start()

            pc[g, :, :both_keep] = kept_c[part]
            pc[g, :, both_keep:] = rest_c[part]

            @pl.when(index % 2 == 1)
            def _():
                p = g // minor
                ycs[p] = pc[g].astype(jnp.bfloat16)
                ryc_copy(p).start()

            pa[g] = kept[part]
            pb[g, :, :tail] = main[part]
            pb[g, :, tail:] = rest[part]

        put(0)

        @pl.when(both)
        def _():
            put(1)

    def add_lanes(p, acc, copy, key, received, direct):
        below = downs(p)
        above = ups(p)
        if direct:
            below &= jnp.logical_not((p == major - 1) & (z == 1))
            above &= jnp.logical_not((p == 0) & (z == major - 2))

        @pl.when(below)
        def _():
            copy(key, 0, z_up).wait_recv()
            acc[...] += received[0, key].astype(jnp.float32)

        @pl.when(above)
        def _():
            copy(key, 1, z_up).wait_recv()
            acc[...] += received[1, key].astype(jnp.float32)

        if direct:

            @pl.when((p == z) & is_end)
            def _():
                copy(key, 2, far).wait_recv()
                acc[...] += received[2, key].astype(jnp.float32)

    def sum_b(p, g):
        acc_b[...] = pb[g]
        add_lanes(p, acc_b, rzb_copy, g, zbr, False)

    def sum_c(p, g):
        ryc_copy(p).wait_recv()
        acc_c[...] = pc[g] + ycr[p].astype(jnp.float32)
        add_lanes(p, acc_c, rzc_copy, p, zcr, True)

    def sum_a(p, g):
        rx_copy(g).wait_recv()
        ry_copy(p).wait_recv()
        acc_a[...] = pa[g] + xr[g].astype(jnp.float32) + yr[p].astype(jnp.float32)
        add_lanes(p, acc_a, rza_copy, p, zar, True)

    def line_order(q):
        above = major - 1 - z
        low = jnp.where(q < above, z + 1 + q, z - 1 - (q - above))
        high = jnp.where(q < z, z - 1 - q, z + 1 + (q - z))
        return jnp.where(2 * z < major, low, high)

    def send_sum(copy, key, p, direct):
        whole = is_end & (p == major - 1 - z)
        step_by = jnp.logical_not(whole) if direct else p != z

        @pl.when((p > z) & step_by)
        def _():
            copy(key, 0, z_up).start()

        @pl.when((p < z) & step_by)
        def _():
            copy(key, 1, z_down).start()

        if direct:

            @pl.when(whole)
            def _():
                copy(key, 2, far).start()

    def do_a(i):
        p, g = slot_group(i)
        line_a(g, au_s, z_up).wait_recv()
        forward(p, g, line_a, au_s, ad_s)
        y_copy(g).start()
        x_copy(g).start()

    def do_c(i):
        p, g = slot_group(i)
        line_c(g, cu_s, z_up).wait_recv()
        forward(p, g, line_c, cu_s, cd_s)
        y_shared(g).start()

    def do_b(i):
        p, g = slot_group(i)
        line_b(g, bu_s, z_up).wait_recv()
        forward(p, g, line_b, bu_s, bd_s)

    def do_x(i):
        _, g = slot_group(i)
        y_copy(g).wait_recv()
        x_copy(g).start()

    def do_k(code):
        i, j = code // (n + 1), code % (n + 1)
        both = j < n
        _, first = slot_group(i)
        _, second = slot_group(jnp.where(both, j, i))

        @pl.when(i == 0)
        def _():
            for k in range(3):
                weight_copy(k, 1 - c).wait_recv()

        def ready(index, g):
            @pl.when(index % 2 == 1)
            def _():
                y_shared(g).wait_recv()

            x_arrival(g).wait_recv()
            wt_arrival(g).wait_recv()

        @pl.when(i > 0)
        def _():
            ready(i, first)

        @pl.when(both)
        def _():
            ready(j, second)

        compute(i, j, first, second, both)

    def do_t(i):
        _, g = slot_group(i)
        rx_copy(g).start()

    def do_r(i):
        p, g = slot_group(i)
        rx_copy(g).wait_recv()
        ys[p] = (pa[g] + xr[g].astype(jnp.float32)).astype(jnp.bfloat16)
        ry_copy(p).start()

    def do_s(_):
        loads[8].wait()
        for k in range(1, tp_count):
            sh_copy(k, lax.rem(t + tp_count - k, tp_count), t).wait_recv()
        share = sg.shape[1]
        for r in range(2):
            shared = jnp.zeros((half, quarter), jnp.float32)
            for q in range(tp_count):
                shared += jnp.dot(
                    sh_all[q, r], sd[q * share : (q + 1) * share, :],
                    preferred_element_type=jnp.float32,
                )
            sh_out[r] = shared

    def do_zb(q):
        p = line_order(q)
        for yy in (1 - y, y):
            g = p * minor + yy
            sum_b(p, g)
            zbs[g] = acc_b[...].astype(jnp.bfloat16)
            send_sum(rzb_copy, g, p, False)

    def do_zc(q):
        p = line_order(q)
        sum_c(p, p * minor + y)
        zcs[p] = acc_c[...].astype(jnp.bfloat16)
        send_sum(rzc_copy, p, p, True)

    def do_za(q):
        p = line_order(q)
        sum_a(p, p * minor + y)
        zas[p] = acc_a[...].astype(jnp.bfloat16)
        send_sum(rza_copy, p, p, True)

    actions = (do_a, do_c, do_b, do_x, do_k, do_t, do_r, do_s, do_zb, do_zc, do_za)

    def main_step(i, carry):
        for a, action in enumerate(actions):
            outer, inner = (
                sum((jnp.where(i == k, slot[a] + 1, 0) for k, slot in enumerate(plan) if slot[a] is not None), i * 0)
                for plan in plans
            )
            code = jnp.where(is_end, outer, inner)

            @pl.when(code > 0)
            def _(action=action, code=code):
                action(code - 1)

        return carry

    lax.fori_loop(0, max(len(plan) for plan in plans), main_step, 0)

    def last_copy(i):
        return remote(fs.at[i], fr.at[i], f_s.at[i], f_r.at[i], (mate_y, across, mate_x)[i])

    last_c = remote(gs, gr, g_s, g_r, mate_x)

    sum_b(z, other_y)
    fs[0] = acc_b[:, :tail].astype(jnp.bfloat16)
    fs[1] = acc_b[:, tail:].astype(jnp.bfloat16)
    last_copy(0).start()
    last_copy(1).start()
    sum_b(z, e)
    fs[2] = acc_b[:, tail:].astype(jnp.bfloat16)
    last_copy(2).start()
    sum_c(z, e)
    gs[...] = acc_c[:, both_keep:].astype(jnp.bfloat16)
    last_c.start()
    sum_a(z, e)

    def place(low, value):
        for q in range(2):
            start, stop = max(low, q * quarter), min(low + value.shape[1], (q + 1) * quarter)
            if start < stop:
                fin[q, :, start - q * quarter : stop - q * quarter] = value[:, start - low : stop - low]

    place(0, acc_a[...])
    last_c.wait_recv()
    place(keep, acc_c[:, :both_keep] + gr[...].astype(jnp.float32))
    for i in range(3):
        last_copy(i).wait_recv()
    place(
        middle,
        acc_b[:, :tail] + fr[0].astype(jnp.float32) + fr[1].astype(jnp.float32) + fr[2].astype(jnp.float32),
    )
    swap = remote(fin.at[1 - c], fin_in, o_s, o_r, mate_c)
    swap.start()
    out_ref[rows_of(c), :] = (fin[c] + sh_out[c]).astype(jnp.bfloat16)
    swap.wait_recv()
    out_ref[rows_of(1 - c), :] = (fin_in[...] + sh_out[1 - c]).astype(jnp.bfloat16)

    swap.wait_send()
    last_c.wait_send()
    for i in range(3):
        last_copy(i).wait_send()
        weight_copy(i, c).wait_send()
    y_first().wait_send()
    for k in range(1, n):
        wt_copy(k, lax.rem(e + k, n)).wait_send()
    for k in range(1, tp_count):
        sh_copy(k, t, lax.rem(t + k, tp_count)).wait_send()

    def drain(i, carry):
        p, g = slot_group(i)

        def sent(line, s_up, s_down):
            @pl.when(ups(p))
            def _():
                line(g, s_up, z_up).wait_send()

            @pl.when(downs(p))
            def _():
                line(g, s_down, z_down).wait_send()

        sent(line_b, bu_s, bd_s)

        @pl.when(i % 2 == 0)
        def _():
            sent(line_a, au_s, ad_s)
            sent(line_c, cu_s, cd_s)
            y_copy(g).wait_send()
            y_shared(g).wait_send()

            @pl.when(p != z)
            def _():
                rza_copy(p, 0, z_up).wait_send()
                rzc_copy(p, 0, z_up).wait_send()

        @pl.when(i % 2 == 1)
        def _():
            ry_copy(p).wait_send()
            ryc_copy(p).wait_send()

        @pl.when(i > 0)
        def _():
            x_copy(g).wait_send()

        rx_copy(g).wait_send()

        @pl.when(p != z)
        def _():
            rzb_copy(g, 0, z_up).wait_send()

        return carry

    lax.fori_loop(0, n, drain, 0)


def slots_of(listing, n):
    slots, last = [], len(KINDS)
    for kind, *args in listing:
        a = KINDS.index(kind)
        if a <= last and (a == last or last == len(KINDS) or a < last):
            slots.append([None] * len(KINDS))
        slots[-1][a] = args[0] * (n + 1) + (args[1] if len(args) > 1 else n) if kind == "k" else args[0]
        last = a
    return slots


def dense_exchange(
    tokens, norm_gain, expert_ids, route_weights, expert_gate, expert_up, expert_down,
    shared_gate, shared_up, shared_down,
):
    n = lax.axis_size("ep")
    tp_count = lax.axis_size("tp")
    minor = 1 << (n.bit_length() - 1) // 2
    major = n // minor
    rows, width = tokens.shape
    half = rows // 2
    side = width // 2
    quarter = width // tp_count
    near = side * NEAR // 8 // LANES * LANES
    wide = 2 * (side * WIDE // 8 // LANES * LANES)
    keep = side * KEEP // 8 // LANES * LANES
    both_keep = side * BOTH_KEEP // 8 // LANES * LANES
    tail = side - keep - both_keep
    ff = expert_gate.shape[2]
    share = shared_gate.shape[1]
    bf16, f32 = jnp.bfloat16, jnp.float32
    dma = pltpu.SemaphoreType.DMA
    vmem = pl.BlockSpec(memory_space=pltpu.VMEM)
    anywhere = pl.BlockSpec(memory_space=pl.ANY)
    return pl.pallas_call(
        functools.partial(dense_kernel, n, tp_count, minor, near, wide, keep, both_keep, [slots_of(p, n) for p in plans_for(n)]),
        out_shape=pltpu.VMEM((rows, quarter), bf16),
        in_specs=[anywhere] * 10,
        out_specs=vmem,
        scratch_shapes=[
            pltpu.VMEM((expert_ids.shape[1], rows), jnp.int32),
            pltpu.VMEM((expert_ids.shape[1], rows), f32),
            pltpu.VMEM((1, width), f32),
            pltpu.VMEM((2, half, width), bf16),
            pltpu.VMEM((n, half, width), bf16),
            pltpu.VMEM((half, width), bf16),
            pltpu.VMEM((n, 1, rows), f32),
            pltpu.VMEM((n, 1, rows), f32),
            pltpu.VMEM((2, width, ff), bf16),
            pltpu.VMEM((2, width, ff), bf16),
            pltpu.VMEM((2, ff, width), bf16),
            pltpu.VMEM((width, share), bf16),
            pltpu.VMEM((width, share), bf16),
            pltpu.VMEM((share * tp_count, quarter), bf16),
            pltpu.VMEM((tp_count, 2, half, share), bf16),
            pltpu.VMEM((2, half, quarter), f32),
            pltpu.VMEM((n, half, keep), f32),
            pltpu.VMEM((n, half, 2 * tail), f32),
            pltpu.VMEM((n, half, 2 * both_keep), f32),
            pltpu.VMEM((n, half, keep), bf16),
            pltpu.VMEM((n, half, keep), bf16),
            pltpu.VMEM((major, half, keep), bf16),
            pltpu.VMEM((major, half, keep), bf16),
            pltpu.VMEM((major, half, 2 * both_keep), bf16),
            pltpu.VMEM((major, half, 2 * both_keep), bf16),
            pltpu.VMEM((major, half, keep), bf16),
            pltpu.VMEM((3, major, half, keep), bf16),
            pltpu.VMEM((n, half, 2 * tail), bf16),
            pltpu.VMEM((2, n, half, 2 * tail), bf16),
            pltpu.VMEM((major, half, 2 * both_keep), bf16),
            pltpu.VMEM((3, major, half, 2 * both_keep), bf16),
            pltpu.VMEM((3, half, tail), bf16),
            pltpu.VMEM((3, half, tail), bf16),
            pltpu.VMEM((half, both_keep), bf16),
            pltpu.VMEM((half, both_keep), bf16),
            pltpu.VMEM((2, half, quarter), f32),
            pltpu.VMEM((half, quarter), f32),
            pltpu.VMEM((half, keep), f32),
            pltpu.VMEM((half, 2 * tail), f32),
            pltpu.VMEM((half, 2 * both_keep), f32),
            dma((12,)), dma((n,)), dma((n,)), dma((3,)), dma((3,)), dma((tp_count,)), dma((tp_count,)), dma,
            dma((n,)), dma((n,)), dma((n,)), dma((n,)), dma((n,)), dma((n,)), dma((n,)), dma((n,)), dma((n,)),
            dma((n,)), dma((n,)), dma((n,)), dma((n,)), dma((n,)), dma((n,)),
            dma((n,)), dma((n,)), dma((major,)), dma((major,)), dma((major,)), dma((major,)),
            dma((major,)), dma((3, major)), dma((n,)), dma((2, n)), dma((major,)), dma((3, major)),
            dma((3,)), dma((3,)), dma, dma, dma, dma,
        ],
        compiler_params=pltpu.CompilerParams(
            collective_id=0, has_side_effects=True, vmem_limit_bytes=60 << 20
        ),
        name="dense_moe",
    )(
        expert_ids.T, route_weights.T, norm_gain.reshape(1, width), tokens,
        expert_gate[0], expert_up[0], expert_down[0],
        shared_gate, shared_up, shared_down,
    )


def local(tokens, *rest):
    ep_count = lax.axis_size("ep")
    pair_count = lax.axis_size("tp") // 2
    dense_bytes = 4 * ep_count * tokens.size * tokens.dtype.itemsize
    minor = 1 << (ep_count.bit_length() - 1) // 2
    if pair_count == 2 and minor == 2 and dense_bytes <= 24 << 20:
        return dense_exchange(tokens, *rest)
    return routed_exchange(tokens, *rest)


def solution(mesh):
    return jax.shard_map(
        local,
        mesh=mesh,
        in_specs=(
            P("ep", None),
            P(),
            P("ep", None),
            P("ep", None),
            P(("ep", "tp"), None, None),
            P(("ep", "tp"), None, None),
            P(("ep", "tp"), None, None),
            P(None, "tp"),
            P(None, "tp"),
            P(None, "tp"),
        ),
        out_specs=P("ep", "tp"),
        check_vma=False,
    )
```

```python
import functools

import jax
import jax.numpy as jnp
from jax import lax
from jax.experimental import pallas as pl
from jax.experimental.pallas import tpu as pltpu
from jax.sharding import PartitionSpec as P

NORM_EPSILON = 1e-06


def swapped(block, axis, distance):
    count = lax.axis_size(axis)
    route = []
    for low in range(count):
        high = low | 1 << distance
        if high != low and high < count:
            route += [(low, high), (high, low)]
    return lax.ppermute(block, axis, route)


def routed_exchange(
    tokens,
    norm_gain,
    expert_ids,
    route_weights,
    expert_gate,
    expert_up,
    expert_down,
    shared_gate,
    shared_up,
    shared_down,
):
    ep_count = lax.axis_size("ep")
    tp_count = lax.axis_size("tp")
    pair_count = tp_count // 2
    tp_index = lax.axis_index("tp")
    column = tp_index // 2
    half_index = tp_index % 2
    token_count, model_width = tokens.shape
    top_count = expert_ids.shape[1]
    expert_count = ep_count * pair_count
    capacity = 2 * max(1, token_count * top_count // expert_count)
    half_cap = capacity // 2
    as_float = tokens.astype(jnp.float32)
    inverse_rms = lax.rsqrt(jnp.mean(as_float * as_float, axis=-1, keepdims=True) + NORM_EPSILON)
    normed = (as_float * inverse_rms * norm_gain).astype(jnp.bfloat16)
    expert_iota = jnp.arange(expert_count, dtype=jnp.int32)
    token_iota = jnp.arange(token_count, dtype=jnp.int32)
    counts = jnp.sum(
        (expert_ids[:, :, None] == expert_iota[None, None, :]).astype(jnp.bfloat16), axis=1
    )
    strict_lower = (token_iota[:, None] > token_iota[None, :]).astype(jnp.bfloat16)
    prefix = jnp.dot(strict_lower, counts, preferred_element_type=jnp.float32)
    slot_index = jnp.take_along_axis(prefix, expert_ids, axis=1).astype(jnp.int32)
    target = expert_ids // pair_count
    owner_column = expert_ids % pair_count
    is_mine = owner_column == column
    position = target * capacity + slot_index
    slot_iota = jnp.arange(ep_count * capacity, dtype=jnp.int32)
    matches = is_mine[None, :, :] & (position[None, :, :] == slot_iota[:, None, None])
    slot_taken = jnp.any(matches, axis=2)
    token_of_slot = jnp.sum(jnp.where(slot_taken, token_iota[None, :], 0), axis=1)
    filled = jnp.any(slot_taken, axis=1)
    buffer = jnp.where(
        filled[:, None], jnp.take(normed, token_of_slot, axis=0), jnp.zeros((), jnp.bfloat16)
    )
    buffer = buffer.reshape(ep_count, capacity, model_width)
    gate_local = expert_gate[0]
    up_local = expert_up[0]
    down_local = expert_down[0]
    received = lax.all_to_all(buffer, "ep", split_axis=0, concat_axis=0, tiled=True)
    flat_rows = received.reshape(-1, model_width)
    hidden = (
        jax.nn.silu(jnp.dot(flat_rows, gate_local, preferred_element_type=jnp.float32))
        * jnp.dot(flat_rows, up_local, preferred_element_type=jnp.float32)
    ).astype(jnp.bfloat16)
    partial_out = jnp.dot(hidden, down_local, preferred_element_type=jnp.float32).astype(
        jnp.bfloat16
    )
    partial_out = partial_out.reshape(received.shape[0], received.shape[1], model_width)
    kept_part = lax.dynamic_slice_in_dim(partial_out, half_index * half_cap, half_cap, 1)
    other_part = lax.dynamic_slice_in_dim(partial_out, (1 - half_index) * half_cap, half_cap, 1)
    partner_part = swapped(other_part, "tp", 0)
    expert_out = (kept_part.astype(jnp.float32) + partner_part.astype(jnp.float32)).astype(
        jnp.bfloat16
    )
    returned = lax.all_to_all(expert_out, "ep", split_axis=0, concat_axis=0, tiled=True)
    row_total = ep_count * half_cap
    flat_rows = returned.reshape(row_total, model_width).astype(jnp.float32)
    is_valid = is_mine & (slot_index // half_cap == half_index)
    row_index = jnp.where(is_valid, target * half_cap + slot_index % half_cap, -1)
    row_iota = jnp.arange(row_total, dtype=jnp.int32)
    hits = row_index[:, :, None] == row_iota[None, None, :]
    combine_table = jnp.sum(jnp.where(hits, route_weights[:, :, None], 0.0), axis=1)
    partial_routed = jnp.dot(
        combine_table,
        flat_rows,
        precision=lax.Precision.HIGHEST,
        preferred_element_type=jnp.float32,
    )
    routed = lax.psum_scatter(partial_routed, "tp", scatter_dimension=1, tiled=True)
    shared_act = (
        jax.nn.silu(jnp.dot(normed, shared_gate, preferred_element_type=jnp.float32))
        * jnp.dot(normed, shared_up, preferred_element_type=jnp.float32)
    ).astype(jnp.bfloat16)
    shared_out = jnp.dot(
        lax.all_gather(shared_act, "tp", axis=1, tiled=True),
        shared_down,
        preferred_element_type=jnp.float32,
    )
    return (routed + shared_out).astype(jnp.bfloat16)


MESH = pl.DeviceIdType.MESH
LANES = 128
BOTH_KEEP = 3
KEEP = 4
WIDE = 3
NEAR = 3


def silu(v):
    return v / (1.0 + jnp.exp(-v))


FIELD = 16
KINDS = ("a", "c", "b", "x", "k", "t", "r", "w", "s", "zb", "zc", "za", "f1", "f2", "f3", "-")
OUTER = [
    ("a", 2), ("b", 1), ("x", 1), ("c", 2), ("s", 0), ("b", 2), ("w", 0), ("k", 0, 1), ("x", 3), ("a", 4), ("t", 1),
    ("t", 0), ("k", 2), ("b", 3), ("k", 3), ("a", 6), ("zb", 0), ("c", 4), ("x", 5), ("r", 1), ("b", 4), ("k", 4),
    ("b", 5), ("zc", 0), ("x", 7), ("c", 6), ("r", 3), ("b", 6), ("k", 5, 6), ("b", 7), ("zb", 1), ("k", 7),
    ("zb", 2), ("za", 0), ("r", 5), ("zc", 1), ("r", 7), ("zc", 2), ("za", 1), ("za", 2), ("f1", 0), ("f2", 0),
    ("f3", 0),
]
INNER = [
    ("a", 2), ("a", 4), ("b", 1), ("x", 1), ("c", 4), ("c", 2), ("s", 0), ("w", 0), ("k", 0), ("a", 6), ("t", 0),
    ("b", 4), ("k", 1, 4), ("x", 5), ("t", 1), ("b", 5), ("b", 2), ("k", 2), ("b", 3), ("x", 3), ("c", 6), ("b", 6),
    ("k", 6), ("x", 7), ("b", 7), ("k", 5), ("r", 1), ("k", 3), ("k", 7), ("r", 5), ("r", 3), ("zb", 0), ("r", 7),
    ("zc", 1), ("zb", 1), ("f1", 0), ("f2", 0), ("zc", 2), ("za", 1), ("zc", 0), ("zb", 2), ("za", 2), ("za", 0),
    ("f3", 0),
]
OUTER += [("-", 0)] * 1
PLANS = {4: (OUTER, INNER)}


def dense_kernel(
    ep_count, tp_count, minor, near, wide, keep, both_keep, plans,
    ids_hbm, rw_hbm, gain_hbm, tok_hbm, gate_hbm, up_hbm, down_hbm, sg_hbm, su_hbm, sd_hbm,
    out_ref,
    ids_ref, rw_ref, gain_ref, tok, xb, xo, wtab, wr, wg, wu, wd, sg, su, sd, sh_all, sh_out,
    pa, pb, pc, xs, xr, ys, yr, ycs, ycr, zas, zar, zbs, zbr, zcs, zcr, fs, fr, gs, gr, fin, fin_in, last_b, last_m, acc_a, acc_b, acc_c,
    load_sem, wt_s, wt_r, we_s, we_r, sh_s, sh_r, yb_s,
    au_s, ad_s, a_r, bu_s, bd_s, b_r, cu_s, cd_s, c_r, ya_s, ya_r, yc_s, yc_r, xa_s, xa_r,
    rx_s, rx_r, ry_s, ry_r, ryc_s, ryc_r, rza_s, rza_r, rzb_s, rzb_r, rzc_s, rzc_r, f_s, f_r, g_s, g_r, o_s, o_r,
):
    n = ep_count
    major = n // minor
    half, width = xo.shape
    side = width // 2
    quarter = width // tp_count
    tail = side - keep - both_keep
    middle = keep + both_keep
    e = lax.axis_index("ep")
    t = lax.axis_index("tp")
    z = e // minor
    y = e % minor
    xi = t // 2
    c = t % 2
    t2 = 2 * (1 - xi) + c
    other_y = z * minor + 1 - y
    mate_x = {"tp": t2}
    mate_c = {"tp": 2 * xi + 1 - c}
    mate_y = {"ep": other_y}
    across = {"ep": other_y, "tp": t2}
    z_up = {"ep": lax.rem(e + minor, n)}
    z_down = {"ep": lax.rem(e + n - minor, n)}
    far = {"ep": (major - 1 - z) * minor + y}
    is_end = (z == 0) | (z == major - 1)

    barrier = pltpu.get_barrier_semaphore()
    for k in range(1, n):
        pl.semaphore_signal(barrier, inc=1, device_id={"ep": lax.rem(e + k, n)}, device_id_type=MESH)
    for k in range(1, tp_count):
        pl.semaphore_signal(barrier, inc=1, device_id={"tp": lax.rem(t + k, tp_count)}, device_id_type=MESH)
    pl.semaphore_signal(barrier, inc=1, device_id=across, device_id_type=MESH)

    def remote(src, dst, s, r, who):
        return pltpu.make_async_remote_copy(
            src_ref=src, dst_ref=dst, send_sem=s, recv_sem=r, device_id=who, device_id_type=MESH
        )

    def rows_of(which):
        return pl.ds(pl.multiple_of(which * half, half), half)

    def side_of(which):
        return pl.ds(pl.multiple_of(which * side, side), side)

    loads = [
        pltpu.make_async_copy(a, b, load_sem.at[i])
        for i, (a, b) in enumerate(
            (
                (tok_hbm.at[rows_of(c)], tok.at[0]),
                (tok_hbm.at[rows_of(1 - c)], tok.at[1]),
                (gate_hbm, wg.at[c]),
                (up_hbm, wu.at[c]),
                (down_hbm.at[:, side_of(xi)], wd.at[c, :, pl.ds(0, side)]),
                (down_hbm.at[:, side_of(1 - xi)], wd.at[c, :, pl.ds(side, side)]),
                (sg_hbm, sg),
                (su_hbm, su),
                (sd_hbm, sd),
                (gain_hbm, gain_ref),
                (ids_hbm, ids_ref),
                (rw_hbm, rw_ref),
            )
        )
    ]
    for i in (0, 9, 10, 11, 2, 3, 4, 5, 1, 6, 7, 8):
        loads[i].start()

    step = 16

    def norm_into(which, store):
        def body(i, carry):
            part = pl.ds(pl.multiple_of(i * step, step), step)
            v = tok[which, part, :].astype(jnp.float32)
            r = lax.rsqrt(jnp.mean(v * v, axis=-1, keepdims=True) + NORM_EPSILON)
            store(part, (v * r * gain_ref[...]).astype(jnp.bfloat16))
            return carry

        lax.fori_loop(0, half // step, body, 0)

    def store_own(part, value):
        xb[e, part, :] = value

    def store_rest(part, value):
        xo[part, :] = value

    def weights_for(expert):
        row = jnp.zeros((1, ids_ref.shape[1]), jnp.float32)
        for k in range(ids_ref.shape[0]):
            row += jnp.where(ids_ref[k : k + 1, :] == expert, rw_ref[k : k + 1, :], 0.0)
        return row

    loads[0].wait()
    loads[9].wait()
    norm_into(0, store_own)
    loads[10].wait()
    loads[11].wait()
    for d in range(n):
        wtab[d] = weights_for(d * (tp_count // 2) + xi)
    wr[e] = weights_for(e * (tp_count // 2) + xi)
    pl.semaphore_wait(barrier, n + tp_count - 1)

    mine = pl.ds(pl.multiple_of(xi * near, LANES), near)
    theirs = pl.ds(pl.multiple_of((1 - xi) * near, LANES), near)
    shared_cols = pl.ds(2 * near, wide)
    rest = pl.ds(2 * near + wide, width - 2 * near - wide)

    def line_a(g, s, who):
        ref = xb.at[g, :, mine]
        return remote(ref, ref, s.at[g], a_r.at[g], who)

    def line_b(g, s, who):
        ref = xb.at[g, :, rest]
        return remote(ref, ref, s.at[g], b_r.at[g], who)

    def line_c(g, s, who):
        ref = xb.at[g, :, shared_cols]
        return remote(ref, ref, s.at[g], c_r.at[g], who)

    def y_shared(g):
        ref = xb.at[g, :, shared_cols]
        return remote(ref, ref, yc_s.at[g], yc_r.at[g], mate_y)

    def y_first():
        ref = xb.at[e, :, rest]
        return remote(ref, ref, yb_s, b_r.at[e], mate_y)

    def y_copy(g):
        ref = xb.at[g, :, mine]
        return remote(ref, ref, ya_s.at[g], ya_r.at[g], mate_y)

    def x_copy(g):
        ref = xb.at[g, :, mine]
        return remote(ref, ref, xa_s.at[g], xa_r.at[g], mate_x)

    def x_arrival(g):
        ref = xb.at[g, :, theirs]
        return remote(ref, ref, xa_s.at[g], xa_r.at[g], mate_x)

    def wt_copy(k, target):
        return remote(wtab.at[target], wr.at[e], wt_s.at[k], wt_r.at[e], {"ep": target})

    def wt_arrival(g):
        return remote(wtab.at[g], wr.at[g], wt_s.at[0], wt_r.at[g], mate_y)

    def weight_copy(i, which):
        ref = (wg, wu, wd)[i].at[which]
        return remote(ref, ref, we_s.at[i], we_r.at[i], mate_c)

    def sh_copy(k, slot, who):
        return remote(sh_all.at[slot], sh_all.at[slot], sh_s.at[k], sh_r.at[k], {"tp": who})

    def order(j):
        k = jnp.minimum(z, major - 1 - z)
        d = (j + 1) // 2
        close = jnp.where((j % 2 == 1) == (2 * z < major), z - d, z + d)
        far = jnp.where(z <= major - 1 - z, j, major - 1 - j)
        return jnp.where(j <= 2 * k, close, far)

    def slot_group(i):
        p = order(i // 2)
        yy = jnp.where(i % 2 == 0, y, 1 - y)
        return p, p * minor + yy

    def ups(p):
        return (p <= z) & (z < major - 1)

    def downs(p):
        return (p >= z) & (z > 0)

    def forward(p, g, line, s_up, s_down):
        @pl.when(ups(p))
        def _():
            line(g, s_up, z_up).start()

        @pl.when(downs(p))
        def _():
            line(g, s_down, z_down).start()

    forward(z, e, line_a, au_s, ad_s)
    y_first().start()
    forward(z, e, line_c, cu_s, cd_s)
    y_copy(e).start()
    y_shared(e).start()
    forward(z, e, line_b, bu_s, bd_s)
    for k in range(1, n):
        wt_copy(k, lax.rem(e + k, n)).start()
    loads[2].wait()
    weight_copy(0, c).start()
    loads[3].wait()
    weight_copy(1, c).start()
    loads[4].wait()
    loads[5].wait()
    weight_copy(2, c).start()
    loads[1].wait()
    norm_into(1, store_rest)
    loads[6].wait()
    loads[7].wait()

    def shared_in(x):
        g_sum = jnp.dot(x, sg[...], preferred_element_type=jnp.float32)
        u_sum = jnp.dot(x, su[...], preferred_element_type=jnp.float32)
        return (silu(g_sum) * u_sum).astype(jnp.bfloat16)

    sh_all[t, c] = shared_in(xb[e])
    sh_all[t, 1 - c] = shared_in(xo[...])
    for k in range(1, tp_count):
        sh_copy(k, t, lax.rem(t + k, tp_count)).start()

    def rx_copy(g):
        return remote(xs.at[g], xr.at[g], rx_s.at[g], rx_r.at[g], mate_x)

    def ry_copy(p):
        return remote(ys.at[p], yr.at[p], ry_s.at[p], ry_r.at[p], mate_y)

    def ryc_copy(p):
        return remote(ycs.at[p], ycr.at[p], ryc_s.at[p], ryc_r.at[p], mate_y)

    def rzc_copy(p, lane, who):
        return remote(zcs.at[p], zcr.at[lane, p], rzc_s.at[p], rzc_r.at[lane, p], who)

    def rza_copy(p, lane, who):
        return remote(zas.at[p], zar.at[lane, p], rza_s.at[p], rza_r.at[lane, p], who)

    def rzb_copy(g, lane, who):
        return remote(zbs.at[g], zbr.at[lane, g], rzb_s.at[g], rzb_r.at[lane, g], who)

    diagonal = lax.broadcasted_iota(jnp.int32, (half, 2 * half), 1) == (
        lax.broadcasted_iota(jnp.int32, (half, 2 * half), 0) + c * half
    )

    def weight_of(g):
        return jnp.sum(jnp.where(diagonal, wr[g], 0.0), axis=1, keepdims=True)

    def compute(i, j, first, second, both):
        pair = ((i, first), (j, second))
        weight = jnp.concatenate([weight_of(first), weight_of(second)], axis=0)
        x = jnp.concatenate([xb[first], xb[second]], axis=0)
        acts = []
        for h in range(2):
            g_sum = jnp.dot(x, wg[h], preferred_element_type=jnp.float32)
            u_sum = jnp.dot(x, wu[h], preferred_element_type=jnp.float32)
            acts.append((silu(g_sum) * u_sum).astype(jnp.bfloat16))

        def columns(low, high):
            total = jnp.dot(acts[0], wd[0, :, low:high], preferred_element_type=jnp.float32)
            total += jnp.dot(acts[1], wd[1, :, low:high], preferred_element_type=jnp.float32)
            return total * weight

        sent = columns(side, side + keep).astype(jnp.bfloat16)
        kept = columns(0, keep)
        kept_c = columns(keep, middle)
        rest_c = columns(side + keep, side + middle)
        main = columns(middle, side)
        rest = columns(side + middle, width)

        def put(k):
            index, g = pair[k]
            part = slice(k * half, (k + 1) * half)
            xs[g] = sent[part]

            @pl.when(index > 1)
            def _():
                rx_copy(g).start()

            pc[g, :, :both_keep] = kept_c[part]
            pc[g, :, both_keep:] = rest_c[part]

            @pl.when(index % 2 == 1)
            def _():
                p = g // minor
                ycs[p] = pc[g].astype(jnp.bfloat16)
                ryc_copy(p).start()

            pa[g] = kept[part]
            pb[g, :, :tail] = main[part]
            pb[g, :, tail:] = rest[part]

        put(0)

        @pl.when(both)
        def _():
            put(1)

    def add_lanes(p, acc, copy, key, received, direct):
        below = downs(p)
        above = ups(p)
        if direct:
            below &= jnp.logical_not((p == major - 1) & (z == 1))
            above &= jnp.logical_not((p == 0) & (z == major - 2))

        @pl.when(below)
        def _():
            copy(key, 0, z_up).wait_recv()
            acc[...] += received[0, key].astype(jnp.float32)

        @pl.when(above)
        def _():
            copy(key, 1, z_up).wait_recv()
            acc[...] += received[1, key].astype(jnp.float32)

        if direct:

            @pl.when((p == z) & is_end)
            def _():
                copy(key, 2, far).wait_recv()
                acc[...] += received[2, key].astype(jnp.float32)

    def sum_b(p, g):
        acc_b[...] = pb[g]
        add_lanes(p, acc_b, rzb_copy, g, zbr, False)

    def sum_c(p, g):
        ryc_copy(p).wait_recv()
        acc_c[...] = pc[g] + ycr[p].astype(jnp.float32)
        add_lanes(p, acc_c, rzc_copy, p, zcr, True)

    def sum_a(p, g):
        rx_copy(g).wait_recv()
        ry_copy(p).wait_recv()
        acc_a[...] = pa[g] + xr[g].astype(jnp.float32) + yr[p].astype(jnp.float32)
        add_lanes(p, acc_a, rza_copy, p, zar, True)

    def line_order(q):
        above = major - 1 - z
        low = jnp.where(q < above, z + 1 + q, z - 1 - (q - above))
        high = jnp.where(q < z, z - 1 - q, z + 1 + (q - z))
        return jnp.where(2 * z < major, low, high)

    def send_sum(copy, key, p, direct):
        whole = is_end & (p == major - 1 - z)
        step_by = jnp.logical_not(whole) if direct else p != z

        @pl.when((p > z) & step_by)
        def _():
            copy(key, 0, z_up).start()

        @pl.when((p < z) & step_by)
        def _():
            copy(key, 1, z_down).start()

        if direct:

            @pl.when(whole)
            def _():
                copy(key, 2, far).start()

    def do_a(i):
        p, g = slot_group(i)
        line_a(g, au_s, z_up).wait_recv()
        forward(p, g, line_a, au_s, ad_s)
        y_copy(g).start()
        x_copy(g).start()

    def do_c(i):
        p, g = slot_group(i)
        line_c(g, cu_s, z_up).wait_recv()
        forward(p, g, line_c, cu_s, cd_s)
        y_shared(g).start()

    def do_b(i):
        p, g = slot_group(i)
        line_b(g, bu_s, z_up).wait_recv()
        forward(p, g, line_b, bu_s, bd_s)

    def do_x(i):
        _, g = slot_group(i)
        y_copy(g).wait_recv()
        x_copy(g).start()

    def do_k(code):
        i, j = code // FIELD, code % FIELD
        both = j < FIELD - 1
        _, first = slot_group(i)
        _, second = slot_group(jnp.where(both, j, i))

        def ready(index, g):
            @pl.when(index % 2 == 1)
            def _():
                y_shared(g).wait_recv()

            x_arrival(g).wait_recv()
            wt_arrival(g).wait_recv()

        @pl.when(i > 0)
        def _():
            ready(i, first)

        @pl.when(both)
        def _():
            ready(j, second)

        compute(i, j, first, second, both)

    def do_w(_):
        for k in range(3):
            weight_copy(k, 1 - c).wait_recv()

    def do_t(i):
        _, g = slot_group(i)
        rx_copy(g).start()

    def do_r(i):
        p, g = slot_group(i)
        rx_copy(g).wait_recv()
        ys[p] = (pa[g] + xr[g].astype(jnp.float32)).astype(jnp.bfloat16)
        ry_copy(p).start()

    def do_s(_):
        loads[8].wait()
        for k in range(1, tp_count):
            sh_copy(k, lax.rem(t + tp_count - k, tp_count), t).wait_recv()
        share = sg.shape[1]
        for r in range(2):
            shared = jnp.zeros((half, quarter), jnp.float32)
            for q in range(tp_count):
                shared += jnp.dot(
                    sh_all[q, r], sd[q * share : (q + 1) * share, :],
                    preferred_element_type=jnp.float32,
                )
            sh_out[r] = shared

    def do_zb(q):
        p = line_order(q)
        for yy in (1 - y, y):
            g = p * minor + yy
            sum_b(p, g)
            zbs[g] = acc_b[...].astype(jnp.bfloat16)
            send_sum(rzb_copy, g, p, False)

    def do_zc(q):
        p = line_order(q)
        sum_c(p, p * minor + y)
        zcs[p] = acc_c[...].astype(jnp.bfloat16)
        send_sum(rzc_copy, p, p, True)

    def do_za(q):
        p = line_order(q)
        sum_a(p, p * minor + y)
        zas[p] = acc_a[...].astype(jnp.bfloat16)
        send_sum(rza_copy, p, p, True)

    def last_copy(i):
        return remote(fs.at[i], fr.at[i], f_s.at[i], f_r.at[i], (mate_y, across, mate_x)[i])

    last_c = remote(gs, gr, g_s, g_r, mate_x)

    def do_f1(_):
        sum_b(z, other_y)
        fs[0] = acc_b[:, :tail].astype(jnp.bfloat16)
        fs[1] = acc_b[:, tail:].astype(jnp.bfloat16)
        last_copy(0).start()
        last_copy(1).start()

    def do_f2(_):
        sum_b(z, e)
        fs[2] = acc_b[:, tail:].astype(jnp.bfloat16)
        last_copy(2).start()
        last_b[...] = acc_b[:, :tail]

    def do_f3(_):
        sum_c(z, e)
        gs[...] = acc_c[:, both_keep:].astype(jnp.bfloat16)
        last_c.start()
        last_m[...] = acc_c[:, :both_keep]

    actions = (
        (do_a, do_c, do_b, do_x, do_k, do_t, do_r, do_w),
        (do_s, do_zb, do_zc, do_za, do_f1, do_f2, do_f3),
    )

    codes = [jnp.where(is_end, outer, inner) for outer, inner in zip(*plans)]

    def main_step(i, carry):
        code = i * 0
        for k, value in enumerate(codes):
            code = jnp.where(i == k, value, code)
        kind = code // (FIELD * FIELD)
        arg = code % (FIELD * FIELD)
        for side_of_list, group in enumerate(actions):

            @pl.when(kind // 8 == side_of_list)
            def _(group=group):
                for a, action in enumerate(group):

                    @pl.when(kind % 8 == a)
                    def _(action=action):
                        action(arg)

        return carry

    lax.fori_loop(0, len(plans[0]), main_step, 0)

    sum_a(z, e)

    def place(low, value):
        for q in range(2):
            start, stop = max(low, q * quarter), min(low + value.shape[1], (q + 1) * quarter)
            if start < stop:
                fin[q, :, start - q * quarter : stop - q * quarter] = value[:, start - low : stop - low]

    place(0, acc_a[...])
    last_c.wait_recv()
    place(keep, last_m[...] + gr[...].astype(jnp.float32))
    for i in range(3):
        last_copy(i).wait_recv()
    place(
        middle,
        last_b[...] + fr[0].astype(jnp.float32) + fr[1].astype(jnp.float32) + fr[2].astype(jnp.float32),
    )
    swap = remote(fin.at[1 - c], fin_in, o_s, o_r, mate_c)
    swap.start()
    out_ref[rows_of(c), :] = (fin[c] + sh_out[c]).astype(jnp.bfloat16)
    swap.wait_recv()
    out_ref[rows_of(1 - c), :] = (fin_in[...] + sh_out[1 - c]).astype(jnp.bfloat16)

    swap.wait_send()
    last_c.wait_send()
    for i in range(3):
        last_copy(i).wait_send()
        weight_copy(i, c).wait_send()
    y_first().wait_send()
    for k in range(1, n):
        wt_copy(k, lax.rem(e + k, n)).wait_send()
    for k in range(1, tp_count):
        sh_copy(k, t, lax.rem(t + k, tp_count)).wait_send()

    def drain(i, carry):
        p, g = slot_group(i)

        def sent(line, s_up, s_down):
            @pl.when(ups(p))
            def _():
                line(g, s_up, z_up).wait_send()

            @pl.when(downs(p))
            def _():
                line(g, s_down, z_down).wait_send()

        sent(line_b, bu_s, bd_s)

        @pl.when(i % 2 == 0)
        def _():
            sent(line_a, au_s, ad_s)
            sent(line_c, cu_s, cd_s)
            y_copy(g).wait_send()
            y_shared(g).wait_send()

            @pl.when(p != z)
            def _():
                rza_copy(p, 0, z_up).wait_send()
                rzc_copy(p, 0, z_up).wait_send()

        @pl.when(i % 2 == 1)
        def _():
            ry_copy(p).wait_send()
            ryc_copy(p).wait_send()

        @pl.when(i > 0)
        def _():
            x_copy(g).wait_send()

        rx_copy(g).wait_send()

        @pl.when(p != z)
        def _():
            rzb_copy(g, 0, z_up).wait_send()

        return carry

    lax.fori_loop(0, n, drain, 0)


def coded(plan):
    codes = []
    for kind, first, *second in plan:
        arg = first * FIELD + (second[0] if second else FIELD - 1) if kind == "k" else first
        codes.append((KINDS.index(kind) * FIELD * FIELD) + arg)
    return codes


def dense_exchange(
    tokens, norm_gain, expert_ids, route_weights, expert_gate, expert_up, expert_down,
    shared_gate, shared_up, shared_down,
):
    n = lax.axis_size("ep")
    tp_count = lax.axis_size("tp")
    minor = 1 << (n.bit_length() - 1) // 2
    major = n // minor
    rows, width = tokens.shape
    half = rows // 2
    side = width // 2
    quarter = width // tp_count
    near = side * NEAR // 8 // LANES * LANES
    wide = 2 * (side * WIDE // 8 // LANES * LANES)
    keep = side * KEEP // 8 // LANES * LANES
    both_keep = side * BOTH_KEEP // 8 // LANES * LANES
    tail = side - keep - both_keep
    ff = expert_gate.shape[2]
    share = shared_gate.shape[1]
    bf16, f32 = jnp.bfloat16, jnp.float32
    dma = pltpu.SemaphoreType.DMA
    vmem = pl.BlockSpec(memory_space=pltpu.VMEM)
    anywhere = pl.BlockSpec(memory_space=pl.ANY)
    return pl.pallas_call(
        functools.partial(dense_kernel, n, tp_count, minor, near, wide, keep, both_keep, [coded(plan) for plan in PLANS[n // minor]]),
        out_shape=pltpu.VMEM((rows, quarter), bf16),
        in_specs=[anywhere] * 10,
        out_specs=vmem,
        scratch_shapes=[
            pltpu.VMEM((expert_ids.shape[1], rows), jnp.int32),
            pltpu.VMEM((expert_ids.shape[1], rows), f32),
            pltpu.VMEM((1, width), f32),
            pltpu.VMEM((2, half, width), bf16),
            pltpu.VMEM((n, half, width), bf16),
            pltpu.VMEM((half, width), bf16),
            pltpu.VMEM((n, 1, rows), f32),
            pltpu.VMEM((n, 1, rows), f32),
            pltpu.VMEM((2, width, ff), bf16),
            pltpu.VMEM((2, width, ff), bf16),
            pltpu.VMEM((2, ff, width), bf16),
            pltpu.VMEM((width, share), bf16),
            pltpu.VMEM((width, share), bf16),
            pltpu.VMEM((share * tp_count, quarter), bf16),
            pltpu.VMEM((tp_count, 2, half, share), bf16),
            pltpu.VMEM((2, half, quarter), f32),
            pltpu.VMEM((n, half, keep), f32),
            pltpu.VMEM((n, half, 2 * tail), f32),
            pltpu.VMEM((n, half, 2 * both_keep), f32),
            pltpu.VMEM((n, half, keep), bf16),
            pltpu.VMEM((n, half, keep), bf16),
            pltpu.VMEM((major, half, keep), bf16),
            pltpu.VMEM((major, half, keep), bf16),
            pltpu.VMEM((major, half, 2 * both_keep), bf16),
            pltpu.VMEM((major, half, 2 * both_keep), bf16),
            pltpu.VMEM((major, half, keep), bf16),
            pltpu.VMEM((3, major, half, keep), bf16),
            pltpu.VMEM((n, half, 2 * tail), bf16),
            pltpu.VMEM((2, n, half, 2 * tail), bf16),
            pltpu.VMEM((major, half, 2 * both_keep), bf16),
            pltpu.VMEM((3, major, half, 2 * both_keep), bf16),
            pltpu.VMEM((3, half, tail), bf16),
            pltpu.VMEM((3, half, tail), bf16),
            pltpu.VMEM((half, both_keep), bf16),
            pltpu.VMEM((half, both_keep), bf16),
            pltpu.VMEM((2, half, quarter), f32),
            pltpu.VMEM((half, quarter), f32),
            pltpu.VMEM((half, tail), f32),
            pltpu.VMEM((half, both_keep), f32),
            pltpu.VMEM((half, keep), f32),
            pltpu.VMEM((half, 2 * tail), f32),
            pltpu.VMEM((half, 2 * both_keep), f32),
            dma((12,)), dma((n,)), dma((n,)), dma((3,)), dma((3,)), dma((tp_count,)), dma((tp_count,)), dma,
            dma((n,)), dma((n,)), dma((n,)), dma((n,)), dma((n,)), dma((n,)), dma((n,)), dma((n,)), dma((n,)),
            dma((n,)), dma((n,)), dma((n,)), dma((n,)), dma((n,)), dma((n,)),
            dma((n,)), dma((n,)), dma((major,)), dma((major,)), dma((major,)), dma((major,)),
            dma((major,)), dma((3, major)), dma((n,)), dma((2, n)), dma((major,)), dma((3, major)),
            dma((3,)), dma((3,)), dma, dma, dma, dma,
        ],
        compiler_params=pltpu.CompilerParams(
            collective_id=0, has_side_effects=True, vmem_limit_bytes=60 << 20
        ),
        name="dense_moe",
    )(
        expert_ids.T, route_weights.T, norm_gain.reshape(1, width), tokens,
        expert_gate[0], expert_up[0], expert_down[0],
        shared_gate, shared_up, shared_down,
    )


def local(tokens, *rest):
    ep_count = lax.axis_size("ep")
    pair_count = lax.axis_size("tp") // 2
    dense_bytes = 4 * ep_count * tokens.size * tokens.dtype.itemsize
    minor = 1 << (ep_count.bit_length() - 1) // 2
    if pair_count == 2 and minor == 2 and dense_bytes <= 24 << 20:
        return dense_exchange(tokens, *rest)
    return routed_exchange(tokens, *rest)


def solution(mesh):
    return jax.shard_map(
        local,
        mesh=mesh,
        in_specs=(
            P("ep", None),
            P(),
            P("ep", None),
            P("ep", None),
            P(("ep", "tp"), None, None),
            P(("ep", "tp"), None, None),
            P(("ep", "tp"), None, None),
            P(None, "tp"),
            P(None, "tp"),
            P(None, "tp"),
        ),
        out_specs=P("ep", "tp"),
        check_vma=False,
    )
```

```python
import functools

import jax
import jax.numpy as jnp
from jax import lax
from jax.experimental import pallas as pl
from jax.experimental.pallas import tpu as pltpu
from jax.sharding import PartitionSpec as P

NORM_EPSILON = 1e-06


def swapped(block, axis, distance):
    count = lax.axis_size(axis)
    route = []
    for low in range(count):
        high = low | 1 << distance
        if high != low and high < count:
            route += [(low, high), (high, low)]
    return lax.ppermute(block, axis, route)


def routed_exchange(
    tokens,
    norm_gain,
    expert_ids,
    route_weights,
    expert_gate,
    expert_up,
    expert_down,
    shared_gate,
    shared_up,
    shared_down,
):
    ep_count = lax.axis_size("ep")
    tp_count = lax.axis_size("tp")
    pair_count = tp_count // 2
    tp_index = lax.axis_index("tp")
    column = tp_index // 2
    half_index = tp_index % 2
    token_count, model_width = tokens.shape
    top_count = expert_ids.shape[1]
    expert_count = ep_count * pair_count
    capacity = 2 * max(1, token_count * top_count // expert_count)
    half_cap = capacity // 2
    as_float = tokens.astype(jnp.float32)
    inverse_rms = lax.rsqrt(jnp.mean(as_float * as_float, axis=-1, keepdims=True) + NORM_EPSILON)
    normed = (as_float * inverse_rms * norm_gain).astype(jnp.bfloat16)
    expert_iota = jnp.arange(expert_count, dtype=jnp.int32)
    token_iota = jnp.arange(token_count, dtype=jnp.int32)
    counts = jnp.sum(
        (expert_ids[:, :, None] == expert_iota[None, None, :]).astype(jnp.bfloat16), axis=1
    )
    strict_lower = (token_iota[:, None] > token_iota[None, :]).astype(jnp.bfloat16)
    prefix = jnp.dot(strict_lower, counts, preferred_element_type=jnp.float32)
    slot_index = jnp.take_along_axis(prefix, expert_ids, axis=1).astype(jnp.int32)
    target = expert_ids // pair_count
    owner_column = expert_ids % pair_count
    is_mine = owner_column == column
    position = target * capacity + slot_index
    slot_iota = jnp.arange(ep_count * capacity, dtype=jnp.int32)
    matches = is_mine[None, :, :] & (position[None, :, :] == slot_iota[:, None, None])
    slot_taken = jnp.any(matches, axis=2)
    token_of_slot = jnp.sum(jnp.where(slot_taken, token_iota[None, :], 0), axis=1)
    filled = jnp.any(slot_taken, axis=1)
    buffer = jnp.where(
        filled[:, None], jnp.take(normed, token_of_slot, axis=0), jnp.zeros((), jnp.bfloat16)
    )
    buffer = buffer.reshape(ep_count, capacity, model_width)
    gate_local = expert_gate[0]
    up_local = expert_up[0]
    down_local = expert_down[0]
    received = lax.all_to_all(buffer, "ep", split_axis=0, concat_axis=0, tiled=True)
    flat_rows = received.reshape(-1, model_width)
    hidden = (
        jax.nn.silu(jnp.dot(flat_rows, gate_local, preferred_element_type=jnp.float32))
        * jnp.dot(flat_rows, up_local, preferred_element_type=jnp.float32)
    ).astype(jnp.bfloat16)
    partial_out = jnp.dot(hidden, down_local, preferred_element_type=jnp.float32).astype(
        jnp.bfloat16
    )
    partial_out = partial_out.reshape(received.shape[0], received.shape[1], model_width)
    kept_part = lax.dynamic_slice_in_dim(partial_out, half_index * half_cap, half_cap, 1)
    other_part = lax.dynamic_slice_in_dim(partial_out, (1 - half_index) * half_cap, half_cap, 1)
    partner_part = swapped(other_part, "tp", 0)
    expert_out = (kept_part.astype(jnp.float32) + partner_part.astype(jnp.float32)).astype(
        jnp.bfloat16
    )
    returned = lax.all_to_all(expert_out, "ep", split_axis=0, concat_axis=0, tiled=True)
    row_total = ep_count * half_cap
    flat_rows = returned.reshape(row_total, model_width).astype(jnp.float32)
    is_valid = is_mine & (slot_index // half_cap == half_index)
    row_index = jnp.where(is_valid, target * half_cap + slot_index % half_cap, -1)
    row_iota = jnp.arange(row_total, dtype=jnp.int32)
    hits = row_index[:, :, None] == row_iota[None, None, :]
    combine_table = jnp.sum(jnp.where(hits, route_weights[:, :, None], 0.0), axis=1)
    partial_routed = jnp.dot(
        combine_table,
        flat_rows,
        precision=lax.Precision.HIGHEST,
        preferred_element_type=jnp.float32,
    )
    routed = lax.psum_scatter(partial_routed, "tp", scatter_dimension=1, tiled=True)
    shared_act = (
        jax.nn.silu(jnp.dot(normed, shared_gate, preferred_element_type=jnp.float32))
        * jnp.dot(normed, shared_up, preferred_element_type=jnp.float32)
    ).astype(jnp.bfloat16)
    shared_out = jnp.dot(
        lax.all_gather(shared_act, "tp", axis=1, tiled=True),
        shared_down,
        preferred_element_type=jnp.float32,
    )
    return (routed + shared_out).astype(jnp.bfloat16)


MESH = pl.DeviceIdType.MESH
LANES = 128
BOTH_KEEP = 2
WIDE = 2
NEAR = 4


def silu(v):
    return v / (1.0 + jnp.exp(-v))


FIELD = 16
KINDS = ("a", "c", "b", "x", "k", "t", "r", "w", "s", "zb", "zc", "za", "f1", "f2", "f3", "-")
OUTER = [
    ("a", 2), ("c", 2), ("b", 1), ("x", 1), ("a", 4), ("x", 3), ("w", 0), ("k", 0, 1), ("b", 3), ("a", 6), ("x", 5),
    ("c", 4), ("b", 2), ("t", 1), ("k", 2), ("k", 3), ("b", 5), ("zb", 0), ("b", 4), ("c", 6), ("x", 7), ("k", 4, 5),
    ("zb", 1), ("r", 3), ("s", 0), ("t", 0), ("b", 7), ("r", 1), ("zc", 1), ("b", 6), ("k", 6, 7), ("zb", 2),
    ("r", 5), ("zc", 2), ("r", 7), ("za", 1), ("zc", 0), ("za", 2), ("f1", 0), ("za", 0), ("f2", 0), ("f3", 0),
]
INNER = [
    ("a", 4), ("a", 2), ("b", 1), ("c", 2), ("a", 6), ("x", 1), ("c", 4), ("b", 3), ("b", 4), ("b", 5), ("c", 6),
    ("x", 3), ("x", 7), ("b", 2), ("x", 5), ("b", 6), ("b", 7), ("w", 0), ("k", 1, 7), ("k", 6), ("zb", 1), ("s", 0),
    ("k", 0, 2), ("zc", 1), ("t", 1), ("r", 7), ("k", 3, 5), ("k", 4), ("t", 0), ("zb", 0), ("zb", 2), ("zc", 2),
    ("r", 3), ("za", 1), ("r", 5), ("zc", 0), ("r", 1), ("za", 2), ("f1", 0), ("f2", 0), ("za", 0), ("f3", 0),
]
PLANS = {4: (OUTER, INNER)}


def dense_kernel(
    ep_count, tp_count, minor, near, wide, keep, both_keep, plans,
    ids_hbm, rw_hbm, gain_hbm, tok_hbm, gate_hbm, up_hbm, down_hbm, sg_hbm, su_hbm, sd_hbm,
    out_ref,
    ids_ref, rw_ref, gain_ref, tok, xb, xo, wtab, wr, wg, wu, wd, sg, su, sd, sh_all, sh_out,
    pa, pb, pc, xs, xr, ys, yr, ycs, ycr, zas, zar, zbs, zbr, zcs, zcr, fs, fr, gs, gr, head, head_in, last_b, last_m, acc_a, acc_b, acc_c,
    load_sem, wt_s, wt_r, we_s, we_r, sh_s, sh_r, yb_s,
    a_s, a_r, b_s, b_r, c_s, c_r, ya_s, ya_r, yc_s, xa_s, xa_r,
    rx_s, rx_r, ry_s, ry_r, ryc_s, ryc_r, rza_s, rza_r, rzb_s, rzb_r, rzc_s, rzc_r, f_s, f_r, g_s, g_r, o_s, o_r,
):
    n = ep_count
    major = n // minor
    half, width = xo.shape
    side = width // 2
    quarter = width // tp_count
    tail = side - keep - both_keep
    middle = keep + both_keep
    e = lax.axis_index("ep")
    t = lax.axis_index("tp")
    z = e // minor
    y = e % minor
    xi = t // 2
    c = t % 2
    t2 = 2 * (1 - xi) + c
    other_y = z * minor + 1 - y
    mate_x = {"tp": t2}
    mate_c = {"tp": 2 * xi + 1 - c}
    mate_y = {"ep": other_y}
    owner = 2 * xi + 1
    far_owner = 2 * (1 - xi) + 1
    z_up = {"ep": lax.rem(e + minor, n)}
    z_down = {"ep": lax.rem(e + n - minor, n)}
    far = {"ep": (major - 1 - z) * minor + y}
    is_end = (z == 0) | (z == major - 1)

    barrier = pltpu.get_barrier_semaphore()
    for k in range(1, n):
        pl.semaphore_signal(barrier, inc=1, device_id={"ep": lax.rem(e + k, n)}, device_id_type=MESH)
    for k in range(1, tp_count):
        pl.semaphore_signal(barrier, inc=1, device_id={"tp": lax.rem(t + k, tp_count)}, device_id_type=MESH)
    for k in range(1, tp_count):
        there = {"ep": other_y, "tp": lax.rem(t + k, tp_count)}
        pl.semaphore_signal(barrier, inc=1, device_id=there, device_id_type=MESH)

    def remote(src, dst, s, r, who):
        return pltpu.make_async_remote_copy(
            src_ref=src, dst_ref=dst, send_sem=s, recv_sem=r, device_id=who, device_id_type=MESH
        )

    def rows_of(which):
        return pl.ds(pl.multiple_of(which * half, half), half)

    def side_of(which):
        return pl.ds(pl.multiple_of(which * side, side), side)

    loads = [
        pltpu.make_async_copy(a, b, load_sem.at[i])
        for i, (a, b) in enumerate(
            (
                (tok_hbm.at[rows_of(c)], tok.at[0]),
                (tok_hbm.at[rows_of(1 - c)], tok.at[1]),
                (gate_hbm, wg.at[c]),
                (up_hbm, wu.at[c]),
                (down_hbm.at[:, side_of(xi)], wd.at[c, :, pl.ds(0, side)]),
                (down_hbm.at[:, side_of(1 - xi)], wd.at[c, :, pl.ds(side, side)]),
                (sg_hbm, sg),
                (su_hbm, su),
                (sd_hbm, sd),
                (gain_hbm, gain_ref),
                (ids_hbm, ids_ref),
                (rw_hbm, rw_ref),
            )
        )
    ]
    for i in (0, 9, 10, 11, 2, 3, 4, 5, 1, 6, 7, 8):
        loads[i].start()

    step = 16

    def norm_into(which, store):
        def body(i, carry):
            part = pl.ds(pl.multiple_of(i * step, step), step)
            v = tok[which, part, :].astype(jnp.float32)
            r = lax.rsqrt(jnp.mean(v * v, axis=-1, keepdims=True) + NORM_EPSILON)
            store(part, (v * r * gain_ref[...]).astype(jnp.bfloat16))
            return carry

        lax.fori_loop(0, half // step, body, 0)

    def store_own(part, value):
        xb[e, part, :] = value

    def store_rest(part, value):
        xo[part, :] = value

    def weights_for(expert):
        row = jnp.zeros((1, ids_ref.shape[1]), jnp.float32)
        for k in range(ids_ref.shape[0]):
            row += jnp.where(ids_ref[k : k + 1, :] == expert, rw_ref[k : k + 1, :], 0.0)
        return row

    loads[0].wait()
    loads[9].wait()
    norm_into(0, store_own)
    loads[10].wait()
    loads[11].wait()
    for d in range(n):
        wtab[d] = weights_for(d * (tp_count // 2) + xi)
    wr[e] = weights_for(e * (tp_count // 2) + xi)
    pl.semaphore_wait(barrier, n - 1 + 2 * (tp_count - 1))

    mine = pl.ds(pl.multiple_of(xi * near, LANES), near)
    theirs = pl.ds(pl.multiple_of((1 - xi) * near, LANES), near)
    shared_cols = pl.ds(2 * near, wide)
    rest = pl.ds(2 * near + wide, width - 2 * near - wide)

    def line_a(g, who):
        ref = xb.at[g, :, mine]
        return remote(ref, ref, a_s, a_r.at[g // minor], who)

    def line_b(g, who):
        ref = xb.at[g, :, rest]
        return remote(ref, ref, b_s, b_r.at[g], who)

    def line_c(g, who):
        ref = xb.at[g, :, shared_cols]
        return remote(ref, ref, c_s, c_r.at[g // minor], who)

    def y_shared(g):
        ref = xb.at[g, :, shared_cols]
        return remote(ref, ref, yc_s, xa_r.at[g], mate_y)

    def y_first():
        ref = xb.at[e, :, rest]
        return remote(ref, ref, yb_s, b_r.at[e], mate_y)

    def y_copy(g):
        ref = xb.at[g, :, mine]
        return remote(ref, ref, ya_s, ya_r.at[g // minor], mate_y)

    def x_copy(g):
        ref = xb.at[g, :, mine]
        return remote(ref, ref, xa_s, xa_r.at[g], mate_x)

    def x_arrival(g):
        ref = xb.at[g, :, theirs]
        return remote(ref, ref, xa_s, xa_r.at[g], mate_x)

    def cross_arrival(g):
        ref = xb.at[g, :, pl.ds(0, near + wide)]
        return remote(ref, ref, xa_s, xa_r.at[g], mate_x)

    def wt_copy(target):
        return remote(wtab.at[target], wr.at[e], wt_s, wt_r, {"ep": target})

    def wt_all():
        return remote(wtab.at[pl.ds(0, n - 1)], wr.at[pl.ds(0, n - 1)], wt_s, wt_r, mate_y)

    def weight_copy(i, which):
        ref = (wg, wu, wd)[i].at[which]
        return remote(ref, ref, we_s.at[i], we_r.at[i], mate_c)

    def sh_copy(who):
        return remote(sh_all.at[t], sh_all.at[t], sh_s, sh_r, {"tp": who})

    def sh_rest():
        ref = sh_all.at[pl.ds(0, tp_count - 1)]
        return remote(ref, ref, sh_s, sh_r, mate_c)

    def order(j):
        k = jnp.minimum(z, major - 1 - z)
        d = (j + 1) // 2
        close = jnp.where((j % 2 == 1) == (2 * z < major), z - d, z + d)
        far = jnp.where(z <= major - 1 - z, j, major - 1 - j)
        return jnp.where(j <= 2 * k, close, far)

    def slot_group(i):
        p = order(i // 2)
        yy = jnp.where(i % 2 == 0, y, 1 - y)
        return p, p * minor + yy

    def ups(p):
        return (p <= z) & (z < major - 1)

    def downs(p):
        return (p >= z) & (z > 0)

    def forward(p, g, line):
        @pl.when(ups(p))
        def _():
            line(g, z_up).start()

        @pl.when(downs(p))
        def _():
            line(g, z_down).start()

    for k in range(1, n):
        wt_copy(lax.rem(e + k, n)).start()
    forward(z, e, line_a)
    y_first().start()
    forward(z, e, line_c)
    y_copy(e).start()
    y_shared(e).start()
    forward(z, e, line_b)
    loads[2].wait()
    weight_copy(0, c).start()
    loads[3].wait()
    weight_copy(1, c).start()
    loads[4].wait()
    loads[5].wait()
    weight_copy(2, c).start()
    loads[1].wait()
    norm_into(1, store_rest)
    loads[6].wait()
    loads[7].wait()

    def shared_in(x):
        g_sum = jnp.dot(x, sg[...], preferred_element_type=jnp.float32)
        u_sum = jnp.dot(x, su[...], preferred_element_type=jnp.float32)
        return (silu(g_sum) * u_sum).astype(jnp.bfloat16)

    sh_all[t, c] = shared_in(xb[e])
    sh_all[t, 1 - c] = shared_in(xo[...])
    for k in range(1, tp_count):
        sh_copy(lax.rem(t + k, tp_count)).start()

    def rx_copy(g):
        return remote(xs.at[g], xr.at[g], rx_s, rx_r.at[g], mate_x)

    def ry_copy(p):
        return remote(ys.at[p], yr.at[p], ry_s, ry_r.at[p], mate_y)

    def ryc_copy(p):
        return remote(ycs.at[p], ycr.at[p], ryc_s, ryc_r.at[p], mate_y)

    def rzc_copy(p, slot, who):
        return remote(zcs.at[p], zcr.at[slot], rzc_s, rzc_r.at[slot], who)

    def rza_copy(p, slot, who):
        return remote(zas.at[p], zar.at[slot], rza_s, rza_r.at[slot], who)

    def rzb_copy(g, slot, who):
        return remote(zbs.at[g], zbr.at[slot], rzb_s, rzb_r.at[slot], who)

    def down_slot(key, p, to, count, extra):
        return jnp.where(p == to, count + extra, key)

    diagonal = lax.broadcasted_iota(jnp.int32, (half, 2 * half), 1) == (
        lax.broadcasted_iota(jnp.int32, (half, 2 * half), 0) + c * half
    )

    def weight_of(g):
        return jnp.sum(jnp.where(diagonal, wr[g], 0.0), axis=1, keepdims=True)

    def compute(i, j, first, second, both):
        pair = ((i, first), (j, second))
        weight = jnp.concatenate([weight_of(first), weight_of(second)], axis=0)
        x = jnp.concatenate([xb[first], xb[second]], axis=0)
        acts = []
        for h in range(2):
            g_sum = jnp.dot(x, wg[h], preferred_element_type=jnp.float32)
            u_sum = jnp.dot(x, wu[h], preferred_element_type=jnp.float32)
            acts.append((silu(g_sum) * u_sum).astype(jnp.bfloat16))

        def columns(low, high):
            total = jnp.dot(acts[0], wd[0, :, low:high], preferred_element_type=jnp.float32)
            total += jnp.dot(acts[1], wd[1, :, low:high], preferred_element_type=jnp.float32)
            return total * weight

        sent = columns(side, side + keep).astype(jnp.bfloat16)
        kept = columns(0, keep)
        kept_c = columns(keep, middle)
        rest_c = columns(side + keep, side + middle)
        main = columns(middle, side)
        rest = columns(side + middle, width)

        def put(k):
            index, g = pair[k]
            part = slice(k * half, (k + 1) * half)
            xs[g] = sent[part]

            @pl.when(index > 1)
            def _():
                rx_copy(g).start()

            pc[g, :, :both_keep] = kept_c[part]
            pc[g, :, both_keep:] = rest_c[part]

            @pl.when(index % 2 == 1)
            def _():
                p = g // minor
                ycs[p] = pc[g].astype(jnp.bfloat16)
                ryc_copy(p).start()

            pa[g] = kept[part]
            pb[g, :, :tail] = main[part]
            pb[g, :, tail:] = rest[part]

        put(0)

        @pl.when(both)
        def _():
            put(1)

    def add_lanes(p, acc, copy, key, received, extra=0, per=1):
        count = major * per
        below = downs(p) & jnp.logical_not((p == major - 1) & (z == 1))
        above = ups(p) & jnp.logical_not((p == 0) & (z == major - 2))

        def add(slot):
            copy(key, slot, z_up).wait_recv()
            acc[...] += received[slot].astype(jnp.float32)

        @pl.when(below)
        def _():
            add(key)

        @pl.when(above)
        def _():
            add(down_slot(key, p, z, count, extra))

        @pl.when((p == z) & is_end)
        def _():
            add(count + per + extra)

    def sum_b(p, g):
        acc_b[...] = pb[g]
        add_lanes(p, acc_b, rzb_copy, g, zbr, g % minor, minor)

    def sum_c(p, g):
        ryc_copy(p).wait_recv()
        acc_c[...] = pc[g] + ycr[p].astype(jnp.float32)
        add_lanes(p, acc_c, rzc_copy, p, zcr)

    def sum_a(p, g):
        rx_copy(g).wait_recv()
        ry_copy(p).wait_recv()
        acc_a[...] = pa[g] + xr[g].astype(jnp.float32) + yr[p].astype(jnp.float32)
        add_lanes(p, acc_a, rza_copy, p, zar)

    def line_order(q):
        above = major - 1 - z
        low = jnp.where(q < above, z + 1 + q, z - 1 - (q - above))
        high = jnp.where(q < z, z - 1 - q, z + 1 + (q - z))
        return jnp.where(2 * z < major, low, high)

    def send_sum(copy, key, p, extra=0, per=1):
        count = major * per
        whole = is_end & (p == major - 1 - z)

        @pl.when((p > z) & jnp.logical_not(whole))
        def _():
            copy(key, key, z_up).start()

        @pl.when((p < z) & jnp.logical_not(whole))
        def _():
            copy(key, down_slot(key, p, z - 1, count, extra), z_down).start()

        @pl.when(whole)
        def _():
            copy(key, count + per + extra, far).start()

    def do_a(i):
        p, g = slot_group(i)
        line_a(g, z_up).wait_recv()
        forward(p, g, line_a)
        y_copy(g).start()
        x_copy(g).start()

    def do_c(i):
        p, g = slot_group(i)
        line_c(g, z_up).wait_recv()
        forward(p, g, line_c)
        y_shared(g).start()

    def do_b(i):
        p, g = slot_group(i)
        line_b(g, z_up).wait_recv()
        forward(p, g, line_b)

    def do_x(i):
        _, g = slot_group(i)
        y_copy(g).wait_recv()
        x_copy(g).start()

    def do_k(code):
        i, j = code // FIELD, code % FIELD
        both = j < FIELD - 1
        _, first = slot_group(i)
        _, second = slot_group(jnp.where(both, j, i))

        def ready(index, g):
            @pl.when(index % 2 == 1)
            def _():
                cross_arrival(g).wait_recv()

            @pl.when(index % 2 == 0)
            def _():
                x_arrival(g).wait_recv()

        @pl.when(i > 0)
        def _():
            ready(i, first)

        @pl.when(both)
        def _():
            ready(j, second)

        compute(i, j, first, second, both)

    def do_w(_):
        for k in range(3):
            weight_copy(k, 1 - c).wait_recv()
        wt_all().wait_recv()

    def do_t(i):
        _, g = slot_group(i)
        rx_copy(g).start()

    def do_r(i):
        p, g = slot_group(i)
        rx_copy(g).wait_recv()
        ys[p] = (pa[g] + xr[g].astype(jnp.float32)).astype(jnp.bfloat16)
        ry_copy(p).start()

    def do_s(_):
        loads[8].wait()
        sh_rest().wait_recv()
        share = sg.shape[1]
        for r in range(2):
            shared = jnp.zeros((half, quarter), jnp.float32)
            for q in range(tp_count):
                shared += jnp.dot(
                    sh_all[q, r], sd[q * share : (q + 1) * share, :],
                    preferred_element_type=jnp.float32,
                )
            sh_out[r] = shared

    def do_zb(q):
        p = line_order(q)
        for yy in (1 - y, y):
            g = p * minor + yy
            sum_b(p, g)
            zbs[g] = acc_b[...].astype(jnp.bfloat16)
            send_sum(rzb_copy, g, p, g % minor, minor)

    def do_zc(q):
        p = line_order(q)
        sum_c(p, p * minor + y)
        zcs[p] = acc_c[...].astype(jnp.bfloat16)
        send_sum(rzc_copy, p, p)

    def do_za(q):
        p = line_order(q)
        sum_a(p, p * minor + y)
        zas[p] = acc_a[...].astype(jnp.bfloat16)
        send_sum(rza_copy, p, p)

    def last_copy(i):
        who = (
            {"ep": other_y, "tp": owner}, {"ep": other_y, "tp": far_owner}, {"tp": far_owner}, {"tp": owner},
        )[i]
        return remote(fs.at[i], fr.at[c, i], f_s, f_r.at[c], who)

    def last_c_copy(i):
        return remote(gs.at[i], gr.at[c, i], g_s, g_r.at[c], ({"tp": far_owner}, {"tp": owner})[i])

    def last_rows(which, count):
        b, m = fr.at[which, pl.ds(0, count + 2)], gr.at[which, pl.ds(0, count)]
        return remote(b, b, f_s, f_r.at[which], mate_c), remote(m, m, g_s, g_r.at[which], mate_c)

    head_copy = remote(head, head_in, o_s, o_r, mate_c)

    def do_f1(_):
        sum_b(z, other_y)
        fs[0] = acc_b[:, :tail].astype(jnp.bfloat16)
        fs[1] = acc_b[:, tail:].astype(jnp.bfloat16)
        last_copy(0).start()
        last_copy(1).start()

    def do_f2(_):
        sum_b(z, e)
        fs[2] = acc_b[:, tail:].astype(jnp.bfloat16)
        last_copy(2).start()
        last_b[...] = acc_b[:, :tail]

        @pl.when(c == 0)
        def _():
            fs[3] = acc_b[:, :tail].astype(jnp.bfloat16)
            last_copy(3).start()

    def do_f3(_):
        sum_c(z, e)
        gs[0] = acc_c[:, both_keep:].astype(jnp.bfloat16)
        last_c_copy(0).start()
        last_m[...] = acc_c[:, :both_keep]

        @pl.when(c == 0)
        def _():
            gs[1] = acc_c[:, :both_keep].astype(jnp.bfloat16)
            last_c_copy(1).start()

    actions = (
        (do_a, do_c, do_b, do_x, do_k, do_t, do_r, do_w),
        (do_s, do_zb, do_zc, do_za, do_f1, do_f2, do_f3),
    )

    block = 8
    codes = [jnp.where(is_end, outer, inner) for outer, inner in zip(*plans)]
    codes += [codes[-1] * 0 + FIELD * FIELD * 15] * (-len(codes) % block)

    def main_block(b, carry):
        held = codes[:block]
        for k in range(block, len(codes), block):
            held = [jnp.where(b == k // block, new, old) for new, old in zip(codes[k : k + block], held)]

        def main_step(i, carry):
            code = held[0]
            for k in range(1, block):
                code = jnp.where(i == k, held[k], code)
            kind = code // (FIELD * FIELD)
            arg = code % (FIELD * FIELD)
            for part, group in enumerate(actions):

                @pl.when(kind // 8 == part)
                def _(group=group):
                    for a, action in enumerate(group):

                        @pl.when(kind % 8 == a)
                        def _(action=action):
                            action(arg)

            return carry

        return lax.fori_loop(0, block, main_step, carry)

    lax.fori_loop(0, len(codes) // block, main_block, 0)

    sum_a(z, e)

    def total(ref):
        return sum(ref[i].astype(jnp.float32) for i in range(1, ref.shape[0])) + ref[0].astype(jnp.float32)

    @pl.when(c == 0)
    def _():
        out_ref[:half, :] = (acc_a[...] + sh_out[0]).astype(jnp.bfloat16)
        head_copy.wait_recv()
        out_ref[half:, :] = (head_in[...] + sh_out[1]).astype(jnp.bfloat16)
        for copy in last_rows(0, 2):
            copy.wait_send()

    @pl.when(c == 1)
    def _():
        head[...] = acc_a[...]
        head_copy.start()
        for copy in last_rows(1, 1):
            copy.wait_recv()
        low, high = slice(0, both_keep), slice(both_keep, quarter)
        out_ref[half:, low] = (last_m[...] + gr[1, 0].astype(jnp.float32) + sh_out[1, :, low]).astype(jnp.bfloat16)
        out_ref[half:, high] = (last_b[...] + total(fr.at[1, pl.ds(0, 3)]) + sh_out[1, :, high]).astype(jnp.bfloat16)
        for copy in last_rows(0, 2):
            copy.wait_recv()
        out_ref[:half, low] = (total(gr.at[0]) + sh_out[0, :, low]).astype(jnp.bfloat16)
        out_ref[:half, high] = (total(fr.at[0]) + sh_out[0, :, high]).astype(jnp.bfloat16)
        for copy in last_rows(1, 1):
            copy.wait_send()
        head_copy.wait_send()

    for i in range(3):
        weight_copy(i, c).wait_send()
    y_first().wait_send()
    wt_all().wait_send()
    sh_rest().wait_send()

    def drained(ref, sem):
        remote(ref, ref, sem, a_r.at[0], mate_c).wait_send()

    def lines_sent(count):
        groups = pl.ds(0, count)
        drained(xb.at[groups, :, pl.ds(0, near)], a_s)
        drained(xb.at[groups, :, pl.ds(0, wide)], c_s)
        drained(xb.at[groups, :, pl.ds(0, 2 * (width - 2 * near - wide))], b_s)

    @pl.when(is_end)
    def _():
        lines_sent(1)

    @pl.when(jnp.logical_not(is_end))
    def _():
        lines_sent(major + 1)

    drained(xb.at[pl.ds(0, major), :, pl.ds(0, near)], ya_s)
    drained(xb.at[pl.ds(0, major), :, pl.ds(0, wide)], yc_s)
    drained(xb.at[pl.ds(0, n - 1), :, pl.ds(0, near)], xa_s)
    drained(xs, rx_s)
    drained(ys, ry_s)
    drained(ycs, ryc_s)
    drained(zas.at[pl.ds(0, major - 1)], rza_s)
    drained(zcs.at[pl.ds(0, major - 1)], rzc_s)
    drained(zbs.at[pl.ds(0, n - minor)], rzb_s)


def coded(plan):
    codes = []
    for kind, first, *second in plan:
        arg = first * FIELD + (second[0] if second else FIELD - 1) if kind == "k" else first
        codes.append((KINDS.index(kind) * FIELD * FIELD) + arg)
    return codes


def dense_exchange(
    tokens, norm_gain, expert_ids, route_weights, expert_gate, expert_up, expert_down,
    shared_gate, shared_up, shared_down,
):
    n = lax.axis_size("ep")
    tp_count = lax.axis_size("tp")
    minor = 1 << (n.bit_length() - 1) // 2
    major = n // minor
    rows, width = tokens.shape
    half = rows // 2
    side = width // 2
    quarter = width // tp_count
    near = side * NEAR // 8 // LANES * LANES
    wide = 2 * (side * WIDE // 8 // LANES * LANES)
    keep = quarter
    both_keep = side * BOTH_KEEP // 8 // LANES * LANES
    tail = side - keep - both_keep
    ff = expert_gate.shape[2]
    share = shared_gate.shape[1]
    bf16, f32 = jnp.bfloat16, jnp.float32
    dma = pltpu.SemaphoreType.DMA
    vmem = pl.BlockSpec(memory_space=pltpu.VMEM)
    anywhere = pl.BlockSpec(memory_space=pl.ANY)
    return pl.pallas_call(
        functools.partial(dense_kernel, n, tp_count, minor, near, wide, keep, both_keep, [coded(plan) for plan in PLANS[n // minor]]),
        out_shape=pltpu.VMEM((rows, quarter), bf16),
        in_specs=[anywhere] * 10,
        out_specs=vmem,
        scratch_shapes=[
            pltpu.VMEM((expert_ids.shape[1], rows), jnp.int32),
            pltpu.VMEM((expert_ids.shape[1], rows), f32),
            pltpu.VMEM((1, width), f32),
            pltpu.VMEM((2, half, width), bf16),
            pltpu.VMEM((n, half, width), bf16),
            pltpu.VMEM((half, width), bf16),
            pltpu.VMEM((n, 1, rows), f32),
            pltpu.VMEM((n, 1, rows), f32),
            pltpu.VMEM((2, width, ff), bf16),
            pltpu.VMEM((2, width, ff), bf16),
            pltpu.VMEM((2, ff, width), bf16),
            pltpu.VMEM((width, share), bf16),
            pltpu.VMEM((width, share), bf16),
            pltpu.VMEM((share * tp_count, quarter), bf16),
            pltpu.VMEM((tp_count, 2, half, share), bf16),
            pltpu.VMEM((2, half, quarter), f32),
            pltpu.VMEM((n, half, keep), f32),
            pltpu.VMEM((n, half, 2 * tail), f32),
            pltpu.VMEM((n, half, 2 * both_keep), f32),
            pltpu.VMEM((n, half, keep), bf16),
            pltpu.VMEM((n, half, keep), bf16),
            pltpu.VMEM((major, half, keep), bf16),
            pltpu.VMEM((major, half, keep), bf16),
            pltpu.VMEM((major, half, 2 * both_keep), bf16),
            pltpu.VMEM((major, half, 2 * both_keep), bf16),
            pltpu.VMEM((major, half, keep), bf16),
            pltpu.VMEM((major + 2, half, keep), bf16),
            pltpu.VMEM((n, half, 2 * tail), bf16),
            pltpu.VMEM((n + 2 * minor, half, 2 * tail), bf16),
            pltpu.VMEM((major, half, 2 * both_keep), bf16),
            pltpu.VMEM((major + 2, half, 2 * both_keep), bf16),
            pltpu.VMEM((4, half, tail), bf16),
            pltpu.VMEM((2, 4, half, tail), bf16),
            pltpu.VMEM((2, half, both_keep), bf16),
            pltpu.VMEM((2, 2, half, both_keep), bf16),
            pltpu.VMEM((half, quarter), f32),
            pltpu.VMEM((half, quarter), f32),
            pltpu.VMEM((half, tail), f32),
            pltpu.VMEM((half, both_keep), f32),
            pltpu.VMEM((half, keep), f32),
            pltpu.VMEM((half, 2 * tail), f32),
            pltpu.VMEM((half, 2 * both_keep), f32),
            dma((12,)), dma, dma, dma((3,)), dma((3,)), dma, dma, dma,
            dma, dma((major,)), dma, dma((n,)), dma, dma((major,)), dma, dma((major,)), dma, dma, dma((n,)),
            dma, dma((n,)), dma, dma((major,)), dma, dma((major,)), dma, dma((major + 2,)),
            dma, dma((n + 2 * minor,)), dma, dma((major + 2,)), dma, dma((2,)), dma, dma((2,)), dma, dma,
        ],
        compiler_params=pltpu.CompilerParams(
            collective_id=0, has_side_effects=True, vmem_limit_bytes=60 << 20
        ),
        name="dense_moe",
    )(
        expert_ids.T, route_weights.T, norm_gain.reshape(1, width), tokens,
        expert_gate[0], expert_up[0], expert_down[0],
        shared_gate, shared_up, shared_down,
    )


def local(tokens, *rest):
    ep_count = lax.axis_size("ep")
    pair_count = lax.axis_size("tp") // 2
    dense_bytes = 4 * ep_count * tokens.size * tokens.dtype.itemsize
    minor = 1 << (ep_count.bit_length() - 1) // 2
    if pair_count == 2 and minor == 2 and dense_bytes <= 24 << 20:
        return dense_exchange(tokens, *rest)
    return routed_exchange(tokens, *rest)


def solution(mesh):
    return jax.shard_map(
        local,
        mesh=mesh,
        in_specs=(
            P("ep", None),
            P(),
            P("ep", None),
            P("ep", None),
            P(("ep", "tp"), None, None),
            P(("ep", "tp"), None, None),
            P(("ep", "tp"), None, None),
            P(None, "tp"),
            P(None, "tp"),
            P(None, "tp"),
        ),
        out_specs=P("ep", "tp"),
        check_vma=False,
    )
```

```python
import functools

import jax
import jax.numpy as jnp
from jax import lax
from jax.experimental import pallas as pl
from jax.experimental.pallas import tpu as pltpu
from jax.sharding import PartitionSpec as P

NORM_EPSILON = 1e-06


def swapped(block, axis, distance):
    count = lax.axis_size(axis)
    route = []
    for low in range(count):
        high = low | 1 << distance
        if high != low and high < count:
            route += [(low, high), (high, low)]
    return lax.ppermute(block, axis, route)


def routed_exchange(
    tokens,
    norm_gain,
    expert_ids,
    route_weights,
    expert_gate,
    expert_up,
    expert_down,
    shared_gate,
    shared_up,
    shared_down,
):
    ep_count = lax.axis_size("ep")
    tp_count = lax.axis_size("tp")
    pair_count = tp_count // 2
    tp_index = lax.axis_index("tp")
    column = tp_index // 2
    half_index = tp_index % 2
    token_count, model_width = tokens.shape
    top_count = expert_ids.shape[1]
    expert_count = ep_count * pair_count
    capacity = 2 * max(1, token_count * top_count // expert_count)
    half_cap = capacity // 2
    as_float = tokens.astype(jnp.float32)
    inverse_rms = lax.rsqrt(jnp.mean(as_float * as_float, axis=-1, keepdims=True) + NORM_EPSILON)
    normed = (as_float * inverse_rms * norm_gain).astype(jnp.bfloat16)
    expert_iota = jnp.arange(expert_count, dtype=jnp.int32)
    token_iota = jnp.arange(token_count, dtype=jnp.int32)
    counts = jnp.sum(
        (expert_ids[:, :, None] == expert_iota[None, None, :]).astype(jnp.bfloat16), axis=1
    )
    strict_lower = (token_iota[:, None] > token_iota[None, :]).astype(jnp.bfloat16)
    prefix = jnp.dot(strict_lower, counts, preferred_element_type=jnp.float32)
    slot_index = jnp.take_along_axis(prefix, expert_ids, axis=1).astype(jnp.int32)
    target = expert_ids // pair_count
    owner_column = expert_ids % pair_count
    is_mine = owner_column == column
    position = target * capacity + slot_index
    slot_iota = jnp.arange(ep_count * capacity, dtype=jnp.int32)
    matches = is_mine[None, :, :] & (position[None, :, :] == slot_iota[:, None, None])
    slot_taken = jnp.any(matches, axis=2)
    token_of_slot = jnp.sum(jnp.where(slot_taken, token_iota[None, :], 0), axis=1)
    filled = jnp.any(slot_taken, axis=1)
    buffer = jnp.where(
        filled[:, None], jnp.take(normed, token_of_slot, axis=0), jnp.zeros((), jnp.bfloat16)
    )
    buffer = buffer.reshape(ep_count, capacity, model_width)
    gate_local = expert_gate[0]
    up_local = expert_up[0]
    down_local = expert_down[0]
    received = lax.all_to_all(buffer, "ep", split_axis=0, concat_axis=0, tiled=True)
    flat_rows = received.reshape(-1, model_width)
    hidden = (
        jax.nn.silu(jnp.dot(flat_rows, gate_local, preferred_element_type=jnp.float32))
        * jnp.dot(flat_rows, up_local, preferred_element_type=jnp.float32)
    ).astype(jnp.bfloat16)
    partial_out = jnp.dot(hidden, down_local, preferred_element_type=jnp.float32).astype(
        jnp.bfloat16
    )
    partial_out = partial_out.reshape(received.shape[0], received.shape[1], model_width)
    kept_part = lax.dynamic_slice_in_dim(partial_out, half_index * half_cap, half_cap, 1)
    other_part = lax.dynamic_slice_in_dim(partial_out, (1 - half_index) * half_cap, half_cap, 1)
    partner_part = swapped(other_part, "tp", 0)
    expert_out = (kept_part.astype(jnp.float32) + partner_part.astype(jnp.float32)).astype(
        jnp.bfloat16
    )
    returned = lax.all_to_all(expert_out, "ep", split_axis=0, concat_axis=0, tiled=True)
    row_total = ep_count * half_cap
    flat_rows = returned.reshape(row_total, model_width).astype(jnp.float32)
    is_valid = is_mine & (slot_index // half_cap == half_index)
    row_index = jnp.where(is_valid, target * half_cap + slot_index % half_cap, -1)
    row_iota = jnp.arange(row_total, dtype=jnp.int32)
    hits = row_index[:, :, None] == row_iota[None, None, :]
    combine_table = jnp.sum(jnp.where(hits, route_weights[:, :, None], 0.0), axis=1)
    partial_routed = jnp.dot(
        combine_table,
        flat_rows,
        precision=lax.Precision.HIGHEST,
        preferred_element_type=jnp.float32,
    )
    routed = lax.psum_scatter(partial_routed, "tp", scatter_dimension=1, tiled=True)
    shared_act = (
        jax.nn.silu(jnp.dot(normed, shared_gate, preferred_element_type=jnp.float32))
        * jnp.dot(normed, shared_up, preferred_element_type=jnp.float32)
    ).astype(jnp.bfloat16)
    shared_out = jnp.dot(
        lax.all_gather(shared_act, "tp", axis=1, tiled=True),
        shared_down,
        preferred_element_type=jnp.float32,
    )
    return (routed + shared_out).astype(jnp.bfloat16)


MESH = pl.DeviceIdType.MESH
LANES = 128
BOTH_KEEP = 3
WIDE = 2
NEAR = 4


def silu(v):
    return v / (1.0 + jnp.exp(-v))


FIELD = 16
KINDS = ("a", "c", "b", "x", "k", "t", "r", "w", "s", "zb", "zc", "za", "f1", "f2", "f3", "-")
PLAN_0 = [
    ("x", 1), ("b", 1), ("a", 2), ("x", 3), ("c", 2), ("a", 4), ("a", 6), ("b", 4), ("x", 5), ("c", 4), ("b", 2),
    ("b", 3), ("w", 0), ("k", 3, 4), ("x", 7), ("c", 6), ("b", 5), ("k", 2, 5), ("zb", 1), ("zc", 0), ("b", 7),
    ("k", 0, 1), ("s", 0), ("b", 6), ("k", 6, 7), ("r", 5), ("zc", 1), ("t", 1), ("zb", 2), ("zb", 0), ("zc", 2),
    ("r", 7), ("r", 3), ("za", 1), ("t", 0), ("r", 1), ("za", 2), ("f3", 0), ("f1", 0), ("za", 0), ("f2", 0),
    ("-", 0),
]
PLAN_1 = [
    ("a", 2), ("c", 2), ("b", 1), ("a", 4), ("b", 4), ("a", 6), ("x", 3), ("c", 4), ("b", 2), ("b", 3), ("c", 6),
    ("x", 7), ("s", 0), ("x", 5), ("b", 5), ("x", 1), ("b", 7), ("w", 0), ("k", 4, 7), ("b", 6), ("k", 0, 3),
    ("k", 5, 6), ("r", 7), ("zc", 1), ("k", 1, 2), ("zb", 2), ("zb", 1), ("t", 1), ("r", 3), ("zb", 0), ("t", 0),
    ("za", 1), ("zc", 2), ("r", 5), ("r", 1), ("zc", 0), ("za", 2), ("f2", 0), ("za", 0), ("f1", 0), ("f3", 0),
    ("-", 0),
]
PLAN_2 = [
    ("a", 4), ("a", 2), ("c", 4), ("a", 6), ("c", 2), ("c", 6), ("b", 4), ("x", 5), ("b", 5), ("b", 1), ("x", 3),
    ("b", 3), ("b", 2), ("x", 7), ("w", 0), ("k", 4, 5), ("b", 7), ("b", 6), ("k", 6, 7), ("zb", 1), ("k", 3),
    ("k", 0, 2), ("r", 7), ("x", 1), ("zc", 1), ("za", 1), ("r", 5), ("zc", 2), ("r", 3), ("k", 1), ("zb", 2),
    ("zb", 0), ("s", 0), ("t", 1), ("zc", 0), ("t", 0), ("r", 1), ("za", 0), ("za", 2), ("f1", 0), ("f2", 0),
    ("f3", 0),
]
PLAN_3 = [
    ("c", 2), ("b", 1), ("x", 1), ("a", 2), ("a", 4), ("x", 3), ("c", 4), ("x", 5), ("a", 6), ("c", 6), ("x", 7),
    ("b", 2), ("b", 5), ("b", 4), ("w", 0), ("k", 4, 5), ("zb", 1), ("b", 7), ("k", 0, 7), ("r", 5), ("b", 6),
    ("zc", 1), ("k", 2, 6), ("zb", 2), ("r", 7), ("b", 3), ("zc", 2), ("k", 1, 3), ("t", 1), ("s", 0), ("za", 1),
    ("za", 2), ("zb", 0), ("r", 3), ("r", 1), ("zc", 0), ("t", 0), ("za", 0), ("f1", 0), ("f2", 0), ("f3", 0),
    ("-", 0),
]
PLANS = {4: (PLAN_0, PLAN_1, PLAN_2, PLAN_3)}


def dense_kernel(
    ep_count, tp_count, minor, near, wide, keep, both_keep, plans,
    ids_hbm, rw_hbm, gain_hbm, tok_hbm, gate_hbm, up_hbm, down_hbm, sg_hbm, su_hbm, sd_hbm,
    out_ref,
    ids_ref, rw_ref, gain_ref, tok, xb, xo, wtab, wr, wg, wu, wd, sg, su, sd, sh_all, sh_out,
    pa, pb, pc, xs, xr, ys, yr, ycs, ycr, zas, zar, zbs, zbr, zcs, zcr, fs, fr, gs, gr, head, head_in, last_b, last_m, acc_a, acc_b, acc_c,
    line_sem, load_sem, wt_s, wt_r, we_s, we_r, sh_s, sh_r, yb_s,
    a_s, a_r, b_s, b_r, c_s, c_r, ya_s, ya_r, yc_s, xa_s, xa_r,
    rx_s, rx_r, ry_s, ry_r, ryc_s, ryc_r, rza_s, rza_r, rzb_s, rzb_r, rzc_s, rzc_r, f_s, f_r, g_s, g_r, o_s, o_r,
):
    n = ep_count
    major = n // minor
    half, width = xo.shape
    side = width // 2
    quarter = width // tp_count
    tail = side - keep - both_keep
    middle = keep + both_keep
    e = lax.axis_index("ep")
    t = lax.axis_index("tp")
    z = e // minor
    y = e % minor
    xi = t // 2
    c = t % 2
    t2 = 2 * (1 - xi) + c
    other_y = z * minor + 1 - y
    mate_x = {"tp": t2}
    mate_c = {"tp": 2 * xi + 1 - c}
    mate_y = {"ep": other_y}
    owner = 2 * xi + 1
    far_owner = 2 * (1 - xi) + 1
    z_up = {"ep": lax.rem(e + minor, n)}
    z_down = {"ep": lax.rem(e + n - minor, n)}
    far = {"ep": (major - 1 - z) * minor + y}
    is_end = (z == 0) | (z == major - 1)

    barrier = pltpu.get_barrier_semaphore()

    def greet_line(sem):
        @pl.when(z < major - 1)
        def _():
            pl.semaphore_signal(sem, inc=1, device_id=z_up, device_id_type=MESH)

        @pl.when(z > 0)
        def _():
            pl.semaphore_signal(sem, inc=1, device_id=z_down, device_id_type=MESH)

    in_line = jnp.where(is_end, 1, 2)
    greet_line(barrier)
    for k in range(1, tp_count):
        pl.semaphore_signal(barrier, inc=1, device_id={"tp": lax.rem(t + k, tp_count)}, device_id_type=MESH)
    for k in range(tp_count):
        there = {"ep": other_y, "tp": lax.rem(t + k, tp_count)}
        pl.semaphore_signal(barrier, inc=1, device_id=there, device_id_type=MESH)

    def remote(src, dst, s, r, who):
        return pltpu.make_async_remote_copy(
            src_ref=src, dst_ref=dst, send_sem=s, recv_sem=r, device_id=who, device_id_type=MESH
        )

    def rows_of(which):
        return pl.ds(pl.multiple_of(which * half, half), half)

    def side_of(which):
        return pl.ds(pl.multiple_of(which * side, side), side)

    loads = [
        pltpu.make_async_copy(a, b, load_sem.at[i])
        for i, (a, b) in enumerate(
            (
                (tok_hbm.at[rows_of(c)], tok.at[0]),
                (tok_hbm.at[rows_of(1 - c)], tok.at[1]),
                (gate_hbm, wg.at[c]),
                (up_hbm, wu.at[c]),
                (down_hbm.at[:, side_of(xi)], wd.at[c, :, pl.ds(0, side)]),
                (down_hbm.at[:, side_of(1 - xi)], wd.at[c, :, pl.ds(side, side)]),
                (sg_hbm, sg),
                (su_hbm, su),
                (sd_hbm, sd),
                (gain_hbm, gain_ref),
                (ids_hbm, ids_ref),
                (rw_hbm, rw_ref),
            )
        )
    ]
    for i in (0, 9, 10, 11, 2, 3, 4, 5, 1, 6, 7, 8):
        loads[i].start()

    step = 16

    def norm_into(which, store):
        def body(i, carry):
            part = pl.ds(pl.multiple_of(i * step, step), step)
            v = tok[which, part, :].astype(jnp.float32)
            r = lax.rsqrt(jnp.mean(v * v, axis=-1, keepdims=True) + NORM_EPSILON)
            store(part, (v * r * gain_ref[...]).astype(jnp.bfloat16))
            return carry

        lax.fori_loop(0, half // step, body, 0, unroll=True)

    def store_own(part, value):
        xb[e, part, :] = value

    def store_rest(part, value):
        xo[part, :] = value

    def weights_for(expert):
        row = jnp.zeros((1, ids_ref.shape[1]), jnp.float32)
        for k in range(ids_ref.shape[0]):
            row += jnp.where(ids_ref[k : k + 1, :] == expert, rw_ref[k : k + 1, :], 0.0)
        return row

    loads[0].wait()
    loads[9].wait()
    norm_into(0, store_own)
    loads[10].wait()
    loads[11].wait()
    for d in range(n):
        wtab[d] = weights_for(d * (tp_count // 2) + xi)
    wr[e] = weights_for(e * (tp_count // 2) + xi)
    pl.semaphore_wait(barrier, 2 * tp_count - 1 + in_line)
    greet_line(line_sem.at[0])

    mine = pl.ds(pl.multiple_of(xi * near, LANES), near)
    theirs = pl.ds(pl.multiple_of((1 - xi) * near, LANES), near)
    shared_cols = pl.ds(2 * near, wide)
    rest = pl.ds(2 * near + wide, width - 2 * near - wide)

    def line_a(g, who):
        ref = xb.at[g, :, mine]
        return remote(ref, ref, a_s, a_r.at[g // minor], who)

    def line_b(g, who):
        ref = xb.at[g, :, rest]
        return remote(ref, ref, b_s, b_r.at[g], who)

    def line_c(g, who):
        ref = xb.at[g, :, shared_cols]
        return remote(ref, ref, c_s, c_r.at[g // minor], who)

    def y_shared(g):
        ref = xb.at[g, :, shared_cols]
        return remote(ref, ref, yc_s, xa_r.at[g], mate_y)

    def y_first():
        ref = xb.at[e, :, rest]
        return remote(ref, ref, yb_s, b_r.at[e], mate_y)

    def y_copy(g):
        ref = xb.at[g, :, mine]
        return remote(ref, ref, ya_s, ya_r.at[g // minor], mate_y)

    def x_copy(g):
        ref = xb.at[g, :, mine]
        return remote(ref, ref, xa_s, xa_r.at[g], mate_x)

    def x_arrival(g):
        ref = xb.at[g, :, theirs]
        return remote(ref, ref, xa_s, xa_r.at[g], mate_x)

    def cross_arrival(g):
        ref = xb.at[g, :, pl.ds(0, near + wide)]
        return remote(ref, ref, xa_s, xa_r.at[g], mate_x)

    def wt_copy(target):
        return remote(wtab.at[target], wr.at[e], wt_s, wt_r, {"ep": target})

    def wt_all():
        return remote(wtab.at[pl.ds(0, n - 1)], wr.at[pl.ds(0, n - 1)], wt_s, wt_r, mate_y)

    def weight_copy(i, which):
        ref = (wg, wu, wd)[i].at[which]
        return remote(ref, ref, we_s.at[i], we_r.at[i], mate_c)

    def sh_copy(who):
        return remote(sh_all.at[t], sh_all.at[t], sh_s, sh_r, {"tp": who})

    def sh_rest():
        ref = sh_all.at[pl.ds(0, tp_count - 1)]
        return remote(ref, ref, sh_s, sh_r, mate_c)

    def order(j):
        k = jnp.minimum(z, major - 1 - z)
        d = (j + 1) // 2
        close = jnp.where((j % 2 == 1) == (2 * z < major), z - d, z + d)
        far = jnp.where(z <= major - 1 - z, j, major - 1 - j)
        return jnp.where(j <= 2 * k, close, far)

    def slot_group(i):
        p = order(i // 2)
        yy = jnp.where(i % 2 == 0, y, 1 - y)
        return p, p * minor + yy

    def ups(p):
        return (p <= z) & (z < major - 1)

    def downs(p):
        return (p >= z) & (z > 0)

    def forward(p, g, line):
        @pl.when(ups(p))
        def _():
            line(g, z_up).start()

        @pl.when(downs(p))
        def _():
            line(g, z_down).start()

    forward(z, e, line_a)
    y_first().start()
    forward(z, e, line_c)
    y_copy(e).start()
    y_shared(e).start()
    forward(z, e, line_b)
    loads[2].wait()
    weight_copy(0, c).start()
    loads[3].wait()
    weight_copy(1, c).start()
    loads[4].wait()
    loads[5].wait()
    weight_copy(2, c).start()
    loads[1].wait()
    norm_into(1, store_rest)
    loads[6].wait()
    loads[7].wait()

    def shared_in(x):
        g_sum = jnp.dot(x, sg[...], preferred_element_type=jnp.float32)
        u_sum = jnp.dot(x, su[...], preferred_element_type=jnp.float32)
        return (silu(g_sum) * u_sum).astype(jnp.bfloat16)

    sh_all[t, c] = shared_in(xb[e])
    sh_all[t, 1 - c] = shared_in(xo[...])
    for k in range(1, tp_count):
        sh_copy(lax.rem(t + k, tp_count)).start()
    for k in range(major - 1):
        pl.semaphore_wait(line_sem.at[k], in_line)
        if k < major - 2:
            greet_line(line_sem.at[k + 1])
    for k in range(1, n):
        wt_copy(lax.rem(e + k, n)).start()

    def rx_copy(g):
        return remote(xs.at[g], xr.at[g], rx_s, rx_r.at[g], mate_x)

    def ry_copy(p):
        return remote(ys.at[p], yr.at[p], ry_s, ry_r.at[p], mate_y)

    def ryc_copy(p):
        return remote(ycs.at[p], ycr.at[p], ryc_s, ryc_r.at[p], mate_y)

    def rzc_copy(p, slot, who):
        return remote(zcs.at[p], zcr.at[slot], rzc_s, rzc_r.at[slot], who)

    def rza_copy(p, slot, who):
        return remote(zas.at[p], zar.at[slot], rza_s, rza_r.at[slot], who)

    def rzb_copy(g, slot, who):
        return remote(zbs.at[g], zbr.at[slot], rzb_s, rzb_r.at[slot], who)

    def down_slot(key, p, to, count, extra):
        return jnp.where(p == to, count + extra, key)

    diagonal = lax.broadcasted_iota(jnp.int32, (half, 2 * half), 1) == (
        lax.broadcasted_iota(jnp.int32, (half, 2 * half), 0) + c * half
    )

    def weight_of(g):
        return jnp.sum(jnp.where(diagonal, wr[g], 0.0), axis=1, keepdims=True)

    def compute(i, j, first, second, both):
        pair = ((i, first), (j, second))
        weight = jnp.concatenate([weight_of(first), weight_of(second)], axis=0)
        x = jnp.concatenate([xb[first], xb[second]], axis=0)
        acts = []
        for h in range(2):
            g_sum = jnp.dot(x, wg[h], preferred_element_type=jnp.float32)
            u_sum = jnp.dot(x, wu[h], preferred_element_type=jnp.float32)
            acts.append((silu(g_sum) * u_sum).astype(jnp.bfloat16))

        def columns(low, high):
            total = jnp.dot(acts[0], wd[0, :, low:high], preferred_element_type=jnp.float32)
            total += jnp.dot(acts[1], wd[1, :, low:high], preferred_element_type=jnp.float32)
            return total * weight

        sent = columns(side, side + keep).astype(jnp.bfloat16)
        kept = columns(0, keep)
        kept_c = columns(keep, middle)
        rest_c = columns(side + keep, side + middle)
        main = columns(middle, side)
        rest = columns(side + middle, width)

        def put(k):
            index, g = pair[k]
            part = slice(k * half, (k + 1) * half)
            xs[g] = sent[part]

            @pl.when(index > 1)
            def _():
                rx_copy(g).start()

            pc[g, :, :both_keep] = kept_c[part]
            pc[g, :, both_keep:] = rest_c[part]

            @pl.when(index % 2 == 1)
            def _():
                p = g // minor
                ycs[p] = pc[g].astype(jnp.bfloat16)
                ryc_copy(p).start()

            pa[g] = kept[part]
            pb[g, :, :tail] = main[part]
            pb[g, :, tail:] = rest[part]

        put(0)

        @pl.when(both)
        def _():
            put(1)

    def add_lanes(p, acc, copy, key, received, extra=0, per=1):
        count = major * per
        below = downs(p) & jnp.logical_not((p == major - 1) & (z == 1))
        above = ups(p) & jnp.logical_not((p == 0) & (z == major - 2))

        def add(slot):
            copy(key, slot, z_up).wait_recv()
            acc[...] += received[slot].astype(jnp.float32)

        @pl.when(below)
        def _():
            add(key)

        @pl.when(above)
        def _():
            add(down_slot(key, p, z, count, extra))

        @pl.when((p == z) & is_end)
        def _():
            add(count + per + extra)

    def sum_b(p, g):
        acc_b[...] = pb[g]
        add_lanes(p, acc_b, rzb_copy, g, zbr, g % minor, minor)

    def sum_c(p, g):
        ryc_copy(p).wait_recv()
        acc_c[...] = pc[g] + ycr[p].astype(jnp.float32)
        add_lanes(p, acc_c, rzc_copy, p, zcr)

    def sum_a(p, g):
        rx_copy(g).wait_recv()
        ry_copy(p).wait_recv()
        acc_a[...] = pa[g] + xr[g].astype(jnp.float32) + yr[p].astype(jnp.float32)
        add_lanes(p, acc_a, rza_copy, p, zar)

    def line_order(q):
        above = major - 1 - z
        low = jnp.where(q < above, z + 1 + q, z - 1 - (q - above))
        high = jnp.where(q < z, z - 1 - q, z + 1 + (q - z))
        return jnp.where(2 * z < major, low, high)

    def send_sum(copy, key, p, extra=0, per=1):
        count = major * per
        whole = is_end & (p == major - 1 - z)

        @pl.when((p > z) & jnp.logical_not(whole))
        def _():
            copy(key, key, z_up).start()

        @pl.when((p < z) & jnp.logical_not(whole))
        def _():
            copy(key, down_slot(key, p, z - 1, count, extra), z_down).start()

        @pl.when(whole)
        def _():
            copy(key, count + per + extra, far).start()

    def do_a(i):
        p, g = slot_group(i)
        line_a(g, z_up).wait_recv()
        forward(p, g, line_a)
        y_copy(g).start()
        x_copy(g).start()

    def do_c(i):
        p, g = slot_group(i)
        line_c(g, z_up).wait_recv()
        forward(p, g, line_c)
        y_shared(g).start()

    def do_b(i):
        p, g = slot_group(i)
        line_b(g, z_up).wait_recv()
        forward(p, g, line_b)

    def do_x(i):
        _, g = slot_group(i)
        y_copy(g).wait_recv()
        x_copy(g).start()

    def do_k(code):
        i, j = code // FIELD, code % FIELD
        both = j < FIELD - 1
        _, first = slot_group(i)
        _, second = slot_group(jnp.where(both, j, i))

        def ready(index, g):
            @pl.when(index % 2 == 1)
            def _():
                cross_arrival(g).wait_recv()

            @pl.when(index % 2 == 0)
            def _():
                x_arrival(g).wait_recv()

        @pl.when(i > 0)
        def _():
            ready(i, first)

        @pl.when(both)
        def _():
            ready(j, second)

        compute(i, j, first, second, both)

    def do_w(_):
        for k in range(3):
            weight_copy(k, 1 - c).wait_recv()
        wt_all().wait_recv()

    def do_t(i):
        _, g = slot_group(i)
        rx_copy(g).start()

    def do_r(i):
        p, g = slot_group(i)
        rx_copy(g).wait_recv()
        ys[p] = (pa[g] + xr[g].astype(jnp.float32)).astype(jnp.bfloat16)
        ry_copy(p).start()

    def do_s(_):
        loads[8].wait()
        sh_rest().wait_recv()
        share = sg.shape[1]
        for r in range(2):
            shared = jnp.zeros((half, quarter), jnp.float32)
            for q in range(tp_count):
                shared += jnp.dot(
                    sh_all[q, r], sd[q * share : (q + 1) * share, :],
                    preferred_element_type=jnp.float32,
                )
            sh_out[r] = shared

    def do_zb(q):
        p = line_order(q)
        for yy in (1 - y, y):
            g = p * minor + yy
            sum_b(p, g)
            zbs[g] = acc_b[...].astype(jnp.bfloat16)
            send_sum(rzb_copy, g, p, g % minor, minor)

    def do_zc(q):
        p = line_order(q)
        sum_c(p, p * minor + y)
        zcs[p] = acc_c[...].astype(jnp.bfloat16)
        send_sum(rzc_copy, p, p)

    def do_za(q):
        p = line_order(q)
        sum_a(p, p * minor + y)
        zas[p] = acc_a[...].astype(jnp.bfloat16)
        send_sum(rza_copy, p, p)

    def last_copy(i):
        who = (
            {"ep": other_y, "tp": owner}, {"ep": other_y, "tp": far_owner}, {"tp": far_owner}, {"tp": owner},
        )[i]
        return remote(fs.at[i], fr.at[c, i], f_s, f_r.at[c], who)

    def last_c_copy(i):
        return remote(gs.at[i], gr.at[c, i], g_s, g_r.at[c], ({"tp": far_owner}, {"tp": owner})[i])

    def last_rows(which, count):
        b, m = fr.at[which, pl.ds(0, count + 2)], gr.at[which, pl.ds(0, count)]
        return remote(b, b, f_s, f_r.at[which], mate_c), remote(m, m, g_s, g_r.at[which], mate_c)

    head_copy = remote(head, head_in, o_s, o_r, mate_c)

    def do_f1(_):
        sum_b(z, other_y)
        fs[0] = acc_b[:, :tail].astype(jnp.bfloat16)
        fs[1] = acc_b[:, tail:].astype(jnp.bfloat16)
        last_copy(0).start()
        last_copy(1).start()

    def do_f2(_):
        sum_b(z, e)
        fs[2] = acc_b[:, tail:].astype(jnp.bfloat16)
        last_copy(2).start()
        last_b[...] = acc_b[:, :tail]

        @pl.when(c == 0)
        def _():
            fs[3] = acc_b[:, :tail].astype(jnp.bfloat16)
            last_copy(3).start()

    def do_f3(_):
        sum_c(z, e)
        gs[0] = acc_c[:, both_keep:].astype(jnp.bfloat16)
        last_c_copy(0).start()
        last_m[...] = acc_c[:, :both_keep]

        @pl.when(c == 0)
        def _():
            gs[1] = acc_c[:, :both_keep].astype(jnp.bfloat16)
            last_c_copy(1).start()

    actions = (
        (do_a, do_c, do_b, do_x, do_k, do_t, do_r, do_w),
        (do_s, do_zb, do_zc, do_za, do_f1, do_f2, do_f3),
    )

    block = 8
    codes = [functools.reduce(lambda held, k: jnp.where(z == k, at[k], held), range(1, major), z * 0 + at[0]) for at in zip(*plans)]
    codes += [codes[-1] * 0 + FIELD * FIELD * 15] * (-len(codes) % block)

    def main_block(b, carry):
        held = codes[:block]
        for k in range(block, len(codes), block):
            held = [jnp.where(b == k // block, new, old) for new, old in zip(codes[k : k + block], held)]

        def main_step(i, carry):
            code = held[0]
            for k in range(1, block):
                code = jnp.where(i == k, held[k], code)
            kind = code // (FIELD * FIELD)
            arg = code % (FIELD * FIELD)
            for part, group in enumerate(actions):

                @pl.when(kind // 8 == part)
                def _(group=group):
                    for a, action in enumerate(group):

                        @pl.when(kind % 8 == a)
                        def _(action=action):
                            action(arg)

            return carry

        return lax.fori_loop(0, block, main_step, carry)

    lax.fori_loop(0, len(codes) // block, main_block, 0)

    sum_a(z, e)

    def total(ref):
        return sum(ref[i].astype(jnp.float32) for i in range(1, ref.shape[0])) + ref[0].astype(jnp.float32)

    @pl.when(c == 0)
    def _():
        out_ref[:half, :] = (acc_a[...] + sh_out[0]).astype(jnp.bfloat16)
        head_copy.wait_recv()
        out_ref[half:, :] = (head_in[...] + sh_out[1]).astype(jnp.bfloat16)
        for copy in last_rows(0, 2):
            copy.wait_send()

    @pl.when(c == 1)
    def _():
        head[...] = acc_a[...]
        head_copy.start()
        for copy in last_rows(1, 1):
            copy.wait_recv()
        low, high = slice(0, both_keep), slice(both_keep, quarter)
        out_ref[half:, low] = (last_m[...] + gr[1, 0].astype(jnp.float32) + sh_out[1, :, low]).astype(jnp.bfloat16)
        out_ref[half:, high] = (last_b[...] + total(fr.at[1, pl.ds(0, 3)]) + sh_out[1, :, high]).astype(jnp.bfloat16)
        for copy in last_rows(0, 2):
            copy.wait_recv()
        out_ref[:half, low] = (total(gr.at[0]) + sh_out[0, :, low]).astype(jnp.bfloat16)
        out_ref[:half, high] = (total(fr.at[0]) + sh_out[0, :, high]).astype(jnp.bfloat16)
        for copy in last_rows(1, 1):
            copy.wait_send()
        head_copy.wait_send()

    for i in range(3):
        weight_copy(i, c).wait_send()
    y_first().wait_send()
    wt_all().wait_send()
    sh_rest().wait_send()

    def drained(ref, sem):
        remote(ref, ref, sem, a_r.at[0], mate_c).wait_send()

    def lines_sent(count):
        groups = pl.ds(0, count)
        drained(xb.at[groups, :, pl.ds(0, near)], a_s)
        drained(xb.at[groups, :, pl.ds(0, wide)], c_s)
        drained(xb.at[groups, :, pl.ds(0, 2 * (width - 2 * near - wide))], b_s)

    @pl.when(is_end)
    def _():
        lines_sent(1)

    @pl.when(jnp.logical_not(is_end))
    def _():
        lines_sent(major + 1)

    drained(xb.at[pl.ds(0, major), :, pl.ds(0, near)], ya_s)
    drained(xb.at[pl.ds(0, major), :, pl.ds(0, wide)], yc_s)
    drained(xb.at[pl.ds(0, n - 1), :, pl.ds(0, near)], xa_s)
    drained(xs, rx_s)
    drained(ys, ry_s)
    drained(ycs, ryc_s)
    drained(zas.at[pl.ds(0, major - 1)], rza_s)
    drained(zcs.at[pl.ds(0, major - 1)], rzc_s)
    drained(zbs.at[pl.ds(0, n - minor)], rzb_s)


def coded(plan):
    codes = []
    for kind, first, *second in plan:
        arg = first * FIELD + (second[0] if second else FIELD - 1) if kind == "k" else first
        codes.append((KINDS.index(kind) * FIELD * FIELD) + arg)
    return codes


def dense_exchange(
    tokens, norm_gain, expert_ids, route_weights, expert_gate, expert_up, expert_down,
    shared_gate, shared_up, shared_down,
):
    n = lax.axis_size("ep")
    tp_count = lax.axis_size("tp")
    minor = 1 << (n.bit_length() - 1) // 2
    major = n // minor
    rows, width = tokens.shape
    half = rows // 2
    side = width // 2
    quarter = width // tp_count
    near = side * NEAR // 8 // LANES * LANES
    wide = 2 * (side * WIDE // 8 // LANES * LANES)
    keep = quarter
    both_keep = side * BOTH_KEEP // 8 // LANES * LANES
    tail = side - keep - both_keep
    ff = expert_gate.shape[2]
    share = shared_gate.shape[1]
    bf16, f32 = jnp.bfloat16, jnp.float32
    dma = pltpu.SemaphoreType.DMA
    vmem = pl.BlockSpec(memory_space=pltpu.VMEM)
    anywhere = pl.BlockSpec(memory_space=pl.ANY)
    return pl.pallas_call(
        functools.partial(dense_kernel, n, tp_count, minor, near, wide, keep, both_keep, [coded(plan) for plan in PLANS[n // minor]]),
        out_shape=pltpu.VMEM((rows, quarter), bf16),
        in_specs=[anywhere] * 10,
        out_specs=vmem,
        scratch_shapes=[
            pltpu.VMEM((expert_ids.shape[1], rows), jnp.int32),
            pltpu.VMEM((expert_ids.shape[1], rows), f32),
            pltpu.VMEM((1, width), f32),
            pltpu.VMEM((2, half, width), bf16),
            pltpu.VMEM((n, half, width), bf16),
            pltpu.VMEM((half, width), bf16),
            pltpu.VMEM((n, 1, rows), f32),
            pltpu.VMEM((n, 1, rows), f32),
            pltpu.VMEM((2, width, ff), bf16),
            pltpu.VMEM((2, width, ff), bf16),
            pltpu.VMEM((2, ff, width), bf16),
            pltpu.VMEM((width, share), bf16),
            pltpu.VMEM((width, share), bf16),
            pltpu.VMEM((share * tp_count, quarter), bf16),
            pltpu.VMEM((tp_count, 2, half, share), bf16),
            pltpu.VMEM((2, half, quarter), f32),
            pltpu.VMEM((n, half, keep), f32),
            pltpu.VMEM((n, half, 2 * tail), f32),
            pltpu.VMEM((n, half, 2 * both_keep), f32),
            pltpu.VMEM((n, half, keep), bf16),
            pltpu.VMEM((n, half, keep), bf16),
            pltpu.VMEM((major, half, keep), bf16),
            pltpu.VMEM((major, half, keep), bf16),
            pltpu.VMEM((major, half, 2 * both_keep), bf16),
            pltpu.VMEM((major, half, 2 * both_keep), bf16),
            pltpu.VMEM((major, half, keep), bf16),
            pltpu.VMEM((major + 2, half, keep), bf16),
            pltpu.VMEM((n, half, 2 * tail), bf16),
            pltpu.VMEM((n + 2 * minor, half, 2 * tail), bf16),
            pltpu.VMEM((major, half, 2 * both_keep), bf16),
            pltpu.VMEM((major + 2, half, 2 * both_keep), bf16),
            pltpu.VMEM((4, half, tail), bf16),
            pltpu.VMEM((2, 4, half, tail), bf16),
            pltpu.VMEM((2, half, both_keep), bf16),
            pltpu.VMEM((2, 2, half, both_keep), bf16),
            pltpu.VMEM((half, quarter), f32),
            pltpu.VMEM((half, quarter), f32),
            pltpu.VMEM((half, tail), f32),
            pltpu.VMEM((half, both_keep), f32),
            pltpu.VMEM((half, keep), f32),
            pltpu.VMEM((half, 2 * tail), f32),
            pltpu.VMEM((half, 2 * both_keep), f32),
            pltpu.SemaphoreType.REGULAR((major - 1,)), dma((12,)), dma, dma, dma((3,)), dma((3,)), dma, dma, dma,
            dma, dma((major,)), dma, dma((n,)), dma, dma((major,)), dma, dma((major,)), dma, dma, dma((n,)),
            dma, dma((n,)), dma, dma((major,)), dma, dma((major,)), dma, dma((major + 2,)),
            dma, dma((n + 2 * minor,)), dma, dma((major + 2,)), dma, dma((2,)), dma, dma((2,)), dma, dma,
        ],
        compiler_params=pltpu.CompilerParams(
            collective_id=0, has_side_effects=True, vmem_limit_bytes=60 << 20
        ),
        name="dense_moe",
    )(
        expert_ids.T, route_weights.T, norm_gain.reshape(1, width), tokens,
        expert_gate[0], expert_up[0], expert_down[0],
        shared_gate, shared_up, shared_down,
    )


def local(tokens, *rest):
    ep_count = lax.axis_size("ep")
    pair_count = lax.axis_size("tp") // 2
    dense_bytes = 4 * ep_count * tokens.size * tokens.dtype.itemsize
    minor = 1 << (ep_count.bit_length() - 1) // 2
    if pair_count == 2 and minor == 2 and dense_bytes <= 24 << 20:
        return dense_exchange(tokens, *rest)
    return routed_exchange(tokens, *rest)


def solution(mesh):
    return jax.shard_map(
        local,
        mesh=mesh,
        in_specs=(
            P("ep", None),
            P(),
            P("ep", None),
            P("ep", None),
            P(("ep", "tp"), None, None),
            P(("ep", "tp"), None, None),
            P(("ep", "tp"), None, None),
            P(None, "tp"),
            P(None, "tp"),
            P(None, "tp"),
        ),
        out_specs=P("ep", "tp"),
        check_vma=False,
    )
```

```python
import functools

import jax
import jax.numpy as jnp
from jax import lax
from jax.experimental import pallas as pl
from jax.experimental.pallas import tpu as pltpu
from jax.sharding import PartitionSpec as P

NORM_EPSILON = 1e-06


def swapped(block, axis, distance):
    count = lax.axis_size(axis)
    route = []
    for low in range(count):
        high = low | 1 << distance
        if high != low and high < count:
            route += [(low, high), (high, low)]
    return lax.ppermute(block, axis, route)


def routed_exchange(
    tokens,
    norm_gain,
    expert_ids,
    route_weights,
    expert_gate,
    expert_up,
    expert_down,
    shared_gate,
    shared_up,
    shared_down,
):
    ep_count = lax.axis_size("ep")
    tp_count = lax.axis_size("tp")
    pair_count = tp_count // 2
    tp_index = lax.axis_index("tp")
    column = tp_index // 2
    half_index = tp_index % 2
    token_count, model_width = tokens.shape
    top_count = expert_ids.shape[1]
    expert_count = ep_count * pair_count
    capacity = 2 * max(1, token_count * top_count // expert_count)
    half_cap = capacity // 2
    as_float = tokens.astype(jnp.float32)
    inverse_rms = lax.rsqrt(jnp.mean(as_float * as_float, axis=-1, keepdims=True) + NORM_EPSILON)
    normed = (as_float * inverse_rms * norm_gain).astype(jnp.bfloat16)
    expert_iota = jnp.arange(expert_count, dtype=jnp.int32)
    token_iota = jnp.arange(token_count, dtype=jnp.int32)
    counts = jnp.sum(
        (expert_ids[:, :, None] == expert_iota[None, None, :]).astype(jnp.bfloat16), axis=1
    )
    strict_lower = (token_iota[:, None] > token_iota[None, :]).astype(jnp.bfloat16)
    prefix = jnp.dot(strict_lower, counts, preferred_element_type=jnp.float32)
    slot_index = jnp.take_along_axis(prefix, expert_ids, axis=1).astype(jnp.int32)
    target = expert_ids // pair_count
    owner_column = expert_ids % pair_count
    is_mine = owner_column == column
    position = target * capacity + slot_index
    slot_iota = jnp.arange(ep_count * capacity, dtype=jnp.int32)
    matches = is_mine[None, :, :] & (position[None, :, :] == slot_iota[:, None, None])
    slot_taken = jnp.any(matches, axis=2)
    token_of_slot = jnp.sum(jnp.where(slot_taken, token_iota[None, :], 0), axis=1)
    filled = jnp.any(slot_taken, axis=1)
    buffer = jnp.where(
        filled[:, None], jnp.take(normed, token_of_slot, axis=0), jnp.zeros((), jnp.bfloat16)
    )
    buffer = buffer.reshape(ep_count, capacity, model_width)
    gate_local = expert_gate[0]
    up_local = expert_up[0]
    down_local = expert_down[0]
    received = lax.all_to_all(buffer, "ep", split_axis=0, concat_axis=0, tiled=True)
    flat_rows = received.reshape(-1, model_width)
    hidden = (
        jax.nn.silu(jnp.dot(flat_rows, gate_local, preferred_element_type=jnp.float32))
        * jnp.dot(flat_rows, up_local, preferred_element_type=jnp.float32)
    ).astype(jnp.bfloat16)
    partial_out = jnp.dot(hidden, down_local, preferred_element_type=jnp.float32).astype(
        jnp.bfloat16
    )
    partial_out = partial_out.reshape(received.shape[0], received.shape[1], model_width)
    kept_part = lax.dynamic_slice_in_dim(partial_out, half_index * half_cap, half_cap, 1)
    other_part = lax.dynamic_slice_in_dim(partial_out, (1 - half_index) * half_cap, half_cap, 1)
    partner_part = swapped(other_part, "tp", 0)
    expert_out = (kept_part.astype(jnp.float32) + partner_part.astype(jnp.float32)).astype(
        jnp.bfloat16
    )
    returned = lax.all_to_all(expert_out, "ep", split_axis=0, concat_axis=0, tiled=True)
    row_total = ep_count * half_cap
    flat_rows = returned.reshape(row_total, model_width).astype(jnp.float32)
    is_valid = is_mine & (slot_index // half_cap == half_index)
    row_index = jnp.where(is_valid, target * half_cap + slot_index % half_cap, -1)
    row_iota = jnp.arange(row_total, dtype=jnp.int32)
    hits = row_index[:, :, None] == row_iota[None, None, :]
    combine_table = jnp.sum(jnp.where(hits, route_weights[:, :, None], 0.0), axis=1)
    partial_routed = jnp.dot(
        combine_table,
        flat_rows,
        precision=lax.Precision.HIGHEST,
        preferred_element_type=jnp.float32,
    )
    routed = lax.psum_scatter(partial_routed, "tp", scatter_dimension=1, tiled=True)
    shared_act = (
        jax.nn.silu(jnp.dot(normed, shared_gate, preferred_element_type=jnp.float32))
        * jnp.dot(normed, shared_up, preferred_element_type=jnp.float32)
    ).astype(jnp.bfloat16)
    shared_out = jnp.dot(
        lax.all_gather(shared_act, "tp", axis=1, tiled=True),
        shared_down,
        preferred_element_type=jnp.float32,
    )
    return (routed + shared_out).astype(jnp.bfloat16)


MESH = pl.DeviceIdType.MESH
LANES = 128
BOTH_KEEP = 2
WIDE = 2
NEAR = 4


def silu(v):
    return v / (1.0 + jnp.exp(-v))


FIELD = 16
KINDS = ("a", "c", "b", "x", "k", "t", "r", "w", "s", "zb", "zc", "za", "f1", "f2", "f3", "-")
PLAN_0 = [
    ("b", 1), ("x", 1), ("s", 0), ("b", 2), ("a", 2), ("a", 4), ("b", 3), ("c", 2), ("x", 3), ("w", 0), ("k", 2),
    ("b", 4), ("a", 6), ("x", 5), ("c", 6), ("x", 7), ("c", 4), ("k", 1, 3), ("b", 6), ("zb", 0), ("k", 0, 6),
    ("b", 7), ("k", 7), ("zb", 2), ("b", 5), ("k", 4, 5), ("zb", 1), ("r", 3), ("r", 5), ("zc", 1), ("zc", 2),
    ("t", 1), ("t", 0), ("r", 7), ("zc", 0), ("f1", 0), ("za", 1), ("za", 0), ("f2", 0), ("r", 1), ("za", 2),
    ("f3", 0),
]
PLAN_1 = [
    ("a", 2), ("a", 4), ("b", 1), ("b", 3), ("x", 1), ("c", 2), ("b", 4), ("x", 3), ("a", 6), ("c", 4), ("b", 2),
    ("c", 6), ("x", 7), ("x", 5), ("b", 6), ("b", 7), ("w", 0), ("k", 1, 6), ("b", 5), ("k", 3, 7), ("zb", 1),
    ("k", 2, 5), ("r", 7), ("zb", 2), ("t", 1), ("zc", 1), ("k", 0), ("r", 3), ("k", 4), ("t", 0), ("zc", 2),
    ("r", 5), ("za", 1), ("zb", 0), ("f1", 0), ("zc", 0), ("f2", 0), ("za", 2), ("r", 1), ("s", 0), ("f3", 0),
    ("za", 0),
]
PLAN_2 = [
    ("a", 2), ("a", 4), ("b", 4), ("a", 6), ("c", 4), ("x", 1), ("c", 2), ("b", 2), ("b", 3), ("x", 5), ("b", 5),
    ("x", 7), ("c", 6), ("b", 7), ("b", 6), ("b", 1), ("x", 3), ("w", 0), ("k", 2, 6), ("k", 4, 7), ("zb", 1),
    ("k", 3, 5), ("zc", 1), ("r", 7), ("zb", 0), ("k", 0, 1), ("t", 1), ("za", 1), ("zb", 2), ("r", 5), ("zc", 2),
    ("t", 0), ("zc", 0), ("r", 3), ("za", 0), ("r", 1), ("za", 2), ("f1", 0), ("f2", 0), ("s", 0), ("f3", 0),
    ("-", 0),
]
PLAN_3 = [
    ("a", 2), ("c", 2), ("b", 1), ("x", 1), ("a", 4), ("a", 6), ("b", 2), ("x", 5), ("b", 4), ("c", 4), ("w", 0),
    ("k", 0, 4), ("b", 5), ("c", 6), ("x", 7), ("k", 1, 5), ("zb", 1), ("b", 7), ("x", 3), ("t", 1), ("b", 6),
    ("k", 6, 7), ("b", 3), ("zb", 2), ("zc", 1), ("r", 5), ("k", 2, 3), ("zc", 2), ("r", 7), ("s", 0), ("za", 1),
    ("zb", 0), ("za", 2), ("zc", 0), ("r", 3), ("t", 0), ("r", 1), ("f1", 0), ("f2", 0), ("za", 0), ("f3", 0),
    ("-", 0),
]
PLANS = {4: (PLAN_0, PLAN_1, PLAN_2, PLAN_3)}


def dense_kernel(
    ep_count, tp_count, minor, near, wide, keep, both_keep, plans,
    ids_hbm, rw_hbm, gain_hbm, tok_hbm, gate_hbm, up_hbm, down_hbm, sg_hbm, su_hbm, sd_hbm,
    out_ref,
    ids_ref, rw_ref, gain_ref, tok, xb, xo, wtab, wr, wg, wu, wd, sg, su, sd, sh_all, sh_out,
    pa, pb, pc, xs, xr, ys, yr, ycs, ycr, zas, zar, zbs, zbr, zcs, zcr, fs, fr, gs, gr, head, head_in, last_b, last_m, acc_a, acc_b, acc_c,
    line_sem, load_sem, wt_s, wt_r, we_s, we_r, sh_s, sh_r, yb_s,
    a_s, a_r, b_s, b_r, c_s, c_r, ya_s, ya_r, yc_s, xa_s, xa_r,
    rx_s, rx_r, ry_s, ry_r, ryc_s, ryc_r, rza_s, rza_r, rzb_s, rzb_r, rzc_s, rzc_r, f_s, f_r, g_s, g_r, o_s, o_r,
):
    n = ep_count
    major = n // minor
    half, width = xo.shape
    side = width // 2
    quarter = width // tp_count
    tail = side - keep - both_keep
    middle = keep + both_keep
    e = lax.axis_index("ep")
    t = lax.axis_index("tp")
    z = e // minor
    y = e % minor
    xi = t // 2
    c = t % 2
    t2 = 2 * (1 - xi) + c
    other_y = z * minor + 1 - y
    mate_x = {"tp": t2}
    mate_c = {"tp": 2 * xi + 1 - c}
    mate_y = {"ep": other_y}
    owner = 2 * xi + 1
    far_owner = 2 * (1 - xi) + 1
    z_up = {"ep": lax.rem(e + minor, n)}
    z_down = {"ep": lax.rem(e + n - minor, n)}
    far = {"ep": (major - 1 - z) * minor + y}
    is_end = (z == 0) | (z == major - 1)

    barrier = pltpu.get_barrier_semaphore()

    def greet_line(sem):
        @pl.when(z < major - 1)
        def _():
            pl.semaphore_signal(sem, inc=1, device_id=z_up, device_id_type=MESH)

        @pl.when(z > 0)
        def _():
            pl.semaphore_signal(sem, inc=1, device_id=z_down, device_id_type=MESH)

    in_line = jnp.where(is_end, 1, 2)
    greet_line(barrier)
    for k in range(1, tp_count):
        pl.semaphore_signal(barrier, inc=1, device_id={"tp": lax.rem(t + k, tp_count)}, device_id_type=MESH)
    for k in range(tp_count):
        there = {"ep": other_y, "tp": lax.rem(t + k, tp_count)}
        pl.semaphore_signal(barrier, inc=1, device_id=there, device_id_type=MESH)

    def remote(src, dst, s, r, who):
        return pltpu.make_async_remote_copy(
            src_ref=src, dst_ref=dst, send_sem=s, recv_sem=r, device_id=who, device_id_type=MESH
        )

    def rows_of(which):
        return pl.ds(pl.multiple_of(which * half, half), half)

    def side_of(which):
        return pl.ds(pl.multiple_of(which * side, side), side)

    loads = [
        pltpu.make_async_copy(a, b, load_sem.at[i])
        for i, (a, b) in enumerate(
            (
                (tok_hbm.at[rows_of(c)], tok.at[0]),
                (tok_hbm.at[rows_of(1 - c)], tok.at[1]),
                (gate_hbm, wg.at[c]),
                (up_hbm, wu.at[c]),
                (down_hbm.at[:, side_of(xi)], wd.at[c, :, pl.ds(0, side)]),
                (down_hbm.at[:, side_of(1 - xi)], wd.at[c, :, pl.ds(side, side)]),
                (sg_hbm, sg),
                (su_hbm, su),
                (sd_hbm, sd),
                (gain_hbm, gain_ref),
                (ids_hbm, ids_ref),
                (rw_hbm, rw_ref),
            )
        )
    ]
    for i in (0, 9, 10, 11, 2, 3, 4, 5, 1, 6, 7, 8):
        loads[i].start()

    step = 16

    def norm_into(which, store):
        def body(i, carry):
            part = pl.ds(pl.multiple_of(i * step, step), step)
            v = tok[which, part, :].astype(jnp.float32)
            r = lax.rsqrt(jnp.mean(v * v, axis=-1, keepdims=True) + NORM_EPSILON)
            store(part, (v * r * gain_ref[...]).astype(jnp.bfloat16))
            return carry

        lax.fori_loop(0, half // step, body, 0, unroll=True)

    def store_own(part, value):
        xb[e, part, :] = value

    def store_rest(part, value):
        xo[part, :] = value

    def weights_for(expert):
        row = jnp.zeros((1, ids_ref.shape[1]), jnp.float32)
        for k in range(ids_ref.shape[0]):
            row += jnp.where(ids_ref[k : k + 1, :] == expert, rw_ref[k : k + 1, :], 0.0)
        return row

    loads[0].wait()
    loads[9].wait()
    norm_into(0, store_own)
    loads[10].wait()
    loads[11].wait()
    for d in range(n):
        wtab[d] = weights_for(d * (tp_count // 2) + xi)
    wr[e] = weights_for(e * (tp_count // 2) + xi)
    pl.semaphore_wait(barrier, 2 * tp_count - 1 + in_line)
    greet_line(line_sem.at[0])

    mine = pl.ds(pl.multiple_of(xi * near, LANES), near)
    theirs = pl.ds(pl.multiple_of((1 - xi) * near, LANES), near)
    shared_cols = pl.ds(2 * near, wide)
    rest = pl.ds(2 * near + wide, width - 2 * near - wide)

    def line_a(g, who):
        ref = xb.at[g, :, mine]
        return remote(ref, ref, a_s, a_r.at[g // minor], who)

    def line_b(g, who):
        ref = xb.at[g, :, rest]
        return remote(ref, ref, b_s, b_r.at[g], who)

    def line_c(g, who):
        ref = xb.at[g, :, shared_cols]
        return remote(ref, ref, c_s, c_r.at[g // minor], who)

    def y_shared(g):
        ref = xb.at[g, :, shared_cols]
        return remote(ref, ref, yc_s, xa_r.at[g], mate_y)

    def y_first():
        ref = xb.at[e, :, rest]
        return remote(ref, ref, yb_s, b_r.at[e], mate_y)

    def y_copy(g):
        ref = xb.at[g, :, mine]
        return remote(ref, ref, ya_s, ya_r.at[g // minor], mate_y)

    def x_copy(g):
        ref = xb.at[g, :, mine]
        return remote(ref, ref, xa_s, xa_r.at[g], mate_x)

    def x_arrival(g):
        ref = xb.at[g, :, theirs]
        return remote(ref, ref, xa_s, xa_r.at[g], mate_x)

    def cross_arrival(g):
        ref = xb.at[g, :, pl.ds(0, near + wide)]
        return remote(ref, ref, xa_s, xa_r.at[g], mate_x)

    def wt_copy(target):
        return remote(wtab.at[target], wr.at[e], wt_s, wt_r, {"ep": target})

    def wt_all():
        return remote(wtab.at[pl.ds(0, n - 1)], wr.at[pl.ds(0, n - 1)], wt_s, wt_r, mate_y)

    def weight_copy(i, which):
        ref = (wg, wu, wd)[i].at[which]
        return remote(ref, ref, we_s.at[i], we_r.at[i], mate_c)

    def sh_copy(who):
        return remote(sh_all.at[t], sh_all.at[t], sh_s, sh_r, {"tp": who})

    def sh_rest():
        ref = sh_all.at[pl.ds(0, tp_count - 1)]
        return remote(ref, ref, sh_s, sh_r, mate_c)

    def order(j):
        k = jnp.minimum(z, major - 1 - z)
        d = (j + 1) // 2
        close = jnp.where((j % 2 == 1) == (2 * z < major), z - d, z + d)
        far = jnp.where(z <= major - 1 - z, j, major - 1 - j)
        return jnp.where(j <= 2 * k, close, far)

    def slot_group(i):
        p = order(i // 2)
        yy = jnp.where(i % 2 == 0, y, 1 - y)
        return p, p * minor + yy

    def ups(p):
        return (p <= z) & (z < major - 1)

    def downs(p):
        return (p >= z) & (z > 0)

    def forward(p, g, line):
        @pl.when(ups(p))
        def _():
            line(g, z_up).start()

        @pl.when(downs(p))
        def _():
            line(g, z_down).start()

    forward(z, e, line_a)
    y_first().start()
    forward(z, e, line_c)
    y_copy(e).start()
    y_shared(e).start()
    forward(z, e, line_b)
    loads[2].wait()
    weight_copy(0, c).start()
    loads[3].wait()
    weight_copy(1, c).start()
    loads[4].wait()
    loads[5].wait()
    weight_copy(2, c).start()
    loads[1].wait()
    norm_into(1, store_rest)
    loads[6].wait()
    loads[7].wait()

    def shared_in(x):
        g_sum = jnp.dot(x, sg[...], preferred_element_type=jnp.float32)
        u_sum = jnp.dot(x, su[...], preferred_element_type=jnp.float32)
        return (silu(g_sum) * u_sum).astype(jnp.bfloat16)

    sh_all[t, c] = shared_in(xb[e])
    sh_all[t, 1 - c] = shared_in(xo[...])
    for k in range(1, tp_count):
        sh_copy(lax.rem(t + k, tp_count)).start()
    for k in range(major - 1):
        pl.semaphore_wait(line_sem.at[k], in_line)
        if k < major - 2:
            greet_line(line_sem.at[k + 1])
    for k in range(1, n):
        wt_copy(lax.rem(e + k, n)).start()

    def rx_copy(g):
        return remote(xs.at[g], xr.at[g], rx_s, rx_r.at[g], mate_x)

    def ry_copy(p):
        return remote(ys.at[p], yr.at[p], ry_s, ry_r.at[p], mate_y)

    def ryc_copy(p):
        return remote(ycs.at[p], ycr.at[p], ryc_s, ryc_r.at[p], mate_y)

    def rzc_copy(p, slot, who):
        return remote(zcs.at[p], zcr.at[slot], rzc_s, rzc_r.at[slot], who)

    def rza_copy(p, slot, who):
        return remote(zas.at[p], zar.at[slot], rza_s, rza_r.at[slot], who)

    def rzb_copy(g, slot, who):
        return remote(zbs.at[g], zbr.at[slot], rzb_s, rzb_r.at[slot], who)

    def down_slot(key, p, to, count, extra):
        return jnp.where(p == to, count + extra, key)

    diagonal = lax.broadcasted_iota(jnp.int32, (half, 2 * half), 1) == (
        lax.broadcasted_iota(jnp.int32, (half, 2 * half), 0) + c * half
    )

    def weight_of(g):
        return jnp.sum(jnp.where(diagonal, wr[g], 0.0), axis=1, keepdims=True)

    def compute(i, j, first, second, both):
        pair = ((i, first), (j, second))
        weight = jnp.concatenate([weight_of(first), weight_of(second)], axis=0)
        x = jnp.concatenate([xb[first], xb[second]], axis=0)
        acts = []
        for h in range(2):
            g_sum = jnp.dot(x, wg[h], preferred_element_type=jnp.float32)
            u_sum = jnp.dot(x, wu[h], preferred_element_type=jnp.float32)
            acts.append((silu(g_sum) * u_sum).astype(jnp.bfloat16))

        def columns(low, high):
            total = jnp.dot(acts[0], wd[0, :, low:high], preferred_element_type=jnp.float32)
            total += jnp.dot(acts[1], wd[1, :, low:high], preferred_element_type=jnp.float32)
            return total * weight

        sent = columns(side, side + keep).astype(jnp.bfloat16)
        kept = columns(0, keep)
        kept_c = columns(keep, middle)
        rest_c = columns(side + keep, side + middle)
        main = columns(middle, side)
        rest = columns(side + middle, width)

        def put(k):
            index, g = pair[k]
            part = slice(k * half, (k + 1) * half)
            xs[g] = sent[part]

            @pl.when(index > 1)
            def _():
                rx_copy(g).start()

            pc[g, :, :both_keep] = kept_c[part]
            pc[g, :, both_keep:] = rest_c[part]

            @pl.when(index % 2 == 1)
            def _():
                p = g // minor
                ycs[p] = pc[g].astype(jnp.bfloat16)
                ryc_copy(p).start()

            pa[g] = kept[part]
            pb[g, :, :tail] = main[part]
            pb[g, :, tail:] = rest[part]

        put(0)

        @pl.when(both)
        def _():
            put(1)

    def add_lanes(p, acc, copy, key, received, extra=0, per=1):
        count = major * per
        below = downs(p) & jnp.logical_not((p == major - 1) & (z == 1))
        above = ups(p) & jnp.logical_not((p == 0) & (z == major - 2))

        def add(slot):
            copy(key, slot, z_up).wait_recv()
            acc[...] += received[slot].astype(jnp.float32)

        @pl.when(below)
        def _():
            add(key)

        @pl.when(above)
        def _():
            add(down_slot(key, p, z, count, extra))

        @pl.when((p == z) & is_end)
        def _():
            add(count + per + extra)

    def sum_b(p, g):
        acc_b[...] = pb[g]
        add_lanes(p, acc_b, rzb_copy, g, zbr, g % minor, minor)

    def sum_c(p, g):
        ryc_copy(p).wait_recv()
        acc_c[...] = pc[g] + ycr[p].astype(jnp.float32)
        add_lanes(p, acc_c, rzc_copy, p, zcr)

    def sum_a(p, g):
        rx_copy(g).wait_recv()
        ry_copy(p).wait_recv()
        acc_a[...] = pa[g] + xr[g].astype(jnp.float32) + yr[p].astype(jnp.float32)
        add_lanes(p, acc_a, rza_copy, p, zar)

    def line_order(q):
        above = major - 1 - z
        low = jnp.where(q < above, z + 1 + q, z - 1 - (q - above))
        high = jnp.where(q < z, z - 1 - q, z + 1 + (q - z))
        return jnp.where(2 * z < major, low, high)

    def send_sum(copy, key, p, extra=0, per=1):
        count = major * per
        whole = is_end & (p == major - 1 - z)

        @pl.when((p > z) & jnp.logical_not(whole))
        def _():
            copy(key, key, z_up).start()

        @pl.when((p < z) & jnp.logical_not(whole))
        def _():
            copy(key, down_slot(key, p, z - 1, count, extra), z_down).start()

        @pl.when(whole)
        def _():
            copy(key, count + per + extra, far).start()

    def do_a(i):
        p, g = slot_group(i)
        line_a(g, z_up).wait_recv()
        forward(p, g, line_a)
        y_copy(g).start()
        x_copy(g).start()

    def do_c(i):
        p, g = slot_group(i)
        line_c(g, z_up).wait_recv()
        forward(p, g, line_c)
        y_shared(g).start()

    def do_b(i):
        p, g = slot_group(i)
        line_b(g, z_up).wait_recv()
        forward(p, g, line_b)

    def do_x(i):
        _, g = slot_group(i)
        y_copy(g).wait_recv()
        x_copy(g).start()

    def do_k(code):
        i, j = code // FIELD, code % FIELD
        both = j < FIELD - 1
        _, first = slot_group(i)
        _, second = slot_group(jnp.where(both, j, i))

        def ready(index, g):
            @pl.when(index % 2 == 1)
            def _():
                cross_arrival(g).wait_recv()

            @pl.when(index % 2 == 0)
            def _():
                x_arrival(g).wait_recv()

        @pl.when(i > 0)
        def _():
            ready(i, first)

        @pl.when(both)
        def _():
            ready(j, second)

        compute(i, j, first, second, both)

    def do_w(_):
        for k in range(3):
            weight_copy(k, 1 - c).wait_recv()
        wt_all().wait_recv()

    def do_t(i):
        _, g = slot_group(i)
        rx_copy(g).start()

    def do_r(i):
        p, g = slot_group(i)
        rx_copy(g).wait_recv()
        ys[p] = (pa[g] + xr[g].astype(jnp.float32)).astype(jnp.bfloat16)
        ry_copy(p).start()

    def do_s(_):
        loads[8].wait()
        sh_rest().wait_recv()
        share = sg.shape[1]
        for r in range(2):
            shared = jnp.zeros((half, quarter), jnp.float32)
            for q in range(tp_count):
                shared += jnp.dot(
                    sh_all[q, r], sd[q * share : (q + 1) * share, :],
                    preferred_element_type=jnp.float32,
                )
            sh_out[r] = shared

    def do_zb(q):
        p = line_order(q)
        for yy in (1 - y, y):
            g = p * minor + yy
            sum_b(p, g)
            zbs[g] = acc_b[...].astype(jnp.bfloat16)
            send_sum(rzb_copy, g, p, g % minor, minor)

    def do_zc(q):
        p = line_order(q)
        sum_c(p, p * minor + y)
        zcs[p] = acc_c[...].astype(jnp.bfloat16)
        send_sum(rzc_copy, p, p)

    def do_za(q):
        p = line_order(q)
        sum_a(p, p * minor + y)
        zas[p] = acc_a[...].astype(jnp.bfloat16)
        send_sum(rza_copy, p, p)

    def last_copy(i):
        who = (
            {"ep": other_y, "tp": owner}, {"ep": other_y, "tp": far_owner}, {"tp": far_owner}, {"tp": owner},
        )[i]
        return remote(fs.at[i], fr.at[c, i], f_s, f_r.at[c], who)

    def last_c_copy(i):
        return remote(gs.at[i], gr.at[c, i], g_s, g_r.at[c], ({"tp": far_owner}, {"tp": owner})[i])

    def last_rows(which, count):
        b, m = fr.at[which, pl.ds(0, count + 2)], gr.at[which, pl.ds(0, count)]
        return remote(b, b, f_s, f_r.at[which], mate_c), remote(m, m, g_s, g_r.at[which], mate_c)

    head_copy = remote(head, head_in, o_s, o_r, mate_c)

    def do_f1(_):
        sum_b(z, other_y)
        fs[0] = acc_b[:, :tail].astype(jnp.bfloat16)
        fs[1] = acc_b[:, tail:].astype(jnp.bfloat16)
        last_copy(0).start()
        last_copy(1).start()

    def do_f2(_):
        sum_b(z, e)
        fs[2] = acc_b[:, tail:].astype(jnp.bfloat16)
        last_copy(2).start()
        last_b[...] = acc_b[:, :tail]

        @pl.when(c == 0)
        def _():
            fs[3] = acc_b[:, :tail].astype(jnp.bfloat16)
            last_copy(3).start()

    def do_f3(_):
        sum_c(z, e)
        gs[0] = acc_c[:, both_keep:].astype(jnp.bfloat16)
        last_c_copy(0).start()
        last_m[...] = acc_c[:, :both_keep]

        @pl.when(c == 0)
        def _():
            gs[1] = acc_c[:, :both_keep].astype(jnp.bfloat16)
            last_c_copy(1).start()

    actions = (
        (do_a, do_c, do_b, do_x, do_k, do_t, do_r, do_w),
        (do_s, do_zb, do_zc, do_za, do_f1, do_f2, do_f3),
    )

    block = 8
    codes = [functools.reduce(lambda held, k: jnp.where(z == k, at[k], held), range(1, major), z * 0 + at[0]) for at in zip(*plans)]
    codes += [codes[-1] * 0 + FIELD * FIELD * 15] * (-len(codes) % block)

    def main_block(b, carry):
        held = codes[:block]
        for k in range(block, len(codes), block):
            held = [jnp.where(b == k // block, new, old) for new, old in zip(codes[k : k + block], held)]

        def main_step(i, carry):
            code = held[0]
            for k in range(1, block):
                code = jnp.where(i == k, held[k], code)
            kind = code // (FIELD * FIELD)
            arg = code % (FIELD * FIELD)
            for part, group in enumerate(actions):

                @pl.when(kind // 8 == part)
                def _(group=group):
                    for a, action in enumerate(group):

                        @pl.when(kind % 8 == a)
                        def _(action=action):
                            action(arg)

            return carry

        return lax.fori_loop(0, block, main_step, carry)

    lax.fori_loop(0, len(codes) // block, main_block, 0)

    sum_a(z, e)

    def total(ref):
        return sum(ref[i].astype(jnp.float32) for i in range(1, ref.shape[0])) + ref[0].astype(jnp.float32)

    @pl.when(c == 0)
    def _():
        out_ref[:half, :] = (acc_a[...] + sh_out[0]).astype(jnp.bfloat16)
        head_copy.wait_recv()
        out_ref[half:, :] = (head_in[...] + sh_out[1]).astype(jnp.bfloat16)
        for copy in last_rows(0, 2):
            copy.wait_send()

    @pl.when(c == 1)
    def _():
        head[...] = acc_a[...]
        head_copy.start()
        for copy in last_rows(1, 1):
            copy.wait_recv()
        low, high = slice(0, both_keep), slice(both_keep, quarter)
        out_ref[half:, low] = (last_m[...] + gr[1, 0].astype(jnp.float32) + sh_out[1, :, low]).astype(jnp.bfloat16)
        out_ref[half:, high] = (last_b[...] + total(fr.at[1, pl.ds(0, 3)]) + sh_out[1, :, high]).astype(jnp.bfloat16)
        for copy in last_rows(0, 2):
            copy.wait_recv()
        out_ref[:half, low] = (total(gr.at[0]) + sh_out[0, :, low]).astype(jnp.bfloat16)
        out_ref[:half, high] = (total(fr.at[0]) + sh_out[0, :, high]).astype(jnp.bfloat16)
        for copy in last_rows(1, 1):
            copy.wait_send()
        head_copy.wait_send()

    for i in range(3):
        weight_copy(i, c).wait_send()
    y_first().wait_send()
    wt_all().wait_send()
    sh_rest().wait_send()

    def drained(ref, sem):
        remote(ref, ref, sem, a_r.at[0], mate_c).wait_send()

    def lines_sent(count):
        groups = pl.ds(0, count)
        drained(xb.at[groups, :, pl.ds(0, near)], a_s)
        drained(xb.at[groups, :, pl.ds(0, wide)], c_s)
        drained(xb.at[groups, :, pl.ds(0, 2 * (width - 2 * near - wide))], b_s)

    @pl.when(is_end)
    def _():
        lines_sent(1)

    @pl.when(jnp.logical_not(is_end))
    def _():
        lines_sent(major + 1)

    drained(xb.at[pl.ds(0, major), :, pl.ds(0, near)], ya_s)
    drained(xb.at[pl.ds(0, major), :, pl.ds(0, wide)], yc_s)
    drained(xb.at[pl.ds(0, n - 1), :, pl.ds(0, near)], xa_s)
    drained(xs, rx_s)
    drained(ys, ry_s)
    drained(ycs, ryc_s)
    drained(zas.at[pl.ds(0, major - 1)], rza_s)
    drained(zcs.at[pl.ds(0, major - 1)], rzc_s)
    drained(zbs.at[pl.ds(0, n - minor)], rzb_s)


def coded(plan):
    codes = []
    for kind, first, *second in plan:
        arg = first * FIELD + (second[0] if second else FIELD - 1) if kind == "k" else first
        codes.append((KINDS.index(kind) * FIELD * FIELD) + arg)
    return codes


def dense_exchange(
    tokens, norm_gain, expert_ids, route_weights, expert_gate, expert_up, expert_down,
    shared_gate, shared_up, shared_down,
):
    n = lax.axis_size("ep")
    tp_count = lax.axis_size("tp")
    minor = 1 << (n.bit_length() - 1) // 2
    major = n // minor
    rows, width = tokens.shape
    half = rows // 2
    side = width // 2
    quarter = width // tp_count
    near = side * NEAR // 8 // LANES * LANES
    wide = 2 * (side * WIDE // 8 // LANES * LANES)
    keep = quarter
    both_keep = side * BOTH_KEEP // 8 // LANES * LANES
    tail = side - keep - both_keep
    ff = expert_gate.shape[2]
    share = shared_gate.shape[1]
    bf16, f32 = jnp.bfloat16, jnp.float32
    dma = pltpu.SemaphoreType.DMA
    vmem = pl.BlockSpec(memory_space=pltpu.VMEM)
    anywhere = pl.BlockSpec(memory_space=pl.ANY)
    return pl.pallas_call(
        functools.partial(dense_kernel, n, tp_count, minor, near, wide, keep, both_keep, [coded(plan) for plan in PLANS[n // minor]]),
        out_shape=pltpu.VMEM((rows, quarter), bf16),
        in_specs=[anywhere] * 10,
        out_specs=vmem,
        scratch_shapes=[
            pltpu.VMEM((expert_ids.shape[1], rows), jnp.int32),
            pltpu.VMEM((expert_ids.shape[1], rows), f32),
            pltpu.VMEM((1, width), f32),
            pltpu.VMEM((2, half, width), bf16),
            pltpu.VMEM((n, half, width), bf16),
            pltpu.VMEM((half, width), bf16),
            pltpu.VMEM((n, 1, rows), f32),
            pltpu.VMEM((n, 1, rows), f32),
            pltpu.VMEM((2, width, ff), bf16),
            pltpu.VMEM((2, width, ff), bf16),
            pltpu.VMEM((2, ff, width), bf16),
            pltpu.VMEM((width, share), bf16),
            pltpu.VMEM((width, share), bf16),
            pltpu.VMEM((share * tp_count, quarter), bf16),
            pltpu.VMEM((tp_count, 2, half, share), bf16),
            pltpu.VMEM((2, half, quarter), f32),
            pltpu.VMEM((n, half, keep), f32),
            pltpu.VMEM((n, half, 2 * tail), f32),
            pltpu.VMEM((n, half, 2 * both_keep), f32),
            pltpu.VMEM((n, half, keep), bf16),
            pltpu.VMEM((n, half, keep), bf16),
            pltpu.VMEM((major, half, keep), bf16),
            pltpu.VMEM((major, half, keep), bf16),
            pltpu.VMEM((major, half, 2 * both_keep), bf16),
            pltpu.VMEM((major, half, 2 * both_keep), bf16),
            pltpu.VMEM((major, half, keep), bf16),
            pltpu.VMEM((major + 2, half, keep), bf16),
            pltpu.VMEM((n, half, 2 * tail), bf16),
            pltpu.VMEM((n + 2 * minor, half, 2 * tail), bf16),
            pltpu.VMEM((major, half, 2 * both_keep), bf16),
            pltpu.VMEM((major + 2, half, 2 * both_keep), bf16),
            pltpu.VMEM((4, half, tail), bf16),
            pltpu.VMEM((2, 4, half, tail), bf16),
            pltpu.VMEM((2, half, both_keep), bf16),
            pltpu.VMEM((2, 2, half, both_keep), bf16),
            pltpu.VMEM((half, quarter), f32),
            pltpu.VMEM((half, quarter), f32),
            pltpu.VMEM((half, tail), f32),
            pltpu.VMEM((half, both_keep), f32),
            pltpu.VMEM((half, keep), f32),
            pltpu.VMEM((half, 2 * tail), f32),
            pltpu.VMEM((half, 2 * both_keep), f32),
            pltpu.SemaphoreType.REGULAR((major - 1,)), dma((12,)), dma, dma, dma((3,)), dma((3,)), dma, dma, dma,
            dma, dma((major,)), dma, dma((n,)), dma, dma((major,)), dma, dma((major,)), dma, dma, dma((n,)),
            dma, dma((n,)), dma, dma((major,)), dma, dma((major,)), dma, dma((major + 2,)),
            dma, dma((n + 2 * minor,)), dma, dma((major + 2,)), dma, dma((2,)), dma, dma((2,)), dma, dma,
        ],
        compiler_params=pltpu.CompilerParams(
            collective_id=0, has_side_effects=True, vmem_limit_bytes=60 << 20
        ),
        name="dense_moe",
    )(
        expert_ids.T, route_weights.T, norm_gain.reshape(1, width), tokens,
        expert_gate[0], expert_up[0], expert_down[0],
        shared_gate, shared_up, shared_down,
    )


def local(tokens, *rest):
    ep_count = lax.axis_size("ep")
    pair_count = lax.axis_size("tp") // 2
    dense_bytes = 4 * ep_count * tokens.size * tokens.dtype.itemsize
    minor = 1 << (ep_count.bit_length() - 1) // 2
    if pair_count == 2 and minor == 2 and dense_bytes <= 24 << 20:
        return dense_exchange(tokens, *rest)
    return routed_exchange(tokens, *rest)


def solution(mesh):
    return jax.shard_map(
        local,
        mesh=mesh,
        in_specs=(
            P("ep", None),
            P(),
            P("ep", None),
            P("ep", None),
            P(("ep", "tp"), None, None),
            P(("ep", "tp"), None, None),
            P(("ep", "tp"), None, None),
            P(None, "tp"),
            P(None, "tp"),
            P(None, "tp"),
        ),
        out_specs=P("ep", "tp"),
        check_vma=False,
    )
```

```python
import functools

import jax
import jax.numpy as jnp
from jax import lax
from jax.experimental import pallas as pl
from jax.experimental.pallas import tpu as pltpu
from jax.sharding import PartitionSpec as P

NORM_EPSILON = 1e-06


def swapped(block, axis, distance):
    count = lax.axis_size(axis)
    route = []
    for low in range(count):
        high = low | 1 << distance
        if high != low and high < count:
            route += [(low, high), (high, low)]
    return lax.ppermute(block, axis, route)


def routed_exchange(
    tokens,
    norm_gain,
    expert_ids,
    route_weights,
    expert_gate,
    expert_up,
    expert_down,
    shared_gate,
    shared_up,
    shared_down,
):
    ep_count = lax.axis_size("ep")
    tp_count = lax.axis_size("tp")
    pair_count = tp_count // 2
    tp_index = lax.axis_index("tp")
    column = tp_index // 2
    half_index = tp_index % 2
    token_count, model_width = tokens.shape
    top_count = expert_ids.shape[1]
    expert_count = ep_count * pair_count
    capacity = 2 * max(1, token_count * top_count // expert_count)
    half_cap = capacity // 2
    as_float = tokens.astype(jnp.float32)
    inverse_rms = lax.rsqrt(jnp.mean(as_float * as_float, axis=-1, keepdims=True) + NORM_EPSILON)
    normed = (as_float * inverse_rms * norm_gain).astype(jnp.bfloat16)
    expert_iota = jnp.arange(expert_count, dtype=jnp.int32)
    token_iota = jnp.arange(token_count, dtype=jnp.int32)
    counts = jnp.sum(
        (expert_ids[:, :, None] == expert_iota[None, None, :]).astype(jnp.bfloat16), axis=1
    )
    strict_lower = (token_iota[:, None] > token_iota[None, :]).astype(jnp.bfloat16)
    prefix = jnp.dot(strict_lower, counts, preferred_element_type=jnp.float32)
    slot_index = jnp.take_along_axis(prefix, expert_ids, axis=1).astype(jnp.int32)
    target = expert_ids // pair_count
    owner_column = expert_ids % pair_count
    is_mine = owner_column == column
    position = target * capacity + slot_index
    slot_iota = jnp.arange(ep_count * capacity, dtype=jnp.int32)
    matches = is_mine[None, :, :] & (position[None, :, :] == slot_iota[:, None, None])
    slot_taken = jnp.any(matches, axis=2)
    token_of_slot = jnp.sum(jnp.where(slot_taken, token_iota[None, :], 0), axis=1)
    filled = jnp.any(slot_taken, axis=1)
    buffer = jnp.where(
        filled[:, None], jnp.take(normed, token_of_slot, axis=0), jnp.zeros((), jnp.bfloat16)
    )
    buffer = buffer.reshape(ep_count, capacity, model_width)
    gate_local = expert_gate[0]
    up_local = expert_up[0]
    down_local = expert_down[0]
    received = lax.all_to_all(buffer, "ep", split_axis=0, concat_axis=0, tiled=True)
    flat_rows = received.reshape(-1, model_width)
    hidden = (
        jax.nn.silu(jnp.dot(flat_rows, gate_local, preferred_element_type=jnp.float32))
        * jnp.dot(flat_rows, up_local, preferred_element_type=jnp.float32)
    ).astype(jnp.bfloat16)
    partial_out = jnp.dot(hidden, down_local, preferred_element_type=jnp.float32).astype(
        jnp.bfloat16
    )
    partial_out = partial_out.reshape(received.shape[0], received.shape[1], model_width)
    kept_part = lax.dynamic_slice_in_dim(partial_out, half_index * half_cap, half_cap, 1)
    other_part = lax.dynamic_slice_in_dim(partial_out, (1 - half_index) * half_cap, half_cap, 1)
    partner_part = swapped(other_part, "tp", 0)
    expert_out = (kept_part.astype(jnp.float32) + partner_part.astype(jnp.float32)).astype(
        jnp.bfloat16
    )
    returned = lax.all_to_all(expert_out, "ep", split_axis=0, concat_axis=0, tiled=True)
    row_total = ep_count * half_cap
    flat_rows = returned.reshape(row_total, model_width).astype(jnp.float32)
    is_valid = is_mine & (slot_index // half_cap == half_index)
    row_index = jnp.where(is_valid, target * half_cap + slot_index % half_cap, -1)
    row_iota = jnp.arange(row_total, dtype=jnp.int32)
    hits = row_index[:, :, None] == row_iota[None, None, :]
    combine_table = jnp.sum(jnp.where(hits, route_weights[:, :, None], 0.0), axis=1)
    partial_routed = jnp.dot(
        combine_table,
        flat_rows,
        precision=lax.Precision.HIGHEST,
        preferred_element_type=jnp.float32,
    )
    routed = lax.psum_scatter(partial_routed, "tp", scatter_dimension=1, tiled=True)
    shared_act = (
        jax.nn.silu(jnp.dot(normed, shared_gate, preferred_element_type=jnp.float32))
        * jnp.dot(normed, shared_up, preferred_element_type=jnp.float32)
    ).astype(jnp.bfloat16)
    shared_out = jnp.dot(
        lax.all_gather(shared_act, "tp", axis=1, tiled=True),
        shared_down,
        preferred_element_type=jnp.float32,
    )
    return (routed + shared_out).astype(jnp.bfloat16)


MESH = pl.DeviceIdType.MESH
LANES = 128
BOTH_KEEP = 2
WIDE = 2
NEAR = 4


def silu(v):
    return v / (1.0 + jnp.exp(-v))


FIELD = 16
KINDS = ("a", "c", "b", "x", "k", "t", "r", "w", "s", "zb", "zc", "za", "f1", "f2", "f3", "-")
PLAN_0 = [
    ("b", 1), ("x", 1), ("s", 0), ("b", 2), ("a", 2), ("a", 4), ("b", 3), ("c", 2), ("x", 3), ("w", 0), ("k", 2),
    ("b", 4), ("a", 6), ("x", 5), ("c", 6), ("x", 7), ("c", 4), ("k", 1, 3), ("b", 6), ("zb", 0), ("k", 0, 6),
    ("b", 7), ("k", 7), ("zb", 2), ("b", 5), ("k", 4, 5), ("zb", 1), ("r", 3), ("r", 5), ("zc", 1), ("zc", 2),
    ("t", 1), ("t", 0), ("r", 7), ("zc", 0), ("f1", 0), ("za", 1), ("za", 0), ("f2", 0), ("r", 1), ("za", 2),
    ("f3", 0),
]
PLAN_1 = [
    ("a", 2), ("a", 4), ("b", 1), ("b", 3), ("x", 1), ("c", 2), ("b", 4), ("x", 3), ("a", 6), ("c", 4), ("b", 2),
    ("c", 6), ("x", 7), ("x", 5), ("b", 6), ("b", 7), ("w", 0), ("k", 1, 6), ("b", 5), ("k", 3, 7), ("zb", 1),
    ("k", 2, 5), ("r", 7), ("zb", 2), ("t", 1), ("zc", 1), ("k", 0), ("r", 3), ("k", 4), ("t", 0), ("zc", 2),
    ("r", 5), ("za", 1), ("zb", 0), ("f1", 0), ("zc", 0), ("f2", 0), ("za", 2), ("r", 1), ("s", 0), ("f3", 0),
    ("za", 0),
]
PLAN_2 = [
    ("a", 2), ("a", 4), ("b", 4), ("a", 6), ("c", 4), ("x", 1), ("c", 2), ("b", 2), ("b", 3), ("x", 5), ("b", 5),
    ("x", 7), ("c", 6), ("b", 7), ("b", 6), ("b", 1), ("x", 3), ("w", 0), ("k", 2, 6), ("k", 4, 7), ("zb", 1),
    ("k", 3, 5), ("zc", 1), ("r", 7), ("zb", 0), ("k", 0, 1), ("t", 1), ("za", 1), ("zb", 2), ("r", 5), ("zc", 2),
    ("t", 0), ("zc", 0), ("r", 3), ("za", 0), ("r", 1), ("za", 2), ("f1", 0), ("f2", 0), ("s", 0), ("f3", 0),
    ("-", 0),
]
PLAN_3 = [
    ("a", 2), ("c", 2), ("b", 1), ("x", 1), ("a", 4), ("a", 6), ("b", 2), ("x", 5), ("b", 4), ("c", 4), ("w", 0),
    ("k", 0, 4), ("b", 5), ("c", 6), ("x", 7), ("k", 1, 5), ("zb", 1), ("b", 7), ("x", 3), ("t", 1), ("b", 6),
    ("k", 6, 7), ("b", 3), ("zb", 2), ("zc", 1), ("r", 5), ("k", 2, 3), ("zc", 2), ("r", 7), ("s", 0), ("za", 1),
    ("zb", 0), ("za", 2), ("zc", 0), ("r", 3), ("t", 0), ("r", 1), ("f1", 0), ("f2", 0), ("za", 0), ("f3", 0),
    ("-", 0),
]
PLANS = {4: (PLAN_0, PLAN_1, PLAN_2, PLAN_3)}


def dense_kernel(
    ep_count, tp_count, minor, near, wide, keep, both_keep, plans,
    ids_hbm, rw_hbm, gain_hbm, tok_hbm, gate_hbm, up_hbm, down_hbm, sg_hbm, su_hbm, sd_hbm,
    out_ref,
    ids_ref, rw_ref, gain_ref, tok, xb, xo, wtab, wr, wg, wu, wd, sg, su, sd, sh_all, sh_out,
    pa, pb, pc, xs, xr, ys, yr, ycs, ycr, zas, zar, zbs, zbr, zcs, zcr, fs, fr, gs, gr, head, head_in, last_b, last_m, acc_a, acc_b, acc_c,
    line_sem, load_sem, wt_s, wt_r, we_s, we_r, sh_s, sh_r, yb_s,
    a_s, a_r, b_s, b_r, c_r, ya_s, ya_r, xa_s, xa_r,
    rx_s, rx_r, ry_s, ry_r, ryc_s, ryc_r, rza_s, rza_r, rzb_s, rzb_r, rzc_s, rzc_r, f_s, f_r, g_s, g_r, o_s, o_r,
):
    n = ep_count
    major = n // minor
    half, width = xo.shape
    side = width // 2
    quarter = width // tp_count
    tail = side - keep - both_keep
    middle = keep + both_keep
    e = lax.axis_index("ep")
    t = lax.axis_index("tp")
    z = e // minor
    y = e % minor
    xi = t // 2
    c = t % 2
    t2 = 2 * (1 - xi) + c
    other_y = z * minor + 1 - y
    mate_x = {"tp": t2}
    mate_c = {"tp": 2 * xi + 1 - c}
    mate_y = {"ep": other_y}
    owner = 2 * xi + 1
    far_owner = 2 * (1 - xi) + 1
    z_up = {"ep": lax.rem(e + minor, n)}
    z_down = {"ep": lax.rem(e + n - minor, n)}
    far = {"ep": (major - 1 - z) * minor + y}
    is_end = (z == 0) | (z == major - 1)

    barrier = pltpu.get_barrier_semaphore()

    def greet_line(sem):
        @pl.when(z < major - 1)
        def _():
            pl.semaphore_signal(sem, inc=1, device_id=z_up, device_id_type=MESH)

        @pl.when(z > 0)
        def _():
            pl.semaphore_signal(sem, inc=1, device_id=z_down, device_id_type=MESH)

    in_line = jnp.where(is_end, 1, 2)
    greet_line(barrier)
    for k in range(1, tp_count):
        pl.semaphore_signal(barrier, inc=1, device_id={"tp": lax.rem(t + k, tp_count)}, device_id_type=MESH)
    for k in range(tp_count):
        there = {"ep": other_y, "tp": lax.rem(t + k, tp_count)}
        pl.semaphore_signal(barrier, inc=1, device_id=there, device_id_type=MESH)

    def remote(src, dst, s, r, who):
        return pltpu.make_async_remote_copy(
            src_ref=src, dst_ref=dst, send_sem=s, recv_sem=r, device_id=who, device_id_type=MESH
        )

    def rows_of(which):
        return pl.ds(pl.multiple_of(which * half, half), half)

    def side_of(which):
        return pl.ds(pl.multiple_of(which * side, side), side)

    loads = [
        pltpu.make_async_copy(a, b, load_sem.at[i])
        for i, (a, b) in enumerate(
            (
                (tok_hbm.at[rows_of(c)], tok.at[0]),
                (tok_hbm.at[rows_of(1 - c)], tok.at[1]),
                (gate_hbm, wg.at[c]),
                (up_hbm, wu.at[c]),
                (down_hbm.at[:, side_of(xi)], wd.at[c, :, pl.ds(0, side)]),
                (down_hbm.at[:, side_of(1 - xi)], wd.at[c, :, pl.ds(side, side)]),
                (sg_hbm, sg),
                (su_hbm, su),
                (sd_hbm, sd),
                (gain_hbm, gain_ref),
                (ids_hbm, ids_ref),
                (rw_hbm, rw_ref),
            )
        )
    ]
    for i in (0, 9, 10, 11, 2, 3, 4, 5, 1, 6, 7, 8):
        loads[i].start()

    step = 16

    def norm_into(which, store):
        def body(i, carry):
            part = pl.ds(pl.multiple_of(i * step, step), step)
            v = tok[which, part, :].astype(jnp.float32)
            r = lax.rsqrt(jnp.mean(v * v, axis=-1, keepdims=True) + NORM_EPSILON)
            store(part, (v * r * gain_ref[...]).astype(jnp.bfloat16))
            return carry

        lax.fori_loop(0, half // step, body, 0, unroll=True)

    def store_own(part, value):
        xb[e, part, :] = value

    def store_rest(part, value):
        xo[part, :] = value

    def weights_for(expert):
        row = jnp.zeros((1, ids_ref.shape[1]), jnp.float32)
        for k in range(ids_ref.shape[0]):
            row += jnp.where(ids_ref[k : k + 1, :] == expert, rw_ref[k : k + 1, :], 0.0)
        return row

    loads[0].wait()
    loads[9].wait()
    norm_into(0, store_own)
    loads[10].wait()
    loads[11].wait()
    for d in range(n):
        wtab[d] = weights_for(d * (tp_count // 2) + xi)
    wr[e] = weights_for(e * (tp_count // 2) + xi)
    pl.semaphore_wait(barrier, 2 * tp_count - 1 + in_line)
    greet_line(line_sem.at[0])

    mine = pl.ds(pl.multiple_of(xi * near, LANES), near)
    theirs = pl.ds(pl.multiple_of((1 - xi) * near, LANES), near)
    shared_cols = pl.ds(2 * near, wide)
    rest = pl.ds(2 * near + wide, width - 2 * near - wide)

    def line_a(g, who):
        ref = xb.at[g, :, mine]
        return remote(ref, ref, a_s, a_r.at[g // minor], who)

    def line_b(g, who):
        ref = xb.at[g, :, rest]
        return remote(ref, ref, b_s, b_r.at[g], who)

    def line_c(g, who):
        ref = xb.at[g, :, shared_cols]
        return remote(ref, ref, a_s, c_r.at[g // minor], who)

    def y_shared(g):
        ref = xb.at[g, :, shared_cols]
        return remote(ref, ref, ya_s, xa_r.at[g], mate_y)

    def y_first():
        ref = xb.at[e, :, rest]
        return remote(ref, ref, yb_s, b_r.at[e], mate_y)

    def y_copy(g):
        ref = xb.at[g, :, mine]
        return remote(ref, ref, ya_s, ya_r.at[g // minor], mate_y)

    def x_copy(g):
        ref = xb.at[g, :, mine]
        return remote(ref, ref, xa_s, xa_r.at[g], mate_x)

    def x_arrival(g):
        ref = xb.at[g, :, theirs]
        return remote(ref, ref, xa_s, xa_r.at[g], mate_x)

    def cross_arrival(g):
        ref = xb.at[g, :, pl.ds(0, near + wide)]
        return remote(ref, ref, xa_s, xa_r.at[g], mate_x)

    def wt_copy(target):
        return remote(wtab.at[target], wr.at[e], wt_s, wt_r, {"ep": target})

    def wt_all():
        return remote(wtab.at[pl.ds(0, n - 1)], wr.at[pl.ds(0, n - 1)], wt_s, wt_r, mate_y)

    def weight_copy(i, which):
        ref = (wg, wu, wd)[i].at[which]
        return remote(ref, ref, we_s.at[i], we_r.at[i], mate_c)

    def sh_copy(who):
        return remote(sh_all.at[t], sh_all.at[t], sh_s, sh_r, {"tp": who})

    def sh_rest():
        ref = sh_all.at[pl.ds(0, tp_count - 1)]
        return remote(ref, ref, sh_s, sh_r, mate_c)

    def order(j):
        k = jnp.minimum(z, major - 1 - z)
        d = (j + 1) // 2
        close = jnp.where((j % 2 == 1) == (2 * z < major), z - d, z + d)
        far = jnp.where(z <= major - 1 - z, j, major - 1 - j)
        return jnp.where(j <= 2 * k, close, far)

    def slot_group(i):
        p = order(i // 2)
        yy = jnp.where(i % 2 == 0, y, 1 - y)
        return p, p * minor + yy

    def ups(p):
        return (p <= z) & (z < major - 1)

    def downs(p):
        return (p >= z) & (z > 0)

    def forward(p, g, line):
        @pl.when(ups(p))
        def _():
            line(g, z_up).start()

        @pl.when(downs(p))
        def _():
            line(g, z_down).start()

    forward(z, e, line_a)
    y_first().start()
    forward(z, e, line_c)
    y_copy(e).start()
    y_shared(e).start()
    forward(z, e, line_b)
    loads[2].wait()
    weight_copy(0, c).start()
    loads[3].wait()
    weight_copy(1, c).start()
    loads[4].wait()
    loads[5].wait()
    weight_copy(2, c).start()
    loads[1].wait()
    norm_into(1, store_rest)
    loads[6].wait()
    loads[7].wait()

    def shared_in(x):
        g_sum = jnp.dot(x, sg[...], preferred_element_type=jnp.float32)
        u_sum = jnp.dot(x, su[...], preferred_element_type=jnp.float32)
        return (silu(g_sum) * u_sum).astype(jnp.bfloat16)

    sh_all[t, c] = shared_in(xb[e])
    sh_all[t, 1 - c] = shared_in(xo[...])
    for k in range(1, tp_count):
        sh_copy(lax.rem(t + k, tp_count)).start()
    for k in range(major - 1):
        pl.semaphore_wait(line_sem.at[k], in_line)
        if k < major - 2:
            greet_line(line_sem.at[k + 1])
    for k in range(1, n):
        wt_copy(lax.rem(e + k, n)).start()

    def rx_copy(g):
        return remote(xs.at[g], xr.at[g], rx_s, rx_r.at[g], mate_x)

    def ry_copy(p):
        return remote(ys.at[p], yr.at[p], ry_s, ry_r.at[p], mate_y)

    def ryc_copy(p):
        return remote(ycs.at[p], ycr.at[p], ryc_s, ryc_r.at[p], mate_y)

    def rzc_copy(p, slot, who):
        return remote(zcs.at[p], zcr.at[slot], rzc_s, rzc_r.at[slot], who)

    def rza_copy(p, slot, who):
        return remote(zas.at[p], zar.at[slot], rza_s, rza_r.at[slot], who)

    def rzb_copy(g, slot, who):
        return remote(zbs.at[g], zbr.at[slot], rzb_s, rzb_r.at[slot], who)

    def down_slot(key, p, to, count, extra):
        return jnp.where(p == to, count + extra, key)

    diagonal = lax.broadcasted_iota(jnp.int32, (half, 2 * half), 1) == (
        lax.broadcasted_iota(jnp.int32, (half, 2 * half), 0) + c * half
    )

    def weight_of(g):
        return jnp.sum(jnp.where(diagonal, wr[g], 0.0), axis=1, keepdims=True)

    def compute(i, j, first, second, both):
        pair = ((i, first), (j, second))
        weight = jnp.concatenate([weight_of(first), weight_of(second)], axis=0)
        x = jnp.concatenate([xb[first], xb[second]], axis=0)
        acts = []
        for h in range(2):
            g_sum = jnp.dot(x, wg[h], preferred_element_type=jnp.float32)
            u_sum = jnp.dot(x, wu[h], preferred_element_type=jnp.float32)
            acts.append((silu(g_sum) * u_sum).astype(jnp.bfloat16))

        def columns(low, high):
            total = jnp.dot(acts[0], wd[0, :, low:high], preferred_element_type=jnp.float32)
            total += jnp.dot(acts[1], wd[1, :, low:high], preferred_element_type=jnp.float32)
            return total * weight

        sent = columns(side, side + keep).astype(jnp.bfloat16)
        kept = columns(0, keep)
        kept_c = columns(keep, middle)
        rest_c = columns(side + keep, side + middle)
        main = columns(middle, side)
        rest = columns(side + middle, width)

        def put(k):
            index, g = pair[k]
            part = slice(k * half, (k + 1) * half)
            xs[g] = sent[part]

            @pl.when(index > 1)
            def _():
                rx_copy(g).start()

            pc[g, :, :both_keep] = kept_c[part]
            pc[g, :, both_keep:] = rest_c[part]

            @pl.when(index % 2 == 1)
            def _():
                p = g // minor
                ycs[p] = pc[g].astype(jnp.bfloat16)
                ryc_copy(p).start()

            pa[g] = kept[part]
            pb[g, :, :tail] = main[part]
            pb[g, :, tail:] = rest[part]

        put(0)

        @pl.when(both)
        def _():
            put(1)

    def add_lanes(p, acc, copy, key, received, extra=0, per=1):
        count = major * per
        below = downs(p) & jnp.logical_not((p == major - 1) & (z == 1))
        above = ups(p) & jnp.logical_not((p == 0) & (z == major - 2))

        def add(slot):
            copy(key, slot, z_up).wait_recv()
            acc[...] += received[slot].astype(jnp.float32)

        @pl.when(below)
        def _():
            add(key)

        @pl.when(above)
        def _():
            add(down_slot(key, p, z, count, extra))

        @pl.when((p == z) & is_end)
        def _():
            add(count + per + extra)

    def sum_b(p, g):
        acc_b[...] = pb[g]
        add_lanes(p, acc_b, rzb_copy, g, zbr, g % minor, minor)

    def sum_c(p, g):
        ryc_copy(p).wait_recv()
        acc_c[...] = pc[g] + ycr[p].astype(jnp.float32)
        add_lanes(p, acc_c, rzc_copy, p, zcr)

    def sum_a(p, g):
        rx_copy(g).wait_recv()
        ry_copy(p).wait_recv()
        acc_a[...] = pa[g] + xr[g].astype(jnp.float32) + yr[p].astype(jnp.float32)
        add_lanes(p, acc_a, rza_copy, p, zar)

    def line_order(q):
        above = major - 1 - z
        low = jnp.where(q < above, z + 1 + q, z - 1 - (q - above))
        high = jnp.where(q < z, z - 1 - q, z + 1 + (q - z))
        return jnp.where(2 * z < major, low, high)

    def send_sum(copy, key, p, extra=0, per=1):
        count = major * per
        whole = is_end & (p == major - 1 - z)

        @pl.when((p > z) & jnp.logical_not(whole))
        def _():
            copy(key, key, z_up).start()

        @pl.when((p < z) & jnp.logical_not(whole))
        def _():
            copy(key, down_slot(key, p, z - 1, count, extra), z_down).start()

        @pl.when(whole)
        def _():
            copy(key, count + per + extra, far).start()

    def do_a(i):
        p, g = slot_group(i)
        line_a(g, z_up).wait_recv()
        forward(p, g, line_a)
        y_copy(g).start()
        x_copy(g).start()

    def do_c(i):
        p, g = slot_group(i)
        line_c(g, z_up).wait_recv()
        forward(p, g, line_c)
        y_shared(g).start()

    def do_b(i):
        p, g = slot_group(i)
        line_b(g, z_up).wait_recv()
        forward(p, g, line_b)

    def do_x(i):
        _, g = slot_group(i)
        y_copy(g).wait_recv()
        x_copy(g).start()

    def do_k(code):
        i, j = code // FIELD, code % FIELD
        both = j < FIELD - 1
        _, first = slot_group(i)
        _, second = slot_group(jnp.where(both, j, i))

        def ready(index, g):
            @pl.when(index % 2 == 1)
            def _():
                cross_arrival(g).wait_recv()

            @pl.when(index % 2 == 0)
            def _():
                x_arrival(g).wait_recv()

        @pl.when(i > 0)
        def _():
            ready(i, first)

        @pl.when(both)
        def _():
            ready(j, second)

        compute(i, j, first, second, both)

    def do_w(_):
        for k in range(3):
            weight_copy(k, 1 - c).wait_recv()
        wt_all().wait_recv()

    def do_t(i):
        _, g = slot_group(i)
        rx_copy(g).start()

    def do_r(i):
        p, g = slot_group(i)
        rx_copy(g).wait_recv()
        ys[p] = (pa[g] + xr[g].astype(jnp.float32)).astype(jnp.bfloat16)
        ry_copy(p).start()

    def do_s(_):
        loads[8].wait()
        sh_rest().wait_recv()
        share = sg.shape[1]
        for r in range(2):
            shared = jnp.zeros((half, quarter), jnp.float32)
            for q in range(tp_count):
                shared += jnp.dot(
                    sh_all[q, r], sd[q * share : (q + 1) * share, :],
                    preferred_element_type=jnp.float32,
                )
            sh_out[r] = shared

    def do_zb(q):
        p = line_order(q)
        for yy in (1 - y, y):
            g = p * minor + yy
            sum_b(p, g)
            zbs[g] = acc_b[...].astype(jnp.bfloat16)
            send_sum(rzb_copy, g, p, g % minor, minor)

    def do_zc(q):
        p = line_order(q)
        sum_c(p, p * minor + y)
        zcs[p] = acc_c[...].astype(jnp.bfloat16)
        send_sum(rzc_copy, p, p)

    def do_za(q):
        p = line_order(q)
        sum_a(p, p * minor + y)
        zas[p] = acc_a[...].astype(jnp.bfloat16)
        send_sum(rza_copy, p, p)

    def last_copy(i):
        who = (
            {"ep": other_y, "tp": owner}, {"ep": other_y, "tp": far_owner}, {"tp": far_owner}, {"tp": owner},
        )[i]
        return remote(fs.at[i], fr.at[c, i], f_s, f_r.at[c], who)

    def last_c_copy(i):
        return remote(gs.at[i], gr.at[c, i], g_s, g_r.at[c], ({"tp": far_owner}, {"tp": owner})[i])

    def last_rows(which, count):
        b, m = fr.at[which, pl.ds(0, count + 2)], gr.at[which, pl.ds(0, count)]
        return remote(b, b, f_s, f_r.at[which], mate_c), remote(m, m, g_s, g_r.at[which], mate_c)

    head_copy = remote(head, head_in, o_s, o_r, mate_c)

    def do_f1(_):
        sum_b(z, other_y)
        fs[0] = acc_b[:, :tail].astype(jnp.bfloat16)
        fs[1] = acc_b[:, tail:].astype(jnp.bfloat16)
        last_copy(0).start()
        last_copy(1).start()

    def do_f2(_):
        sum_b(z, e)
        fs[2] = acc_b[:, tail:].astype(jnp.bfloat16)
        last_copy(2).start()
        last_b[...] = acc_b[:, :tail]

        @pl.when(c == 0)
        def _():
            fs[3] = acc_b[:, :tail].astype(jnp.bfloat16)
            last_copy(3).start()

    def do_f3(_):
        sum_c(z, e)
        gs[0] = acc_c[:, both_keep:].astype(jnp.bfloat16)
        last_c_copy(0).start()
        last_m[...] = acc_c[:, :both_keep]

        @pl.when(c == 0)
        def _():
            gs[1] = acc_c[:, :both_keep].astype(jnp.bfloat16)
            last_c_copy(1).start()

    actions = (
        (do_a, do_c, do_b, do_x, do_k, do_t, do_r, do_w),
        (do_s, do_zb, do_zc, do_za, do_f1, do_f2, do_f3),
    )

    block = 8
    codes = [functools.reduce(lambda held, k: jnp.where(z == k, at[k], held), range(1, major), z * 0 + at[0]) for at in zip(*plans)]
    codes += [codes[-1] * 0 + FIELD * FIELD * 15] * (-len(codes) % block)

    def main_block(b, carry):
        held = codes[:block]
        for k in range(block, len(codes), block):
            held = [jnp.where(b == k // block, new, old) for new, old in zip(codes[k : k + block], held)]

        def main_step(i, carry):
            code = held[0]
            for k in range(1, block):
                code = jnp.where(i == k, held[k], code)
            kind = code // (FIELD * FIELD)
            arg = code % (FIELD * FIELD)
            for part, group in enumerate(actions):

                @pl.when(kind // 8 == part)
                def _(group=group):
                    for a, action in enumerate(group):

                        @pl.when(kind % 8 == a)
                        def _(action=action):
                            action(arg)

            return carry

        return lax.fori_loop(0, block, main_step, carry)

    lax.fori_loop(0, len(codes) // block, main_block, 0)

    def drained(ref, sem):
        remote(ref, ref, sem, a_r.at[0], mate_c).wait_send()

    def lines_sent(count):
        groups = pl.ds(0, count)
        drained(xb.at[groups, :, pl.ds(0, near + wide)], a_s)
        drained(xb.at[groups, :, pl.ds(0, 2 * (width - 2 * near - wide))], b_s)

    @pl.when(is_end)
    def _():
        lines_sent(1)

    @pl.when(jnp.logical_not(is_end))
    def _():
        lines_sent(major + 1)

    drained(xb.at[pl.ds(0, major), :, pl.ds(0, near + wide)], ya_s)
    drained(xb.at[pl.ds(0, n - 1), :, pl.ds(0, near)], xa_s)
    drained(xs, rx_s)
    drained(ys, ry_s)
    drained(ycs, ryc_s)
    for i in range(3):
        weight_copy(i, c).wait_send()
    y_first().wait_send()
    wt_all().wait_send()
    sh_rest().wait_send()

    sum_a(z, e)

    def total(ref):
        return sum(ref[i].astype(jnp.float32) for i in range(1, ref.shape[0])) + ref[0].astype(jnp.float32)

    @pl.when(c == 0)
    def _():
        out_ref[:half, :] = (acc_a[...] + sh_out[0]).astype(jnp.bfloat16)
        head_copy.wait_recv()
        out_ref[half:, :] = (head_in[...] + sh_out[1]).astype(jnp.bfloat16)
        for copy in last_rows(0, 2):
            copy.wait_send()

    @pl.when(c == 1)
    def _():
        head[...] = acc_a[...]
        head_copy.start()
        for copy in last_rows(1, 1):
            copy.wait_recv()
        low, high = slice(0, both_keep), slice(both_keep, quarter)
        out_ref[half:, low] = (last_m[...] + gr[1, 0].astype(jnp.float32) + sh_out[1, :, low]).astype(jnp.bfloat16)
        out_ref[half:, high] = (last_b[...] + total(fr.at[1, pl.ds(0, 3)]) + sh_out[1, :, high]).astype(jnp.bfloat16)
        for copy in last_rows(0, 2):
            copy.wait_recv()
        out_ref[:half, low] = (total(gr.at[0]) + sh_out[0, :, low]).astype(jnp.bfloat16)
        out_ref[:half, high] = (total(fr.at[0]) + sh_out[0, :, high]).astype(jnp.bfloat16)
        for copy in last_rows(1, 1):
            copy.wait_send()
        head_copy.wait_send()


    drained(zas.at[pl.ds(0, major - 1)], rza_s)
    drained(zcs.at[pl.ds(0, major - 1)], rzc_s)
    drained(zbs.at[pl.ds(0, n - minor)], rzb_s)


def coded(plan):
    codes = []
    for kind, first, *second in plan:
        arg = first * FIELD + (second[0] if second else FIELD - 1) if kind == "k" else first
        codes.append((KINDS.index(kind) * FIELD * FIELD) + arg)
    return codes


def dense_exchange(
    tokens, norm_gain, expert_ids, route_weights, expert_gate, expert_up, expert_down,
    shared_gate, shared_up, shared_down,
):
    n = lax.axis_size("ep")
    tp_count = lax.axis_size("tp")
    minor = 1 << (n.bit_length() - 1) // 2
    major = n // minor
    rows, width = tokens.shape
    half = rows // 2
    side = width // 2
    quarter = width // tp_count
    near = side * NEAR // 8 // LANES * LANES
    wide = 2 * (side * WIDE // 8 // LANES * LANES)
    keep = quarter
    both_keep = side * BOTH_KEEP // 8 // LANES * LANES
    tail = side - keep - both_keep
    ff = expert_gate.shape[2]
    share = shared_gate.shape[1]
    bf16, f32 = jnp.bfloat16, jnp.float32
    dma = pltpu.SemaphoreType.DMA
    vmem = pl.BlockSpec(memory_space=pltpu.VMEM)
    anywhere = pl.BlockSpec(memory_space=pl.ANY)
    return pl.pallas_call(
        functools.partial(dense_kernel, n, tp_count, minor, near, wide, keep, both_keep, [coded(plan) for plan in PLANS[n // minor]]),
        out_shape=pltpu.VMEM((rows, quarter), bf16),
        in_specs=[anywhere] * 10,
        out_specs=vmem,
        scratch_shapes=[
            pltpu.VMEM((expert_ids.shape[1], rows), jnp.int32),
            pltpu.VMEM((expert_ids.shape[1], rows), f32),
            pltpu.VMEM((1, width), f32),
            pltpu.VMEM((2, half, width), bf16),
            pltpu.VMEM((n, half, width), bf16),
            pltpu.VMEM((half, width), bf16),
            pltpu.VMEM((n, 1, rows), f32),
            pltpu.VMEM((n, 1, rows), f32),
            pltpu.VMEM((2, width, ff), bf16),
            pltpu.VMEM((2, width, ff), bf16),
            pltpu.VMEM((2, ff, width), bf16),
            pltpu.VMEM((width, share), bf16),
            pltpu.VMEM((width, share), bf16),
            pltpu.VMEM((share * tp_count, quarter), bf16),
            pltpu.VMEM((tp_count, 2, half, share), bf16),
            pltpu.VMEM((2, half, quarter), f32),
            pltpu.VMEM((n, half, keep), f32),
            pltpu.VMEM((n, half, 2 * tail), f32),
            pltpu.VMEM((n, half, 2 * both_keep), f32),
            pltpu.VMEM((n, half, keep), bf16),
            pltpu.VMEM((n, half, keep), bf16),
            pltpu.VMEM((major, half, keep), bf16),
            pltpu.VMEM((major, half, keep), bf16),
            pltpu.VMEM((major, half, 2 * both_keep), bf16),
            pltpu.VMEM((major, half, 2 * both_keep), bf16),
            pltpu.VMEM((major, half, keep), bf16),
            pltpu.VMEM((major + 2, half, keep), bf16),
            pltpu.VMEM((n, half, 2 * tail), bf16),
            pltpu.VMEM((n + 2 * minor, half, 2 * tail), bf16),
            pltpu.VMEM((major, half, 2 * both_keep), bf16),
            pltpu.VMEM((major + 2, half, 2 * both_keep), bf16),
            pltpu.VMEM((4, half, tail), bf16),
            pltpu.VMEM((2, 4, half, tail), bf16),
            pltpu.VMEM((2, half, both_keep), bf16),
            pltpu.VMEM((2, 2, half, both_keep), bf16),
            pltpu.VMEM((half, quarter), f32),
            pltpu.VMEM((half, quarter), f32),
            pltpu.VMEM((half, tail), f32),
            pltpu.VMEM((half, both_keep), f32),
            pltpu.VMEM((half, keep), f32),
            pltpu.VMEM((half, 2 * tail), f32),
            pltpu.VMEM((half, 2 * both_keep), f32),
            pltpu.SemaphoreType.REGULAR((major - 1,)), dma((12,)), dma, dma, dma((3,)), dma((3,)), dma, dma, dma,
            dma, dma((major,)), dma, dma((n,)), dma((major,)), dma, dma((major,)), dma, dma((n,)),
            dma, dma((n,)), dma, dma((major,)), dma, dma((major,)), dma, dma((major + 2,)),
            dma, dma((n + 2 * minor,)), dma, dma((major + 2,)), dma, dma((2,)), dma, dma((2,)), dma, dma,
        ],
        compiler_params=pltpu.CompilerParams(
            collective_id=0, has_side_effects=True, vmem_limit_bytes=60 << 20
        ),
        name="dense_moe",
    )(
        expert_ids.T, route_weights.T, norm_gain.reshape(1, width), tokens,
        expert_gate[0], expert_up[0], expert_down[0],
        shared_gate, shared_up, shared_down,
    )


def local(tokens, *rest):
    ep_count = lax.axis_size("ep")
    pair_count = lax.axis_size("tp") // 2
    dense_bytes = 4 * ep_count * tokens.size * tokens.dtype.itemsize
    minor = 1 << (ep_count.bit_length() - 1) // 2
    if pair_count == 2 and minor == 2 and ep_count // minor in PLANS and dense_bytes <= 24 << 20:
        return dense_exchange(tokens, *rest)
    return routed_exchange(tokens, *rest)


def solution(mesh):
    return jax.shard_map(
        local,
        mesh=mesh,
        in_specs=(
            P("ep", None),
            P(),
            P("ep", None),
            P("ep", None),
            P(("ep", "tp"), None, None),
            P(("ep", "tp"), None, None),
            P(("ep", "tp"), None, None),
            P(None, "tp"),
            P(None, "tp"),
            P(None, "tp"),
        ),
        out_specs=P("ep", "tp"),
        check_vma=False,
    )
```
